32 devices in a mesh: ep: 8 (over z, x), tp: 4 (over y, core).
Axes of the slice: x: 2, y: 2, z: 4, core: 2. Of those that a mesh axis runs over, the one named last changes fastest.
Arguments:
- tokens: bfloat16 [1024, 2048], P('ep'), may hold values from -6 to 6
- routing: int32 [1024, 2], P('ep'), may hold values from 0 to 7, all different within a row; in each aligned block of 128 rows (0 to 127, 128 to 255, ...) at most 56 rows name the same one
- router_weight: bfloat16 [2048, 8], replicated, may hold values from -0.125 to 0.125
- gate_weight: bfloat16 [8, 2048, 2048], P('ep', None, 'tp'), may hold values from -0.125 to 0.125
- up_weight: bfloat16 [8, 2048, 2048], P('ep', None, 'tp'), may hold values from -0.125 to 0.125
- down_weight: bfloat16 [8, 2048, 2048], P('ep', 'tp'), may hold values from -0.125 to 0.125
- cotangent: bfloat16 [1024, 2048], P('ep'), may hold values from -0.796875 to 0.796875
Outputs:
- token_grad: bfloat16 [1024, 2048], P('ep')
- router_grad: float32 [2048, 8], P('tp')
- router_rows: float32 [2048], P('tp')
- gate_grad: bfloat16 [8, 2048, 2048], P('ep', None, 'tp')
- up_grad: bfloat16 [8, 2048, 2048], P('ep', None, 'tp')
- down_grad: bfloat16 [8, 2048, 2048], P('ep', 'tp')
- gate_rows: float32 [8, 2048], P('ep')
- up_rows: float32 [8, 2048], P('ep')
- down_rows: float32 [8, 2048], P('ep', 'tp')
The draws below stay inside these ranges and needn't reach their ends.
Inputs may be any that keep to these rules, and one draw needn't show every extreme that they name: `routing`: A row's 2 experts differ. Within the rows of one index of ep (128 rows), no expert is named more than 56 times, a bound that some block reaches.
All inputs are finite; a program needn't handle non-finite values.
Results may differ from the reference program's by a relative error of at most 0.01.
Values may be sent and summed in bfloat16 or wider, within the bound.
No kernel may reach another device: no remote copies, remote signals or barrier semaphores. Data moves between devices by JAX's collectives and lax.ppermute only.
A program may use at most 64 MiB of HBM per device.

```python
import math
import jax
import jax.numpy as jnp
import numpy as np
from jax import lax

D = 2048
FF = 2048
TOPK = 2
TOK_DEV = 128
EXPERTS = 8
TOKENS = 1024
CAP = 56
N_EP = 8


def level_of(stream_key, shape, pieces, low, high):
    gain = 1.0
    for axis_at, parts in pieces:
        steps = jax.random.uniform(jax.random.fold_in(jax.random.fold_in(stream_key, 6), axis_at), (parts,), jnp.float32, low / len(pieces), high / len(pieces))
        gain = gain * jnp.repeat(jnp.exp(steps), shape[axis_at] // parts).reshape((-1,) + (1,) * (len(shape) - 1 - axis_at))
    return gain


def shared_out(rng, own, number, rows, number_of, top, most, lean):
    sequence = jax.random.permutation(rng, number_of)
    crowded, common = shares(number_of, rows * top, most, lean, True), shares(number_of, rows * top, most, lean, False)
    places = jnp.arange(number_of)

    def named(lengths, turn):
        used = int((lengths > 0).sum())
        fixed = max(1, used // 4)
        moved = fixed + (places - fixed + turn * (used - fixed)) % max(1, number_of - fixed)
        return jnp.zeros((number_of,), jnp.int32).at[sequence[jnp.where(places < fixed, places, moved)]].set(jnp.asarray(lengths, jnp.int32))

    lengths = jnp.where(number % 4 == 0, named(crowded, number // 4), named(common, number - number // 4 - 1))
    mixed = jax.random.permutation(jax.random.fold_in(own, 3), number_of)
    donor, sink = mixed[0:number_of // 2 * 2:2], mixed[1:number_of // 2 * 2:2]
    room = jnp.minimum(lengths[donor] - 1, most - lengths[sink]) // 2
    room = jnp.where((donor == sequence[0]) | (sink == sequence[0]) | (lengths[sink] == 0), 0, jnp.maximum(room, 0))
    moved = jax.random.randint(jax.random.fold_in(own, 4), (number_of // 2,), 0, 1 << 20) % (room + 1)
    lengths = lengths.at[donor].add(-moved).at[sink].add(moved)
    members = jnp.searchsorted(jnp.cumsum(lengths), jnp.arange(rows * top), side="right").astype(jnp.int32)
    grid = members.reshape(top, rows).T
    grid = grid[jax.random.permutation(jax.random.fold_in(own, 1), rows)]
    turn = jax.random.randint(jax.random.fold_in(own, 2), (rows, 1), 0, top)
    return jnp.take_along_axis(grid, (jnp.arange(top)[None, :] + turn) % top, axis=1)


def shares(number_of, total, bound, lean, full):
    portions = [(1 << 20) // math.isqrt(standing ** lean) + 1 for standing in range(1, number_of + 1)]
    largest = bound if full else min(bound, max(-(-total // number_of), total * portions[0] // sum(portions)))
    least = 1 if total - largest >= number_of - 1 else 0
    holding, spare = [largest] + [least] * (number_of - 1), total - largest - least * (number_of - 1)
    while spare > 0:
        candidates = [i for i in range(1, number_of) if holding[i] < largest] or [i for i in range(1, number_of) if holding[i] < bound]
        whole, left = sum([portions[i] for i in candidates]), spare
        for i in candidates:
            extra = min(bound - holding[i], max(1, left * portions[i] // whole), spare)
            holding[i] = holding[i] + extra
            spare = spare - extra
    return np.array(holding)


def gaussian(stream_key, extent, width, reach, split=(), held_as=jnp.bfloat16):
    drawn = width * jax.random.normal(stream_key, extent, jnp.float32)
    if split:
        drawn = drawn * level_of(stream_key, extent, split, -0.22, 0.18)
    return jnp.clip(drawn, -reach, reach).astype(held_as)


def setup_inputs(seed: int = 0) -> dict:
    keys = jax.random.split(jax.random.key(seed), 8)
    tokens = gaussian(keys[0], (TOKENS, D), 1.0, 6.0, ((0, 8),))
    routing_keys = jax.random.split(jax.random.fold_in(keys[1], 1), TOKENS // TOK_DEV)
    routing_turns = jax.random.permutation(jax.random.fold_in(keys[1], 3), TOKENS // TOK_DEV)
    routing = jax.vmap(lambda own, number: shared_out(jax.random.fold_in(keys[1], 2), own, number, TOK_DEV, EXPERTS, TOPK, CAP, 2))(routing_keys, routing_turns).reshape((TOKENS, TOPK))
    router_weight = gaussian(keys[2], (D, EXPERTS), D ** -0.5, 0.125)
    gate_weight = gaussian(keys[3], (EXPERTS, D, FF), D ** -0.5, 0.125, ((0, 8), (2, 4)))
    up_weight = gaussian(keys[4], (EXPERTS, D, FF), D ** -0.5, 0.125, ((0, 8), (2, 4)))
    down_weight = gaussian(keys[5], (EXPERTS, FF, D), FF ** -0.5, 0.125, ((0, 8), (1, 4)))
    cotangent = gaussian(keys[6], (TOKENS, D), 0.1, 0.796875, ((0, 8),))
    return dict(tokens=tokens, routing=routing, router_weight=router_weight, gate_weight=gate_weight, up_weight=up_weight, down_weight=down_weight, cotangent=cotangent)


def block_slots(route_block):
    flat_ids = route_block.reshape(-1)
    onehot = (flat_ids[:, None] == jnp.arange(EXPERTS, dtype=jnp.int32)[None, :]).astype(jnp.int32)
    position = jnp.sum((jnp.cumsum(onehot, axis=0) - 1) * onehot, axis=1)
    return flat_ids, position.astype(jnp.int32)


def expert_backward(rows_in, cots_in, slot_scale, w_gate, w_up, w_down):
    pre_gate = jnp.dot(rows_in, w_gate, preferred_element_type=jnp.float32)
    pre_up = jnp.dot(rows_in, w_up, preferred_element_type=jnp.float32)
    sigmoid_gate = jax.nn.sigmoid(pre_gate)
    hidden = (pre_gate * sigmoid_gate * pre_up).astype(jnp.bfloat16)
    back_proj = lax.dot_general(cots_in, w_down, (((1,), (1,)), ((), ())), preferred_element_type=jnp.float32)
    gate_term = jnp.sum(hidden.astype(jnp.float32) * back_proj, axis=1)
    scaled = slot_scale * back_proj
    grad_up_pre = (scaled * pre_gate * sigmoid_gate).astype(jnp.bfloat16)
    grad_gate_pre = (scaled * pre_up * sigmoid_gate * (1.0 + pre_gate * (1.0 - sigmoid_gate))).astype(jnp.bfloat16)
    weighted = (slot_scale * cots_in.astype(jnp.float32)).astype(jnp.bfloat16)
    contract_rows = (((0,), (0,)), ((), ()))
    grad_down = lax.dot_general(hidden, weighted, contract_rows, preferred_element_type=jnp.float32)
    grad_gate = lax.dot_general(rows_in, grad_gate_pre, contract_rows, preferred_element_type=jnp.float32)
    grad_up = lax.dot_general(rows_in, grad_up_pre, contract_rows, preferred_element_type=jnp.float32)
    contract_hidden = (((1,), (1,)), ((), ()))
    partial_value = lax.dot_general(grad_gate_pre, w_gate, contract_hidden, preferred_element_type=jnp.float32)
    partial_value = partial_value + lax.dot_general(grad_up_pre, w_up, contract_hidden, preferred_element_type=jnp.float32)
    return partial_value, gate_term, grad_gate, grad_up, grad_down


def reference(tokens, routing, router_weight, gate_weight, up_weight, down_weight, cotangent):
    logits = jnp.dot(tokens, router_weight, preferred_element_type=jnp.float32)
    affinity = jax.nn.sigmoid(logits)
    chosen = jnp.take_along_axis(affinity, routing, axis=1)
    total_aff = jnp.sum(chosen, axis=1, keepdims=True)
    weights = chosen / total_aff
    assigns = TOKENS * TOPK
    flat_ids, positions = jax.vmap(block_slots)(routing.reshape(N_EP, TOK_DEV, TOPK))
    source = jnp.arange(N_EP, dtype=jnp.int32)[:, None]
    slot_index = ((flat_ids * N_EP + source) * CAP + positions).reshape(-1)
    slot_table = jnp.full((EXPERTS * N_EP * CAP,), assigns, jnp.int32)
    slot_table = slot_table.at[slot_index].set(jnp.arange(assigns, dtype=jnp.int32))
    slot_table = slot_table.reshape(EXPERTS, N_EP * CAP)
    zero_row = jnp.zeros((1, D), jnp.bfloat16)
    tok_pad = jnp.concatenate([tokens, zero_row], axis=0)
    cot_pad = jnp.concatenate([cotangent, zero_row], axis=0)
    weight_pad = jnp.concatenate([weights.astype(jnp.bfloat16).reshape(-1), jnp.zeros((1,), jnp.bfloat16)])

    def expert(operands):
        slot_ids, w_gate, w_up, w_down = operands
        rows_in = tok_pad[slot_ids // TOPK]
        cots_in = cot_pad[slot_ids // TOPK]
        slot_scale = weight_pad[slot_ids].astype(jnp.float32)[:, None]
        return expert_backward(rows_in, cots_in, slot_scale, w_gate, w_up, w_down)

    partial_value, gate_term, grad_gate, grad_up, grad_down = lax.map(expert, (slot_table, gate_weight, up_weight, down_weight))
    gate_rows = jnp.sum(grad_gate * grad_gate, axis=2)
    up_rows = jnp.sum(grad_up * grad_up, axis=2)
    down_rows = jnp.sum(grad_down * grad_down, axis=2)
    flat_table = slot_table.reshape(-1)
    slot_grad = jnp.zeros((assigns + 1, D), jnp.bfloat16).at[flat_table].set(partial_value.astype(jnp.bfloat16).reshape(-1, D))
    slot_gate = jnp.zeros((assigns + 1,), jnp.bfloat16).at[flat_table].set(gate_term.astype(jnp.bfloat16).reshape(-1))
    back_rows = jnp.sum(slot_grad[:assigns].astype(jnp.float32).reshape(TOKENS, TOPK, D), axis=1)
    d_weights = slot_gate[:assigns].astype(jnp.float32).reshape(TOKENS, TOPK)
    d_chosen = (d_weights - jnp.sum(d_weights * weights, axis=1, keepdims=True)) / total_aff
    d_logit = d_chosen * chosen * (1.0 - chosen)
    onehot = (routing[:, :, None] == jnp.arange(EXPERTS, dtype=jnp.int32)[None, None, :]).astype(jnp.float32)
    d_logits = jnp.sum(d_logit[:, :, None] * onehot, axis=1).astype(jnp.bfloat16)
    router_grad = lax.dot_general(tokens, d_logits, (((0,), (0,)), ((), ())), preferred_element_type=jnp.float32)
    router_rows = jnp.sum(router_grad * router_grad, axis=1)
    router_back = lax.dot_general(d_logits, router_weight, (((1,), (1,)), ((), ())), preferred_element_type=jnp.float32)
    token_grad = (back_rows + router_back).astype(jnp.bfloat16)
    return (token_grad, router_grad, router_rows, grad_gate.astype(jnp.bfloat16), grad_up.astype(jnp.bfloat16),
            grad_down.astype(jnp.bfloat16), gate_rows, up_rows, down_rows)
```

```python
import functools

import jax
import jax.numpy as jnp
from jax import lax
from jax.experimental import pallas as pl
from jax.experimental.pallas import tpu as pltpu
from jax.sharding import PartitionSpec as P

BF16 = jnp.bfloat16
F32 = jnp.float32
VMEM = pl.BlockSpec(memory_space=pltpu.VMEM)
SMEM = pl.BlockSpec(memory_space=pltpu.SMEM)
LO_LANE = 64


def dot(a, b, ca=1, cb=0):
    return lax.dot_general(a, b, (((ca,), (cb,)), ((), ())), preferred_element_type=F32)


def params(mib=40):
    return pltpu.CompilerParams(vmem_limit_bytes=mib * 1024 * 1024)


def cost(flops, bytes_accessed):
    return pl.CostEstimate(flops=flops, bytes_accessed=bytes_accessed, transcendentals=0)


def one_hot(place, slots):
    experts, toks = place.shape
    rows = lax.broadcasted_iota(jnp.int32, (slots, toks), 0).astype(F32)
    return [(rows == place[e : e + 1, :]).astype(F32) for e in range(experts)]


def route_kernel(slots, q_ref, tok_ref, routing_ref, router_ref, rows_ref, aff_ref, place_ref):
    toks = tok_ref.shape[0]
    experts = router_ref.shape[1]
    cols = rows_ref.shape[2]
    start = pl.multiple_of(q_ref[0] * cols, 128)
    logits = dot(tok_ref[...], router_ref[...])
    aff = jax.nn.sigmoid(logits.T)
    ids = lax.broadcasted_iota(jnp.int32, (toks, experts), 1)
    routed = routing_ref[...]
    named = jnp.zeros((toks, experts), F32)
    for k in range(routed.shape[1]):
        named = named + (ids == routed[:, k : k + 1]).astype(F32)
    named = named.T
    before = lax.broadcasted_iota(jnp.int32, (toks, toks), 0)
    after = lax.broadcasted_iota(jnp.int32, (toks, toks), 1)
    earlier = (before < after).astype(F32).astype(BF16)
    position = dot(named.astype(BF16), earlier)
    place = jnp.where(named > 0, position, -1.0)
    chosen = named * aff
    weights = chosen / jnp.sum(chosen, axis=0, keepdims=True)
    aff_ref[...] = aff
    place_ref[...] = place
    hot = one_hot(place, slots)
    full = jnp.concatenate(hot, axis=0).astype(BF16)
    sent = dot(full, tok_ref[:, pl.ds(start, cols)])
    lane = lax.broadcasted_iota(jnp.int32, (8, cols), 1)
    for e in range(experts):
        column = jnp.sum(hot[e] * weights[e : e + 1, :], axis=1, keepdims=True)
        tile = jnp.zeros((8, cols), F32)
        for g in range(slots // 8):
            tile = jnp.where(lane == g, column[8 * g : 8 * g + 8, :], tile)
        block = jnp.concatenate([sent[e * slots : (e + 1) * slots, :], tile], axis=0)
        rows_ref[e] = block.astype(BF16)


def cots_kernel(slots, q_ref, cot_ref, place_ref, cots_ref):
    cols = cots_ref.shape[2]
    start = pl.multiple_of((q_ref[0] % 2) * cols, 128)
    hot = one_hot(place_ref[...], slots)
    full = jnp.concatenate(hot, axis=0).astype(BF16)
    sent = dot(full, cot_ref[:, pl.ds(start, cols)])
    for e in range(len(hot)):
        cots_ref[e] = sent[e * slots : (e + 1) * slots, :].astype(BF16)


def gate_up_kernel(q_ref, x_ref, wg_ref, wu_ref, hid_ref, up_ref, gate_ref, acc_g, acc_u):
    step = pl.program_id(0)
    x = x_ref[0]
    part_g = dot(x, wg_ref[...])
    part_u = dot(x, wu_ref[...])

    @pl.when(step == 0)
    def _():
        acc_g[...] = part_g
        acc_u[...] = part_u

    @pl.when(step > 0)
    def _():
        acc_g[...] += part_g
        acc_u[...] += part_u

    @pl.when(step == pl.num_programs(0) - 1)
    def _():
        pre_gate = acc_g[...]
        pre_up = acc_u[...]
        sig = jax.nn.sigmoid(pre_gate)
        act = pre_gate * sig
        hid_ref[...] = (act * pre_up).astype(BF16)
        up_ref[...] = act
        gate_ref[...] = pre_up * sig * (1.0 + pre_gate * (1.0 - sig))


def back_kernel(half, q_ref, z_ref, wd_ref, back_ref):
    cols = z_ref.shape[1]
    start = pl.multiple_of(((q_ref[0] % 2) ^ half) * cols, 128)
    back_ref[...] = dot(z_ref[...], wd_ref[:, pl.ds(start, cols)], 1, 1)


def slot_parts(q_ref, first, gg, gu, wg_ref, wu_ref, shares):
    cols = wg_ref.shape[0] // shares
    start = pl.multiple_of((q_ref[0] ^ first) * cols, 128)
    return dot(gg, wg_ref[pl.ds(start, cols), :], 1, 1) + dot(
        gu, wu_ref[pl.ds(start, cols), :], 1, 1
    )


def split_tile(value, cols):
    lane = lax.broadcasted_iota(jnp.int32, (8, cols), 1)
    high = value.astype(BF16).astype(F32)
    low = pltpu.roll(jnp.where(lane < LO_LANE, value - high, 0.0), LO_LANE, 1)
    return jnp.where(lane < LO_LANE, high, low)


def join_tile(value, cols):
    lane = lax.broadcasted_iota(jnp.int32, (8, cols), 1)
    low = pltpu.roll(jnp.where((lane >= LO_LANE) & (lane < 2 * LO_LANE), value, 0.0), cols - LO_LANE, 1)
    return jnp.where(lane < LO_LANE, value + low, 0.0)


def middle_kernel(
    slots, shares, q_ref, back_ref, z_ref, wd_ref, scale_ref, hid_ref, up_ref, gate_ref,
    wg_ref, wu_ref, gg_ref, gu_ref, odd_ref, term_ref,
):
    cols = z_ref.shape[1]
    start = pl.multiple_of(((q_ref[0] % 2) ^ 1) * cols, 128)
    back = back_ref[...] + dot(z_ref[...], wd_ref[:, pl.ds(start, cols)], 1, 1)
    term = jnp.sum(hid_ref[...].astype(F32) * back, axis=1, keepdims=True)
    scaled = scale_ref[...] * back
    gu = (scaled * up_ref[...]).astype(BF16)
    gg = (scaled * gate_ref[...]).astype(BF16)
    gu_ref[...] = gu
    gg_ref[...] = gg
    groups = odd_ref.shape[1]
    width = odd_ref.shape[3]
    lane = lax.broadcasted_iota(jnp.int32, (8, width), 1)
    for e in range(groups):
        tile = jnp.zeros((8, width), F32)
        for g in range(slots // 8):
            at = e * slots + 8 * g
            tile = jnp.where(lane == g, term[at : at + 8, :], tile)
        term_ref[e] = tile
    for j in range(shares // 2):
        part = slot_parts(q_ref, 2 * j + 1, gg, gu, wg_ref, wu_ref, shares)
        for e in range(groups):
            tile = split_tile(term_ref[e], width)
            block = jnp.concatenate([part[e * slots : (e + 1) * slots, :], tile], axis=0)
            odd_ref[j, e] = block.astype(BF16)


def even_kernel(slots, shares, q_ref, gg_ref, gu_ref, wg_ref, wu_ref, term_ref, even_ref):
    groups = even_ref.shape[1]
    for j in range(shares // 2):
        part = slot_parts(q_ref, 2 * j, gg_ref[...], gu_ref[...], wg_ref, wu_ref, shares)
        for e in range(groups):
            even_ref[j, e, :slots, :] = part[e * slots : (e + 1) * slots, :]
            even_ref[j, e, slots:, :] = term_ref[e]


def add_core_kernel(slots, own_ref, got_ref, out_ref):
    width = out_ref.shape[3]
    for j in range(out_ref.shape[0]):
        for e in range(out_ref.shape[1]):
            got = got_ref[j + 1, e].astype(F32)
            own = own_ref[j + 1, e]
            tile = own[slots:] + join_tile(got[slots:], width)
            block = jnp.concatenate([own[:slots] + got[:slots], split_tile(tile, width)], axis=0)
            out_ref[j, e] = block.astype(BF16)


def add_chip_kernel(slots, own_ref, core_ref, chip_ref, out_ref):
    width = out_ref.shape[2]
    for e in range(out_ref.shape[0]):
        own = own_ref[0, e]
        got = core_ref[0, e].astype(F32)
        rows = own[:slots] + got[:slots]
        tile = own[slots:] + join_tile(got[slots:], width)
        for j in range(chip_ref.shape[0]):
            got = chip_ref[j, e].astype(F32)
            rows = rows + got[:slots]
            tile = tile + join_tile(got[slots:], width)
        out_ref[e] = jnp.concatenate([rows, tile], axis=0).astype(BF16)


def grads_kernel(
    q_ref, x_ref, gg_ref, gu_ref, gate_out, up_out, rows_out
):
    x = x_ref[0]
    gate = dot(x, gg_ref[...], 0, 0)
    up = dot(x, gu_ref[...], 0, 0)
    gate_out[...] = gate.astype(BF16)
    up_out[...] = up.astype(BF16)
    rows_out[0, 0:1, :] = square_rows(gate)
    rows_out[0, 1:2, :] = square_rows(up)


def square_rows(value):
    square = value * value
    folded = square[:, :128]
    for at in range(128, value.shape[1], 128):
        folded = folded + square[:, at : at + 128]
    return jnp.sum(folded.T, axis=0, keepdims=True)


def down_kernel(q_ref, z_ref, scale_ref, hid_ref, down_out, rows_out):
    weighted = (scale_ref[...] * z_ref[0].astype(F32)).astype(BF16)
    down = dot(hid_ref[...], weighted, 0, 0)
    down_out[...] = down.astype(BF16)
    rows_out[0] = square_rows(down)


def home_kernel(slots, q_ref, got_ref, place_ref, aff_ref, tok_ref, router_ref, token_out, part_out):
    experts, span, cols = got_ref.shape
    toks = place_ref.shape[1]
    start = pl.multiple_of(q_ref[0] * cols, 128)
    place = place_ref[...]
    aff = aff_ref[...]
    hot = one_hot(place, span)
    full = jnp.concatenate(hot, axis=0).astype(BF16)
    got = got_ref[...].reshape(experts * span, cols)
    back = dot(full, got, 0, 0)
    rows = []
    for e in range(experts):
        tile = got_ref[e, slots:, :128].astype(F32)
        total = jnp.zeros((8, toks), F32)
        for g in range(slots // 8):
            total = total + hot[e][8 * g : 8 * g + 8, :] * tile[:, g : g + 1]
        rows.append(jnp.sum(total, axis=0, keepdims=True))
    term = jnp.concatenate(rows, axis=0)
    named = (place >= 0).astype(F32)
    chosen = named * aff
    total_aff = jnp.sum(chosen, axis=0, keepdims=True)
    weights = chosen / total_aff
    d_chosen = (term - jnp.sum(term * weights, axis=0, keepdims=True)) / total_aff
    d_logit = named * d_chosen * aff * (1.0 - aff)
    d_logits = d_logit.astype(BF16)
    part_out[...] = dot(d_logits, tok_ref[:, pl.ds(start, cols)])
    router_back = dot(d_logit.T.astype(BF16), router_ref[pl.ds(start, cols), :], 1, 1)
    token_out[...] = (back + router_back).astype(BF16)


def per_device(tokens, routing, router_weight, gate_weight, up_weight, down_weight, cotangent):
    groups = lax.axis_size("ep")
    shares = lax.axis_size("tp")
    chips = shares // 2
    toks, width = tokens.shape
    top = routing.shape[1]
    experts = router_weight.shape[1]
    hidden = gate_weight.shape[2]
    capacity = 7 * toks * top // (4 * experts)
    slots = -(-capacity // 8) * 8
    span = slots + 8
    count = groups * slots
    cols = width // shares
    half = width // 2
    wg, wu, wd = gate_weight[0], up_weight[0], down_weight[0]
    q = lax.axis_index("tp").astype(jnp.int32).reshape(1)

    def swap(value, bit):
        return lax.ppermute(value, "tp", [(i, i ^ bit) for i in range(shares)])

    def exchange(value):
        return lax.all_to_all(value, "ep", split_axis=0, concat_axis=0, tiled=True)

    rows_send, aff, place = pl.pallas_call(
        functools.partial(route_kernel, slots),
        out_shape=(
            jax.ShapeDtypeStruct((experts, span, cols), BF16),
            jax.ShapeDtypeStruct((experts, toks), F32),
            jax.ShapeDtypeStruct((experts, toks), F32),
        ),
        in_specs=[SMEM, VMEM, VMEM, VMEM],
        out_specs=(VMEM, VMEM, VMEM),
        compiler_params=params(),
        name="route",
    )(q, tokens, routing, router_weight)
    rows_got = exchange(rows_send)

    cots_send = pl.pallas_call(
        functools.partial(cots_kernel, slots),
        out_shape=jax.ShapeDtypeStruct((experts, slots, half), BF16),
        in_specs=[SMEM, VMEM, VMEM],
        out_specs=VMEM,
        compiler_params=params(),
        cost_estimate=cost(2 * count * toks * half, 2 * count * half),
        name="cots",
    )(q, cotangent, place)
    cots_send, rows_got = lax.optimization_barrier((cots_send, rows_got))
    cots_got = exchange(cots_send)

    own = rows_got[:, :slots].reshape(count, cols)
    scale = rows_got[:, slots:, : slots // 8].transpose(0, 2, 1).reshape(count, 1).astype(F32)
    far = [own] + [swap(own, 2 * j) for j in range(1, chips)]
    x_parts = [part for value in far for part in (value, swap(value, 1))]
    x_all = jnp.stack(x_parts)

    weight_spec = pl.BlockSpec((cols, hidden), lambda r, q: (q[0] ^ r, 0))
    keep_spec = pl.BlockSpec((count, hidden), lambda r, q: (0, 0))
    hid, up_factor, gate_factor = pl.pallas_call(
        gate_up_kernel,
        out_shape=(
            jax.ShapeDtypeStruct((count, hidden), BF16),
            jax.ShapeDtypeStruct((count, hidden), F32),
            jax.ShapeDtypeStruct((count, hidden), F32),
        ),
        grid_spec=pltpu.PrefetchScalarGridSpec(
            num_scalar_prefetch=1,
            grid=(shares,),
            in_specs=[
                pl.BlockSpec((1, count, cols), lambda r, q: (r, 0, 0)),
                weight_spec,
                weight_spec,
            ],
            out_specs=(keep_spec, keep_spec, keep_spec),
            scratch_shapes=[pltpu.VMEM((count, hidden), F32)] * 2,
        ),
        compiler_params=params(),
        cost_estimate=cost(4 * count * width * hidden, 4 * width * hidden),
        name="gate_up",
    )(q, x_all, wg, wu)

    z_own = cots_got.reshape(count, half)
    z_far = swap(z_own, 1)
    back = pl.pallas_call(
        functools.partial(back_kernel, 0),
        out_shape=jax.ShapeDtypeStruct((count, hidden), F32),
        in_specs=[SMEM, VMEM, VMEM],
        out_specs=VMEM,
        compiler_params=params(),
        cost_estimate=cost(2 * count * half * hidden, 2 * half * hidden),
        name="back",
    )(q, z_own, wd)
    gg, gu, odd, term = pl.pallas_call(
        functools.partial(middle_kernel, slots, shares),
        out_shape=(
            jax.ShapeDtypeStruct((count, hidden), BF16),
            jax.ShapeDtypeStruct((count, hidden), BF16),
            jax.ShapeDtypeStruct((chips, groups, span, cols), BF16),
            jax.ShapeDtypeStruct((groups, 8, cols), F32),
        ),
        in_specs=[SMEM] + [VMEM] * 9,
        out_specs=(VMEM, VMEM, VMEM, VMEM),
        compiler_params=params(),
        cost_estimate=cost(4 * count * half * hidden, 4 * half * hidden),
        name="middle",
    )(q, back, z_far, wd, scale, hid, up_factor, gate_factor, wg, wu)
    core_got = swap(odd, 1)
    even = pl.pallas_call(
        functools.partial(even_kernel, slots, shares),
        out_shape=jax.ShapeDtypeStruct((chips, groups, span, cols), F32),
        in_specs=[SMEM] + [VMEM] * 5,
        out_specs=VMEM,
        compiler_params=params(),
        cost_estimate=cost(4 * count * half * hidden, 4 * half * hidden),
        name="even",
    )(q, gg, gu, wg, wu, term)
    chip_send = pl.pallas_call(
        functools.partial(add_core_kernel, slots),
        out_shape=jax.ShapeDtypeStruct((chips - 1, groups, span, cols), BF16),
        in_specs=[VMEM, VMEM],
        out_specs=VMEM,
        compiler_params=params(),
        name="add_core",
    )(even, core_got)
    chip_got = jnp.stack([swap(chip_send[j], 2 * (j + 1)) for j in range(chips - 1)])
    home_send = pl.pallas_call(
        functools.partial(add_chip_kernel, slots),
        out_shape=jax.ShapeDtypeStruct((groups, span, cols), BF16),
        in_specs=[VMEM, VMEM, VMEM],
        out_specs=VMEM,
        compiler_params=params(),
        name="add_chip",
    )(even, core_got, chip_got)
    home_got = exchange(home_send)

    grad_spec = pl.BlockSpec((cols, hidden), lambda r, q: (q[0] ^ r, 0))
    whole_spec = pl.BlockSpec((count, hidden), lambda r, q: (0, 0))
    gate_grad, up_grad, norms = pl.pallas_call(
        grads_kernel,
        out_shape=(
            jax.ShapeDtypeStruct((width, hidden), BF16),
            jax.ShapeDtypeStruct((width, hidden), BF16),
            jax.ShapeDtypeStruct((shares, 2, cols), F32),
        ),
        grid_spec=pltpu.PrefetchScalarGridSpec(
            num_scalar_prefetch=1,
            grid=(shares,),
            in_specs=[
                pl.BlockSpec((1, count, cols), lambda r, q: (r, 0, 0)),
                whole_spec,
                whole_spec,
            ],
            out_specs=(
                grad_spec,
                grad_spec,
                pl.BlockSpec((1, 2, cols), lambda r, q: (q[0] ^ r, 0, 0)),
            ),
        ),
        compiler_params=params(),
        cost_estimate=cost(4 * count * width * hidden, 4 * width * hidden),
        name="grads",
    )(q, x_all, gg, gu)
    down_grad, down_norms = pl.pallas_call(
        down_kernel,
        out_shape=(
            jax.ShapeDtypeStruct((hidden, width), BF16),
            jax.ShapeDtypeStruct((2, 1, hidden), F32),
        ),
        grid_spec=pltpu.PrefetchScalarGridSpec(
            num_scalar_prefetch=1,
            grid=(2,),
            in_specs=[
                pl.BlockSpec((1, count, half), lambda h, q: (h, 0, 0)),
                pl.BlockSpec((count, 1), lambda h, q: (0, 0)),
                pl.BlockSpec((count, hidden), lambda h, q: (0, 0)),
            ],
            out_specs=(
                pl.BlockSpec((hidden, half), lambda h, q: (0, (q[0] % 2) ^ h)),
                pl.BlockSpec((1, 1, hidden), lambda h, q: (h, 0, 0)),
            ),
        ),
        compiler_params=params(),
        cost_estimate=cost(2 * count * width * hidden, 2 * width * hidden),
        name="down",
    )(q, jnp.stack([z_own, z_far]), scale, hid)
    norms = norms.transpose(1, 0, 2).reshape(2, width)
    bit = 1
    while bit < shares:
        norms = norms + swap(norms, bit)
        bit *= 2
    down_rows = (down_norms[0] + down_norms[1]).reshape(1, hidden)

    token_part, router_part = pl.pallas_call(
        functools.partial(home_kernel, slots),
        out_shape=(
            jax.ShapeDtypeStruct((toks, cols), BF16),
            jax.ShapeDtypeStruct((experts, cols), F32),
        ),
        in_specs=[SMEM] + [VMEM] * 5,
        out_specs=(VMEM, VMEM),
        compiler_params=params(),
        name="home",
    )(q, home_got, place, aff, tokens, router_weight)
    parts = exchange(jnp.broadcast_to(router_part, (groups, experts, cols)))
    token_grad = lax.all_gather(token_part, "tp", axis=1, tiled=True)
    router_sum = jnp.sum(parts, axis=0)
    router_grad = router_sum.T
    router_rows = jnp.sum(router_sum * router_sum, axis=0)
    return (
        token_grad,
        router_grad,
        router_rows,
        gate_grad[None],
        up_grad[None],
        down_grad[None],
        norms[0:1],
        norms[1:2],
        down_rows,
    )


def solution(mesh):
    return jax.shard_map(
        per_device,
        mesh=mesh,
        in_specs=(
            P("ep", None),
            P("ep", None),
            P(),
            P("ep", None, "tp"),
            P("ep", None, "tp"),
            P("ep", "tp", None),
            P("ep", None),
        ),
        out_specs=(
            P("ep", None),
            P("tp", None),
            P("tp"),
            P("ep", None, "tp"),
            P("ep", None, "tp"),
            P("ep", "tp", None),
            P("ep", None),
            P("ep", None),
            P("ep", "tp"),
        ),
        check_vma=False,
    )
```

```python
import functools

import jax
import jax.numpy as jnp
from jax import lax
from jax.experimental import pallas as pl
from jax.experimental.pallas import tpu as pltpu
from jax.sharding import PartitionSpec as P


BF16 = jnp.bfloat16
F32 = jnp.float32
VMEM = pl.BlockSpec(memory_space=pltpu.VMEM)
SMEM = pl.BlockSpec(memory_space=pltpu.SMEM)


def dot(a, b, ca=1, cb=0):
    return lax.dot_general(a, b, (((ca,), (cb,)), ((), ())), preferred_element_type=F32)


def params(mib=40):
    return pltpu.CompilerParams(vmem_limit_bytes=mib * 1024 * 1024)


def cost(flops, bytes_accessed):
    return pl.CostEstimate(flops=flops, bytes_accessed=bytes_accessed, transcendentals=0)


def one_hot(place, slots):
    experts, toks = place.shape
    rows = lax.broadcasted_iota(jnp.int32, (slots, toks), 0).astype(F32)
    return [(rows == place[e : e + 1, :]).astype(F32) for e in range(experts)]


def route_kernel(slots, q_ref, tok_ref, routing_ref, router_ref, rows_ref, aff_ref, place_ref):
    toks = tok_ref.shape[0]
    experts = router_ref.shape[0]
    cols = rows_ref.shape[2]
    start = pl.multiple_of(q_ref[0] * cols, 128)
    aff = jax.nn.sigmoid(dot(router_ref[...], tok_ref[...], 1, 1))
    ids = lax.broadcasted_iota(jnp.int32, (experts, toks), 0)
    routed = routing_ref[...]
    named = jnp.zeros((experts, toks), F32)
    for k in range(routed.shape[0]):
        named = named + (ids == routed[k : k + 1, :]).astype(F32)
    before = lax.broadcasted_iota(jnp.int32, (toks, toks), 0)
    after = lax.broadcasted_iota(jnp.int32, (toks, toks), 1)
    earlier = (before < after).astype(F32).astype(BF16)
    position = dot(named.astype(BF16), earlier)
    place = jnp.where(named > 0, position, -1.0)
    chosen = named * aff
    weights = chosen / jnp.sum(chosen, axis=0, keepdims=True)
    aff_ref[...] = aff
    place_ref[...] = place
    hot = one_hot(place, slots)
    full = jnp.concatenate(hot, axis=0).astype(BF16)
    sent = dot(full, tok_ref[:, pl.ds(start, cols)])
    lane = lax.broadcasted_iota(jnp.int32, (8, cols), 1)
    for e in range(experts):
        column = jnp.sum(hot[e] * weights[e : e + 1, :], axis=1, keepdims=True)
        tile = jnp.zeros((8, cols), F32)
        for g in range(slots // 8):
            tile = jnp.where(lane == g, column[8 * g : 8 * g + 8, :], tile)
        block = jnp.concatenate([sent[e * slots : (e + 1) * slots, :], tile], axis=0)
        rows_ref[e] = block.astype(BF16)


def cots_kernel(slots, q_ref, cot_ref, place_ref, cots_ref):
    cols = cots_ref.shape[2]
    start = pl.multiple_of((q_ref[0] % 2) * cols, 128)
    hot = one_hot(place_ref[...], slots)
    full = jnp.concatenate(hot, axis=0).astype(BF16)
    sent = dot(full, cot_ref[:, pl.ds(start, cols)])
    for e in range(len(hot)):
        cots_ref[e] = sent[e * slots : (e + 1) * slots, :].astype(BF16)


def gate_up_kernel(slots, shares, q_ref, *refs):
    x_refs = refs[:shares]
    wg_ref, wu_ref, hid_ref, up_ref, gate_ref, acc_g, acc_u = refs[shares:]
    groups, span, cols = x_refs[0].shape
    for r in range(shares):
        x = x_refs[r][...].reshape(groups * span, cols)
        rows = pl.ds(pl.multiple_of((q_ref[0] ^ r) * cols, 128), cols)
        part_g = dot(x, wg_ref[rows, :])
        part_u = dot(x, wu_ref[rows, :])
        if r == 0:
            acc_g[...] = part_g
            acc_u[...] = part_u
        else:
            acc_g[...] += part_g
            acc_u[...] += part_u
    for e in range(groups):
        scale = scale_column(x_refs[0], e, slots)
        at = slice(e * span, e * span + slots)
        pre_gate = acc_g[at, :]
        pre_up = acc_u[at, :]
        sig = jax.nn.sigmoid(pre_gate)
        act = pre_gate * sig
        hid_ref[e] = (act * pre_up).astype(BF16)
        up_ref[e] = scale * act
        gate_ref[e] = scale * (pre_up * sig * (1.0 + pre_gate * (1.0 - sig)))


def scale_column(x_ref, e, slots):
    tile = x_ref[e, slots:, :128].astype(F32)
    return jnp.concatenate([tile[:, g : g + 1] for g in range(slots // 8)], axis=0)


def back_kernel(half, q_ref, z_ref, wd_ref, back_ref):
    cols = z_ref.shape[1]
    start = pl.multiple_of(((q_ref[0] % 2) ^ half) * cols, 128)
    back_ref[...] = dot(z_ref[...], wd_ref[:, pl.ds(start, cols)], 1, 1)


def slot_parts(q_ref, first, gg, gu, wg_ref, wu_ref, shares):
    cols = wg_ref.shape[0] // shares
    start = pl.multiple_of((q_ref[0] ^ first) * cols, 128)
    return dot(gg, wg_ref[pl.ds(start, cols), :], 1, 1) + dot(
        gu, wu_ref[pl.ds(start, cols), :], 1, 1
    )


def middle_kernel(
    slots, shares, q_ref, back_ref, z_ref, wd_ref, hid_ref, up_ref, gate_ref,
    wg_ref, wu_ref, gg_ref, gu_ref, odd_ref, term_ref,
):
    cols = z_ref.shape[1]
    groups = gg_ref.shape[0]
    start = pl.multiple_of(((q_ref[0] % 2) ^ 1) * cols, 128)
    back = back_ref[...] + dot(z_ref[...], wd_ref[:, pl.ds(start, cols)], 1, 1)
    term = jnp.sum(hid_ref[...].astype(F32) * back, axis=1, keepdims=True)
    gu = back * up_ref[...]
    gg = back * gate_ref[...]
    pad = jnp.zeros((8, gu.shape[1]), F32)
    for e in range(groups):
        at = slice(e * slots, (e + 1) * slots)
        gu_ref[e] = jnp.concatenate([gu[at], pad], axis=0).astype(BF16)
        gg_ref[e] = jnp.concatenate([gg[at], pad], axis=0).astype(BF16)
    lane = lax.broadcasted_iota(jnp.int32, term_ref.shape, 1)
    tile = jnp.zeros(term_ref.shape, F32)
    for c in range(term.shape[0] // 8):
        tile = jnp.where(lane == c, term[8 * c : 8 * c + 8, :], tile)
    term_ref[...] = tile
    gg = gg.astype(BF16)
    gu = gu.astype(BF16)
    for j in range(shares // 2):
        part = slot_parts(q_ref, 2 * j + 1, gg, gu, wg_ref, wu_ref, shares)
        odd_ref[j] = part.astype(BF16)


def even_kernel(slots, shares, q_ref, gg_ref, gu_ref, wg_ref, wu_ref, even_ref):
    groups, span, hidden = gg_ref.shape
    gg = gg_ref[...].reshape(groups * span, hidden)
    gu = gu_ref[...].reshape(groups * span, hidden)
    for j in range(shares // 2):
        part = slot_parts(q_ref, 2 * j, gg, gu, wg_ref, wu_ref, shares)
        for e in range(groups):
            even_ref[j, e] = part[e * span : e * span + slots, :]


def add_core_kernel(own_ref, got_ref, out_ref):
    for j in range(out_ref.shape[0]):
        out_ref[j] = (own_ref[j + 1] + got_ref[j + 1].astype(F32)).astype(BF16)


def add_chip_kernel(own_ref, core_ref, *refs):
    total = own_ref[0] + core_ref[0].astype(F32)
    for chip_ref in refs[:-1]:
        total = total + chip_ref[...].astype(F32)
    refs[-1][...] = total.astype(BF16)


def term_kernel(slots, own_ref, got_ref, out_ref):
    total = (own_ref[...] + got_ref[...]).astype(BF16).astype(F32)
    count = slots // 8
    out_ref[...] = jnp.zeros(out_ref.shape, F32)
    for b in range(out_ref.shape[0]):
        out_ref[b, :, :count] = total[:, b * count : (b + 1) * count]


def grads_kernel(shares, q_ref, *refs):
    x_refs = refs[:shares]
    gg_ref, gu_ref, gate_out, up_out, rows_out = refs[shares:]
    groups, span, cols = x_refs[0].shape
    hidden = gg_ref.shape[2]
    for r in range(shares):

        @pl.when(pl.program_id(0) == r)
        def _(x_ref=x_refs[r]):
            x = x_ref[...].reshape(groups * span, cols)
            gate = dot(x, gg_ref[...].reshape(groups * span, hidden), 0, 0)
            up = dot(x, gu_ref[...].reshape(groups * span, hidden), 0, 0)
            gate_out[...] = gate.astype(BF16)
            up_out[...] = up.astype(BF16)
            rows_out[0, 0:1, :] = square_rows(gate)
            rows_out[0, 1:2, :] = square_rows(up)


def square_rows(value):
    square = value * value
    folded = square[:, :128]
    for at in range(128, value.shape[1], 128):
        folded = folded + square[:, at : at + 128]
    return jnp.sum(folded.T, axis=0, keepdims=True)


def down_kernel(slots, q_ref, own_ref, far_ref, x_ref, hid_ref, down_out, rows_out):
    groups = x_ref.shape[0]
    for h, z_ref in enumerate((own_ref, far_ref)):

        @pl.when(pl.program_id(0) == h)
        def _(z_ref=z_ref):
            scale = jnp.concatenate([scale_column(x_ref, e, slots) for e in range(groups)], axis=0)
            weighted = (scale * z_ref[...].astype(F32)).astype(BF16)
            down = dot(hid_ref[...], weighted, 0, 0)
            down_out[...] = down.astype(BF16)
            rows_out[0] = square_rows(down)


def router_kernel(slots, q_ref, term_ref, place_ref, aff_ref, tok_ref, logit_out, part_out):
    experts, toks = place_ref.shape
    cols = part_out.shape[1]
    start = pl.multiple_of(q_ref[0] * cols, 128)
    place = place_ref[...]
    aff = aff_ref[...]
    hot = one_hot(place, slots)
    rows = []
    for e in range(experts):
        tile = term_ref[e]
        total = jnp.zeros((8, toks), F32)
        for g in range(slots // 8):
            total = total + hot[e][8 * g : 8 * g + 8, :] * tile[:, g : g + 1]
        rows.append(jnp.sum(total, axis=0, keepdims=True))
    term = jnp.concatenate(rows, axis=0)
    named = (place >= 0).astype(F32)
    chosen = named * aff
    total_aff = jnp.sum(chosen, axis=0, keepdims=True)
    weights = chosen / total_aff
    d_chosen = (term - jnp.sum(term * weights, axis=0, keepdims=True)) / total_aff
    d_logit = named * d_chosen * aff * (1.0 - aff)
    logit_out[...] = d_logit
    part_out[...] = dot(d_logit.astype(BF16), tok_ref[:, pl.ds(start, cols)])


def home_kernel(q_ref, got_ref, place_ref, logit_ref, router_ref, token_out):
    cols = got_ref.shape[1]
    start = pl.multiple_of(q_ref[0] * cols, 128)
    experts = place_ref.shape[0]
    full = jnp.concatenate(one_hot(place_ref[...], got_ref.shape[0] // experts), axis=0).astype(BF16)
    back = dot(full, got_ref[...], 0, 0)
    router_back = dot(logit_ref[...].T.astype(BF16), router_ref[:, pl.ds(start, cols)])
    token_out[...] = (back + router_back).astype(BF16)


def assemble_kernel(q_ref, *refs):
    out_ref = refs[-1]
    for r, ref in enumerate(refs[:-1]):
        cols = ref.shape[1]
        out_ref[:, pl.ds(pl.multiple_of((q_ref[0] ^ r) * cols, 128), cols)] = ref[...]


def call(kernel, outs, scalar, *args, flops=0, nbytes=0, scratch=()):
    single = not isinstance(outs, tuple)
    return pl.pallas_call(
        kernel,
        out_shape=outs,
        in_specs=([SMEM] if scalar else []) + [VMEM] * (len(args) - int(scalar)),
        out_specs=VMEM if single else tuple(VMEM for _ in outs),
        scratch_shapes=list(scratch),
        compiler_params=params(),
        cost_estimate=cost(flops, nbytes),
    )(*args)


def shape(*dims, dtype=BF16):
    return jax.ShapeDtypeStruct(dims, dtype)


def per_device(tokens, routing, router_weight, gate_weight, up_weight, down_weight, cotangent):
    return layer(tokens, routing.T, router_weight.T, gate_weight[0], up_weight[0], down_weight[0], cotangent)


def layer(tokens, routing, router, wg, wu, wd, cotangent):
    groups = lax.axis_size("ep")
    shares = lax.axis_size("tp")
    chips = shares // 2
    toks, width = tokens.shape
    top = routing.shape[0]
    experts = router.shape[0]
    hidden = wg.shape[1]
    capacity = 7 * toks * top // (4 * experts)
    slots = -(-capacity // 8) * 8
    span = slots + 8
    count = groups * slots
    cols = width // shares
    half = width // 2
    unit = 2 * count * half * hidden
    q = lax.axis_index("tp").astype(jnp.int32).reshape(1)

    def swap(value, bit, axis="tp"):
        size = lax.axis_size(axis)
        return lax.ppermute(value, axis, [(i, i ^ bit) for i in range(size)])

    def exchange(value):
        return lax.all_to_all(value, "ep", split_axis=0, concat_axis=0, tiled=True)

    def spread(value):
        far = [value] + [swap(value, 2 * j) for j in range(1, chips)]
        return [part for piece in far for part in (piece, swap(piece, 1))]

    rows_send, aff, place = call(
        functools.partial(route_kernel, slots),
        (shape(experts, span, cols), shape(experts, toks, dtype=F32), shape(experts, toks, dtype=F32)),
        True, q, tokens, routing, router,
    )
    rows_got = exchange(rows_send)
    cots_send = call(
        functools.partial(cots_kernel, slots), shape(experts, slots, half),
        True, q, cotangent, place, flops=2 * count * toks * half,
    )
    cots_send, rows_got = lax.optimization_barrier((cots_send, rows_got))
    cots_got = exchange(cots_send)

    x_parts = spread(rows_got)
    hid, up_factor, gate_factor = call(
        functools.partial(gate_up_kernel, slots, shares),
        (shape(groups, slots, hidden), shape(groups, slots, hidden, dtype=F32), shape(groups, slots, hidden, dtype=F32)),
        True, q, *x_parts, wg, wu, flops=4 * unit,
        scratch=[pltpu.VMEM((groups * span, hidden), F32)] * 2,
    )
    hid = hid.reshape(count, hidden)
    up_factor = up_factor.reshape(count, hidden)
    gate_factor = gate_factor.reshape(count, hidden)

    z_own = cots_got.reshape(count, half)
    z_far = swap(z_own, 1)
    back = call(
        functools.partial(back_kernel, 0), shape(count, hidden, dtype=F32),
        True, q, z_own, wd, flops=unit,
    )
    gg, gu, odd, term = call(
        functools.partial(middle_kernel, slots, shares),
        (
            shape(groups, span, hidden),
            shape(groups, span, hidden),
            shape(chips, count, cols),
            shape(8, -(-count // 1024) * 128, dtype=F32),
        ),
        True, q, back, z_far, wd, hid, up_factor, gate_factor, wg, wu, flops=3 * unit,
    )
    term_got = swap(term, 1)
    core_got = swap(odd, 1)
    even = call(
        functools.partial(even_kernel, slots, shares), shape(chips, groups, slots, cols, dtype=F32),
        True, q, gg, gu, wg, wu, flops=2 * unit,
    ).reshape(chips, count, cols)
    term = term + term_got
    bit = 2
    while 2 * bit < shares:
        term = term + swap(term, bit)
        bit *= 2
    term_got = swap(term, bit)
    chip_send = call(add_core_kernel, shape(chips - 1, count, cols), False, even, core_got)
    chip_got = [swap(chip_send[j], 2 * (j + 1)) for j in range(chips - 1)]
    terms = call(
        functools.partial(term_kernel, slots), shape(groups, 8, 128, dtype=F32), False, term, term_got,
    )
    terms = exchange(terms)
    home_send = call(add_chip_kernel, shape(count, cols), False, even, core_got, *chip_got)
    home_got = exchange(home_send.reshape(groups, slots, cols)).reshape(count, cols)

    grad_spec = pl.BlockSpec((cols, hidden), lambda r, q: (q[0] ^ r, 0))
    gate_grad, up_grad, norms = pl.pallas_call(
        functools.partial(grads_kernel, shares),
        out_shape=(shape(width, hidden), shape(width, hidden), shape(shares, 2, cols, dtype=F32)),
        grid_spec=pltpu.PrefetchScalarGridSpec(
            num_scalar_prefetch=1,
            grid=(shares,),
            in_specs=[VMEM] * (shares + 2),
            out_specs=(grad_spec, grad_spec, pl.BlockSpec((1, 2, cols), lambda r, q: (q[0] ^ r, 0, 0))),
        ),
        compiler_params=params(),
        cost_estimate=cost(4 * unit, 0),
        name="grads",
    )(q, *x_parts, gg, gu)
    down_grad, down_norms = pl.pallas_call(
        functools.partial(down_kernel, slots),
        out_shape=(shape(hidden, width), shape(2, 1, hidden, dtype=F32)),
        grid_spec=pltpu.PrefetchScalarGridSpec(
            num_scalar_prefetch=1,
            grid=(2,),
            in_specs=[VMEM] * 4,
            out_specs=(
                pl.BlockSpec((hidden, half), lambda h, q: (0, (q[0] % 2) ^ h)),
                pl.BlockSpec((1, 1, hidden), lambda h, q: (h, 0, 0)),
            ),
        ),
        compiler_params=params(),
        cost_estimate=cost(2 * unit, 0),
        name="down",
    )(q, z_own, z_far, rows_got, hid)
    norms = norms.transpose(1, 0, 2).reshape(2, width)
    bit = 1
    while bit < shares:
        norms = norms + swap(norms, bit)
        bit *= 2
    down_rows = (down_norms[0] + down_norms[1]).reshape(1, hidden)

    d_logits, router_sum = call(
        functools.partial(router_kernel, slots),
        (shape(experts, toks, dtype=F32), shape(experts, cols, dtype=F32)),
        True, q, terms, place, aff, tokens,
    )
    bit = 1
    while bit < groups:
        router_sum = router_sum + swap(router_sum, bit, "ep")
        bit *= 2
    router_rows = jnp.sum(router_sum * router_sum, axis=0)
    token_part = call(home_kernel, shape(toks, cols), True, q, home_got, place, d_logits, router)
    token_grad = call(assemble_kernel, shape(toks, width), True, q, *spread(token_part))
    return (
        token_grad,
        router_sum.T,
        router_rows,
        gate_grad[None],
        up_grad[None],
        down_grad[None],
        norms[0:1],
        norms[1:2],
        down_rows,
    )


def solution(mesh):
    return jax.shard_map(
        per_device,
        mesh=mesh,
        in_specs=(
            P("ep", None),
            P("ep", None),
            P(),
            P("ep", None, "tp"),
            P("ep", None, "tp"),
            P("ep", "tp", None),
            P("ep", None),
        ),
        out_specs=(
            P("ep", None),
            P("tp", None),
            P("tp"),
            P("ep", None, "tp"),
            P("ep", None, "tp"),
            P("ep", "tp", None),
            P("ep", None),
            P("ep", None),
            P("ep", "tp"),
        ),
        check_vma=False,
    )
```

```python
import functools

import jax
import jax.numpy as jnp
from jax import lax
from jax.experimental import pallas as pl
from jax.experimental.pallas import tpu as pltpu
from jax.sharding import PartitionSpec as P


BF16 = jnp.bfloat16
F32 = jnp.float32
VMEM = pl.BlockSpec(memory_space=pltpu.VMEM)
SMEM = pl.BlockSpec(memory_space=pltpu.SMEM)
HBM = pl.BlockSpec(memory_space=pltpu.HBM)


def dot(a, b, ca=1, cb=0):
    return lax.dot_general(a, b, (((ca,), (cb,)), ((), ())), preferred_element_type=F32)


ALONE = 67043328
SHARED = 16 * 1024 * 1024
JOIN = 1
BACK = 1


def params(limit=SHARED):
    return pltpu.CompilerParams(vmem_limit_bytes=limit)


def cost(flops, bytes_accessed):
    return pl.CostEstimate(flops=flops, bytes_accessed=bytes_accessed, transcendentals=0)


def fetch(sems, *pairs):
    copies = [pltpu.make_async_copy(src, dst, sems.at[i]) for i, (src, dst) in enumerate(pairs)]
    for copy in copies:
        copy.start()
    return copies


def one_hot(place, slots):
    experts, toks = place.shape
    rows = lax.broadcasted_iota(jnp.int32, (slots, toks), 0).astype(F32)
    return [(rows == place[e : e + 1, :]).astype(F32) for e in range(experts)]


def route_kernel(
    slots, tok_hbm, routing_hbm, router_hbm, rows_ref, aff_ref, place_ref,
    tok_ref, routing_ref, router_ref, sems,
):
    copies = fetch(sems, (tok_hbm, tok_ref), (routing_hbm, routing_ref), (router_hbm, router_ref))
    toks = tok_ref.shape[0]
    experts = router_ref.shape[0]
    cols = rows_ref.shape[2]
    start = pl.multiple_of(lax.axis_index("tp") * cols, 128)
    for copy in copies:
        copy.wait()
    aff = jax.nn.sigmoid(dot(router_ref[...], tok_ref[...], 1, 1))
    ids = lax.broadcasted_iota(jnp.int32, (experts, toks), 0)
    routed = routing_ref[...]
    named = jnp.zeros((experts, toks), F32)
    for k in range(routed.shape[0]):
        named = named + (ids == routed[k : k + 1, :]).astype(F32)
    before = lax.broadcasted_iota(jnp.int32, (toks, toks), 0)
    after = lax.broadcasted_iota(jnp.int32, (toks, toks), 1)
    earlier = (before < after).astype(F32).astype(BF16)
    position = dot(named.astype(BF16), earlier)
    place = jnp.where(named > 0, position, -1.0)
    chosen = named * aff
    weights = chosen / jnp.sum(chosen, axis=0, keepdims=True)
    aff_ref[...] = aff
    place_ref[...] = place
    hot = one_hot(place, slots)
    full = jnp.concatenate(hot, axis=0).astype(BF16)
    sent = dot(full, tok_ref[:, pl.ds(start, cols)])
    lane = lax.broadcasted_iota(jnp.int32, (8, cols), 1)
    for e in range(experts):
        column = jnp.sum(hot[e] * weights[e : e + 1, :], axis=1, keepdims=True)
        tile = jnp.zeros((8, cols), F32)
        for g in range(slots // 8):
            tile = jnp.where(lane == g, column[8 * g : 8 * g + 8, :], tile)
        block = jnp.concatenate([sent[e * slots : (e + 1) * slots, :], tile], axis=0)
        rows_ref[e] = block.astype(BF16)


def cots_kernel(slots, cot_hbm, place_ref, *refs):
    cot_ref, sems = refs[-2:]
    experts, toks = place_ref.shape
    cols = cot_ref.shape[1]
    start = pl.multiple_of((lax.axis_index("tp") % 2) * cols, 128)
    copies = fetch(sems, (cot_hbm.at[:, pl.ds(start, cols)], cot_ref))
    rows = lax.broadcasted_iota(jnp.int32, (slots, toks), 0).astype(F32)
    hot = [
        (rows == place_ref[pl.ds(lax.axis_index("ep") ^ k, 1), :]).astype(F32) for k in range(experts)
    ]
    full = jnp.concatenate(hot, axis=0).astype(BF16)
    copies[0].wait()
    sent = dot(full, cot_ref[...])
    for k in range(experts):
        refs[k][...] = sent[k * slots : (k + 1) * slots, :].astype(BF16)


def join_kernel(*refs):
    for k, ref in enumerate(refs[:-1]):
        refs[-1][lax.axis_index("ep") ^ k] = ref[...]


def gate_up_kernel(slots, shares, *refs):
    x_refs = refs[:shares]
    wg_ref, wu_ref, hid_ref, up_ref, gate_ref, acc_g, acc_u = refs[shares:]
    groups, span, cols = x_refs[0].shape
    for r in range(shares):
        x = x_refs[r][...].reshape(groups * span, cols)
        rows = pl.ds(pl.multiple_of((lax.axis_index("tp") ^ r) * cols, 128), cols)
        part_g = dot(x, wg_ref[rows, :])
        part_u = dot(x, wu_ref[rows, :])
        if r == 0:
            acc_g[...] = part_g
            acc_u[...] = part_u
        else:
            acc_g[...] += part_g
            acc_u[...] += part_u
    for e in range(groups):
        scale = scale_column(x_refs[0], e, slots)
        at = slice(e * span, e * span + slots)
        pre_gate = acc_g[at, :]
        pre_up = acc_u[at, :]
        sig = jax.nn.sigmoid(pre_gate)
        act = pre_gate * sig
        hid_ref[e] = (act * pre_up).astype(BF16)
        up_ref[e] = scale * act
        gate_ref[e] = scale * (pre_up * sig * (1.0 + pre_gate * (1.0 - sig)))


def scale_column(x_ref, e, slots):
    tile = x_ref[e, slots:, :128].astype(F32)
    return jnp.concatenate([tile[:, g : g + 1] for g in range(slots // 8)], axis=0)


def back_kernel(half, z_ref, wd_ref, back_ref):
    cols = z_ref.shape[1]
    start = pl.multiple_of(((lax.axis_index("tp") % 2) ^ half) * cols, 128)
    back_ref[...] = dot(z_ref[...], wd_ref[:, pl.ds(start, cols)], 1, 1)


def slot_parts(first, gg, gu, wg_ref, wu_ref, shares):
    cols = wg_ref.shape[0] // shares
    start = pl.multiple_of((lax.axis_index("tp") ^ first) * cols, 128)
    return dot(gg, wg_ref[pl.ds(start, cols), :], 1, 1) + dot(
        gu, wu_ref[pl.ds(start, cols), :], 1, 1
    )


def middle_kernel(
    slots, shares, back_ref, z_ref, wd_ref, hid_ref, up_ref, gate_ref,
    wg_ref, wu_ref, gg_ref, gu_ref, home_ref, chip_ref, term_ref,
):
    cols = z_ref.shape[1]
    groups = gg_ref.shape[0]
    start = pl.multiple_of(((lax.axis_index("tp") % 2) ^ 1) * cols, 128)
    back = back_ref[...] + dot(z_ref[...], wd_ref[:, pl.ds(start, cols)], 1, 1)
    term = jnp.sum(hid_ref[...].astype(F32) * back, axis=1, keepdims=True)
    gu = back * up_ref[...]
    gg = back * gate_ref[...]
    pad = jnp.zeros((8, gu.shape[1]), F32)
    for e in range(groups):
        at = slice(e * slots, (e + 1) * slots)
        gu_ref[e] = jnp.concatenate([gu[at], pad], axis=0).astype(BF16)
        gg_ref[e] = jnp.concatenate([gg[at], pad], axis=0).astype(BF16)
    lane = lax.broadcasted_iota(jnp.int32, term_ref.shape, 1)
    tile = jnp.zeros(term_ref.shape, F32)
    for c in range(term.shape[0] // 8):
        tile = jnp.where(lane == c, term[8 * c : 8 * c + 8, :], tile)
    term_ref[...] = tile
    gg = gg.astype(BF16)
    gu = gu.astype(BF16)
    for j in range(shares // 2):
        part = slot_parts(2 * j + 1, gg, gu, wg_ref, wu_ref, shares)
        if j == 0:
            home_ref[...] = part.astype(BF16)
        else:
            chip_ref[j - 1] = part.astype(BF16)


def even_kernel(slots, shares, gg_ref, gu_ref, wg_ref, wu_ref, home_ref, chip_ref):
    groups, span, hidden = gg_ref.shape
    gg = gg_ref[...].reshape(groups * span, hidden)
    gu = gu_ref[...].reshape(groups * span, hidden)
    for j in range(shares // 2):
        part = slot_parts(2 * j, gg, gu, wg_ref, wu_ref, shares)
        for e in range(groups):
            block = part[e * span : e * span + slots, :]
            if j == 0:
                home_ref[e * slots : (e + 1) * slots, :] = block
            else:
                chip_ref[j - 1, e * slots : (e + 1) * slots, :] = block


def add_core_kernel(own_ref, got_ref, out_ref):
    out_ref[...] = (own_ref[...] + got_ref[...].astype(F32)).astype(BF16)


def add_chip_kernel(own_ref, core_ref, *refs):
    total = own_ref[...] + core_ref[...].astype(F32)
    for chip_ref in refs[:-1]:
        total = total + chip_ref[...].astype(F32)
    refs[-1][...] = total.astype(BF16)


def grads_kernel(shares, q_ref, *refs):
    x_refs = refs[:shares]
    gg_ref, gu_ref, gate_out, up_out, rows_out = refs[shares:]
    groups, span, cols = x_refs[0].shape
    hidden = gg_ref.shape[2]
    for r in range(shares):

        @pl.when(pl.program_id(0) == r)
        def _(x_ref=x_refs[r]):
            x = x_ref[...].reshape(groups * span, cols)
            gate = dot(x, gg_ref[...].reshape(groups * span, hidden), 0, 0)
            up = dot(x, gu_ref[...].reshape(groups * span, hidden), 0, 0)
            gate_out[...] = gate.astype(BF16)
            up_out[...] = up.astype(BF16)
            rows_out[0, 0:1, :] = square_rows(gate)
            rows_out[0, 1:2, :] = square_rows(up)


def square_rows(value):
    square = value * value
    folded = square[:, :128]
    for at in range(128, value.shape[1], 128):
        folded = folded + square[:, at : at + 128]
    return jnp.sum(folded.T, axis=0, keepdims=True)


def down_kernel(slots, q_ref, own_ref, far_ref, x_ref, hid_ref, down_out, rows_out):
    groups = x_ref.shape[0]
    for h, z_ref in enumerate((own_ref, far_ref)):

        @pl.when(pl.program_id(0) == h)
        def _(z_ref=z_ref):
            scale = jnp.concatenate([scale_column(x_ref, e, slots) for e in range(groups)], axis=0)
            weighted = (scale * z_ref[...].astype(F32)).astype(BF16)
            down = dot(hid_ref[...], weighted, 0, 0)
            down_out[...] = down.astype(BF16)
            rows_out[0] = square_rows(down)


def router_kernel(slots, term_ref, place_ref, aff_ref, tok_ref, router_ref, base_out, part_out):
    experts, toks = place_ref.shape
    cols = part_out.shape[1]
    start = pl.multiple_of(lax.axis_index("tp") * cols, 128)
    place = place_ref[...]
    aff = aff_ref[...]
    slot = lax.broadcasted_iota(jnp.int32, (slots, toks), 0).astype(F32)
    lanes = term_ref.shape[2]
    own = lax.axis_index("ep")
    row = lax.broadcasted_iota(jnp.int32, (experts, toks), 0)
    term = jnp.zeros((experts, toks), F32)
    for r in range(experts):
        tile = pltpu.roll(term_ref[r], lanes - own * (slots // 8), 1)
        hot = (slot == place_ref[pl.ds(own ^ r, 1), :]).astype(F32)
        total = jnp.zeros((8, toks), F32)
        for g in range(slots // 8):
            total = total + hot[8 * g : 8 * g + 8, :] * tile[:, g : g + 1]
        term = jnp.where(row == (own ^ r), jnp.sum(total, axis=0, keepdims=True), term)
    named = (place >= 0).astype(F32)
    chosen = named * aff
    total_aff = jnp.sum(chosen, axis=0, keepdims=True)
    weights = chosen / total_aff
    d_chosen = (term - jnp.sum(term * weights, axis=0, keepdims=True)) / total_aff
    d_logit = named * d_chosen * aff * (1.0 - aff)
    base_out[...] = dot(d_logit.T.astype(BF16), router_ref[:, pl.ds(start, cols)])
    part_out[...] = dot(d_logit.astype(BF16), tok_ref[:, pl.ds(start, cols)])


def slot_map_kernel(slots, place_ref, hot_ref):
    hot_ref[...] = jnp.concatenate(one_hot(place_ref[...], slots), axis=0).astype(BF16)


def home_kernel(got_hbm, hot_hbm, base_hbm, token_out, got_ref, hot_ref, base_ref, sems):
    copies = fetch(sems, (hot_hbm, hot_ref), (got_hbm, got_ref), (base_hbm, base_ref))
    for copy in copies:
        copy.wait()
    token_out[...] = (dot(hot_ref[...], got_ref[...], 0, 0) + base_ref[...]).astype(BF16)


def assemble_kernel(*refs):
    out_hbm, sems = refs[-2:]
    pairs = []
    for r, ref in enumerate(refs[:-2]):
        cols = ref.shape[1]
        start = pl.multiple_of((lax.axis_index("tp") ^ r) * cols, 128)
        pairs.append((ref, out_hbm.at[:, pl.ds(start, cols)]))
    for copy in fetch(sems, *pairs):
        copy.wait()


def call(kernel, outs, scalar, *args, flops=0, nbytes=0, scratch=(), hbm=(), out_hbm=False, limit=SHARED):
    single = not isinstance(outs, tuple)
    ins = [HBM if i in hbm else VMEM for i in range(int(scalar), len(args))]
    out = HBM if out_hbm else VMEM
    return pl.pallas_call(
        kernel,
        out_shape=outs,
        in_specs=([SMEM] if scalar else []) + ins,
        out_specs=out if single else tuple(out for _ in outs),
        scratch_shapes=list(scratch),
        compiler_params=params(limit),
        cost_estimate=cost(flops, nbytes),
    )(*args)


DMAS = pltpu.SemaphoreType.DMA


def buffer(*dims, dtype=BF16):
    return pltpu.VMEM(dims, dtype)


def shape(*dims, dtype=BF16):
    return jax.ShapeDtypeStruct(dims, dtype)


def per_device(tokens, routing, router_weight, gate_weight, up_weight, down_weight, cotangent):
    return layer(tokens, routing.T, router_weight.T, gate_weight[0], up_weight[0], down_weight[0], cotangent)


def layer(tokens, routing, router, wg, wu, wd, cotangent):
    groups = lax.axis_size("ep")
    shares = lax.axis_size("tp")
    chips = shares // 2
    toks, width = tokens.shape
    top = routing.shape[0]
    experts = router.shape[0]
    hidden = wg.shape[1]
    capacity = 7 * toks * top // (4 * experts)
    slots = -(-capacity // 8) * 8
    span = slots + 8
    count = groups * slots
    cols = width // shares
    half = width // 2
    unit = 2 * count * half * hidden
    q = lax.axis_index("tp").astype(jnp.int32).reshape(1)

    def swap(value, bit, axis="tp"):
        size = lax.axis_size(axis)
        return lax.ppermute(value, axis, [(i, i ^ bit) for i in range(size)])

    def exchange(value):
        return lax.all_to_all(value, "ep", split_axis=0, concat_axis=0, tiled=True)

    def spread(value):
        far = [value] + [swap(value, 2 * j) for j in range(1, chips)]
        return [part for piece in far for part in (piece, swap(piece, 1))]

    rows_send, aff, place = call(
        functools.partial(route_kernel, slots),
        (shape(experts, span, cols), shape(experts, toks, dtype=F32), shape(experts, toks, dtype=F32)),
        False, tokens, routing, router, hbm=(0, 1, 2), limit=ALONE,
        scratch=[buffer(toks, width), buffer(top, toks, dtype=jnp.int32), buffer(experts, width), DMAS((3,))],
    )
    rows_got = exchange(rows_send)
    pieces = call(
        functools.partial(cots_kernel, slots), tuple(shape(slots, half) for _ in range(experts)),
        False, cotangent, place, flops=2 * count * toks * half, hbm=(0,), limit=ALONE,
        scratch=[buffer(toks, half), DMAS((1,))],
    )
    pieces = list(pieces)
    for k in range(experts - 1, 0, -1):
        pieces[k] = swap(pieces[k], k, "ep")

    hot = call(functools.partial(slot_map_kernel, slots), shape(count, toks), False, place)

    x_parts = spread(rows_got)
    hid, up_factor, gate_factor = call(
        functools.partial(gate_up_kernel, slots, shares),
        (shape(groups, slots, hidden), shape(groups, slots, hidden, dtype=F32), shape(groups, slots, hidden, dtype=F32)),
        False, *x_parts, wg, wu, flops=4 * unit,
        scratch=[pltpu.VMEM((groups * span, hidden), F32)] * 2,
    )
    hid = hid.reshape(count, hidden)
    up_factor = up_factor.reshape(count, hidden)
    gate_factor = gate_factor.reshape(count, hidden)

    z_own = call(join_kernel, shape(groups, slots, half), False, *pieces, flops=JOIN * unit).reshape(count, half)
    z_far = swap(z_own, 1)
    back = call(
        functools.partial(back_kernel, 0), shape(count, hidden, dtype=F32),
        False, z_own, wd, flops=BACK * unit,
    )
    gg, gu, odd_home, odd_chip, term = call(
        functools.partial(middle_kernel, slots, shares),
        (
            shape(groups, span, hidden),
            shape(groups, span, hidden),
            shape(count, cols),
            shape(chips - 1, count, cols),
            shape(8, -(-count // 1024) * 128, dtype=F32),
        ),
        False, back, z_far, wd, hid, up_factor, gate_factor, wg, wu, flops=3 * unit,
    )
    term_got = swap(term, 1)
    core_chip = swap(odd_chip, 1)
    core_home = swap(odd_home, 1)
    even_home, even_chip = call(
        functools.partial(even_kernel, slots, shares),
        (shape(count, cols, dtype=F32), shape(chips - 1, count, cols, dtype=F32)),
        False, gg, gu, wg, wu, flops=2 * unit,
    )
    term = term + term_got
    bit = 2
    while 2 * bit < shares:
        term = term + swap(term, bit)
        bit *= 2
    term_got = swap(term, bit)
    chip_send = call(add_core_kernel, shape(chips - 1, count, cols), False, even_chip, core_chip)
    chip_got = [swap(chip_send[j], 2 * (j + 1)) for j in range(chips - 1)]
    terms = (term + term_got).astype(BF16).astype(F32)[None]
    bit = 1
    while bit < groups:
        terms = jnp.concatenate([terms, swap(terms, bit, "ep")], axis=0)
        bit *= 2
    home_send = call(add_chip_kernel, shape(count, cols), False, even_home, core_home, *chip_got)
    home_got = exchange(home_send.reshape(groups, slots, cols)).reshape(count, cols)

    grad_spec = pl.BlockSpec((cols, hidden), lambda r, q: (q[0] ^ r, 0))
    gate_grad, up_grad, norms = pl.pallas_call(
        functools.partial(grads_kernel, shares),
        out_shape=(shape(width, hidden), shape(width, hidden), shape(shares, 2, cols, dtype=F32)),
        grid_spec=pltpu.PrefetchScalarGridSpec(
            num_scalar_prefetch=1,
            grid=(shares,),
            in_specs=[VMEM] * (shares + 2),
            out_specs=(grad_spec, grad_spec, pl.BlockSpec((1, 2, cols), lambda r, q: (q[0] ^ r, 0, 0))),
        ),
        compiler_params=params(),
        cost_estimate=cost(4 * unit, 0),
        name="grads",
    )(q, *x_parts, gg, gu)
    down_grad, down_norms = pl.pallas_call(
        functools.partial(down_kernel, slots),
        out_shape=(shape(hidden, width), shape(2, 1, hidden, dtype=F32)),
        grid_spec=pltpu.PrefetchScalarGridSpec(
            num_scalar_prefetch=1,
            grid=(2,),
            in_specs=[VMEM] * 4,
            out_specs=(
                pl.BlockSpec((hidden, half), lambda h, q: (0, (q[0] % 2) ^ h)),
                pl.BlockSpec((1, 1, hidden), lambda h, q: (h, 0, 0)),
            ),
        ),
        compiler_params=params(),
        cost_estimate=cost(2 * unit, 0),
        name="down",
    )(q, z_own, z_far, rows_got, hid)
    norms = norms.transpose(1, 0, 2).reshape(2, width)
    norms = spread(norms)
    while len(norms) > 1:
        norms = [a + b for a, b in zip(norms[::2], norms[1::2])]
    norms = norms[0]
    down_rows = (down_norms[0] + down_norms[1]).reshape(1, hidden)

    token_base, router_sum = call(
        functools.partial(router_kernel, slots),
        (shape(toks, cols, dtype=F32), shape(experts, cols, dtype=F32)),
        False, terms, place, aff, tokens, router,
    )
    bit = 1
    while bit < groups:
        router_sum = router_sum + swap(router_sum, bit, "ep")
        bit *= 2
    router_rows = jnp.sum(router_sum * router_sum, axis=0)
    token_part = call(
        home_kernel, shape(toks, cols), False, home_got, hot, token_base, hbm=(0, 1, 2), limit=ALONE,
        scratch=[buffer(count, cols), buffer(count, toks), buffer(toks, cols, dtype=F32), DMAS((3,))],
    )
    token_grad = call(
        assemble_kernel, shape(toks, width), False, *spread(token_part), out_hbm=True, scratch=[DMAS((shares,))],
    )
    return (
        token_grad,
        router_sum.T,
        router_rows,
        gate_grad[None],
        up_grad[None],
        down_grad[None],
        norms[0:1],
        norms[1:2],
        down_rows,
    )


def solution(mesh):
    return jax.shard_map(
        per_device,
        mesh=mesh,
        in_specs=(
            P("ep", None),
            P("ep", None),
            P(),
            P("ep", None, "tp"),
            P("ep", None, "tp"),
            P("ep", "tp", None),
            P("ep", None),
        ),
        out_specs=(
            P("ep", None),
            P("tp", None),
            P("tp"),
            P("ep", None, "tp"),
            P("ep", None, "tp"),
            P("ep", "tp", None),
            P("ep", None),
            P("ep", None),
            P("ep", "tp"),
        ),
        check_vma=False,
    )
```

```python
import functools

import jax
import jax.numpy as jnp
from jax import lax
from jax.experimental import pallas as pl
from jax.experimental.pallas import tpu as pltpu
from jax.sharding import PartitionSpec as P


BF16 = jnp.bfloat16
F32 = jnp.float32
VMEM = pl.BlockSpec(memory_space=pltpu.VMEM)
SMEM = pl.BlockSpec(memory_space=pltpu.SMEM)
HBM = pl.BlockSpec(memory_space=pltpu.HBM)


def dot(a, b, ca=1, cb=0):
    return lax.dot_general(a, b, (((ca,), (cb,)), ((), ())), preferred_element_type=F32)


ALONE = 67043328
SHARED = 16 * 1024 * 1024
COEF_LANE = 64


def params(limit=SHARED):
    return pltpu.CompilerParams(vmem_limit_bytes=limit)


def cost(flops, bytes_accessed):
    return pl.CostEstimate(flops=flops, bytes_accessed=bytes_accessed, transcendentals=0)


def fetch(sems, *pairs):
    copies = [pltpu.make_async_copy(src, dst, sems.at[i]) for i, (src, dst) in enumerate(pairs)]
    for copy in copies:
        copy.start()
    return copies


def one_hot(place, slots):
    experts, toks = place.shape
    rows = lax.broadcasted_iota(jnp.int32, (slots, toks), 0).astype(F32)
    return [(rows == place[e : e + 1, :]).astype(F32) for e in range(experts)]


def route_kernel(
    slots, tok_hbm, routing_hbm, router_hbm, rows_ref, aff_ref, place_ref,
    tok_ref, routing_ref, router_ref, sems,
):
    copies = fetch(sems, (tok_hbm, tok_ref), (routing_hbm, routing_ref), (router_hbm, router_ref))
    toks = tok_ref.shape[0]
    experts = router_ref.shape[0]
    cols = rows_ref.shape[2]
    start = pl.multiple_of(lax.axis_index("tp") * cols, 128)
    for copy in copies:
        copy.wait()
    aff = jax.nn.sigmoid(dot(router_ref[...], tok_ref[...], 1, 1))
    ids = lax.broadcasted_iota(jnp.int32, (experts, toks), 0)
    routed = routing_ref[...]
    named = jnp.zeros((experts, toks), F32)
    for k in range(routed.shape[0]):
        named = named + (ids == routed[k : k + 1, :]).astype(F32)
    before = lax.broadcasted_iota(jnp.int32, (toks, toks), 0)
    after = lax.broadcasted_iota(jnp.int32, (toks, toks), 1)
    earlier = (before < after).astype(F32).astype(BF16)
    position = dot(named.astype(BF16), earlier)
    place = jnp.where(named > 0, position, -1.0)
    chosen = named * aff
    weights = chosen / jnp.sum(chosen, axis=0, keepdims=True)
    aff_ref[...] = aff
    place_ref[...] = place
    hot = one_hot(place, slots)
    full = jnp.concatenate(hot, axis=0).astype(BF16)
    sent = dot(full, tok_ref[:, pl.ds(start, cols)])
    slope = named * aff * (1.0 - aff) / jnp.sum(chosen, axis=0, keepdims=True)
    row = lax.broadcasted_iota(jnp.int32, (experts, toks), 0)
    lane = lax.broadcasted_iota(jnp.int32, (8, 128), 1)
    for e in range(experts):
        own = weights[e : e + 1, :]
        others = jnp.sum(jnp.where(row == e, 0.0, weights), axis=0, keepdims=True)
        factors = jnp.where(row == e, others, -own) * slope
        table = jnp.concatenate([factors, own, jnp.zeros((127 - experts, toks), F32)], axis=0)
        values = dot(hot[e].astype(BF16), table.astype(BF16), 1, 1)
        tile = jnp.zeros((8, 128), F32)
        for g in range(slots // 8):
            part = values[8 * g : 8 * g + 8, :]
            tile = jnp.where(lane == g, part[:, experts : experts + 1], tile)
            shift = COEF_LANE + g * experts
            moved = pltpu.roll(part, shift, 1)
            tile = jnp.where((lane >= shift) & (lane < shift + experts), moved, tile)
        if cols > 128:
            tile = jnp.concatenate([tile, jnp.zeros((8, cols - 128), F32)], axis=1)
        block = jnp.concatenate([sent[e * slots : (e + 1) * slots, :], tile], axis=0)
        rows_ref[e] = block.astype(BF16)


def cots_kernel(slots, cot_hbm, place_ref, *refs):
    cot_ref, sems = refs[-2:]
    experts, toks = place_ref.shape
    cols = cot_ref.shape[1]
    start = pl.multiple_of((lax.axis_index("tp") % 2) * cols, 128)
    copies = fetch(sems, (cot_hbm.at[:, pl.ds(start, cols)], cot_ref))
    rows = lax.broadcasted_iota(jnp.int32, (slots, toks), 0).astype(F32)
    hot = [
        (rows == place_ref[pl.ds(lax.axis_index("ep") ^ k, 1), :]).astype(F32) for k in range(experts)
    ]
    full = jnp.concatenate(hot, axis=0).astype(BF16)
    copies[0].wait()
    sent = dot(full, cot_ref[...])
    for k in range(experts):
        refs[k][...] = sent[k * slots : (k + 1) * slots, :].astype(BF16)


def half_of(groups):
    me = lax.axis_index("ep")
    return me // (groups // 2), me % (groups // 2)


def join_kernel(*refs):
    out_ref = refs[-1]
    count = out_ref.shape[0]
    _, place = half_of(2 * count)
    for k in range(count):
        out_ref[place ^ k] = refs[k][...]


def gate_up_kernel(slots, shares, *refs):
    x_refs = refs[:shares]
    wg_ref, wu_ref, hid_ref, up_ref, gate_ref, acc_g, acc_u = refs[shares:]
    groups, span, cols = x_refs[0].shape
    for r in range(shares):
        x = x_refs[r][...].reshape(groups * span, cols)
        rows = pl.ds(pl.multiple_of((lax.axis_index("tp") ^ r) * cols, 128), cols)
        part_g = dot(x, wg_ref[rows, :])
        part_u = dot(x, wu_ref[rows, :])
        if r == 0:
            acc_g[...] = part_g
            acc_u[...] = part_u
        else:
            acc_g[...] += part_g
            acc_u[...] += part_u
    for e in range(groups):
        scale = scale_column(x_refs[0], e, slots)
        at = slice(e * span, e * span + slots)
        pre_gate = acc_g[at, :]
        pre_up = acc_u[at, :]
        sig = jax.nn.sigmoid(pre_gate)
        act = pre_gate * sig
        hid_ref[e] = (act * pre_up).astype(BF16)
        up_ref[e] = scale * act
        gate_ref[e] = scale * (pre_up * sig * (1.0 + pre_gate * (1.0 - sig)))


def scale_column(x_ref, e, slots):
    tile = x_ref[e, slots:, :128].astype(F32)
    return jnp.concatenate([tile[:, g : g + 1] for g in range(slots // 8)], axis=0)


def back_kernel(groups, near_hbm, far_hbm, wd_hbm, back_ref):
    cols = near_hbm.shape[1]
    side, _ = half_of(groups)
    start = pl.multiple_of((lax.axis_index("tp") % 2) * cols, 128)
    wd = wd_hbm[:, pl.ds(start, cols)]
    back_ref[side] = dot(near_hbm[...], wd, 1, 1)
    back_ref[1 - side] = dot(far_hbm[...], wd, 1, 1)


def slot_parts(first, gg, gu, wg_ref, wu_ref, shares):
    cols = wg_ref.shape[0] // shares
    start = pl.multiple_of((lax.axis_index("tp") ^ first) * cols, 128)
    return dot(gg, wg_ref[pl.ds(start, cols), :], 1, 1) + dot(
        gu, wu_ref[pl.ds(start, cols), :], 1, 1
    )


def middle_kernel(
    slots, shares, back_ref, near_ref, far_ref, wd_ref, hid_ref, up_ref, gate_ref, wg_ref, wu_ref,
    g_ref, home_ref, chip_ref, term_ref, sum_ref,
):
    cols = near_ref.shape[1]
    groups = g_ref.shape[0]
    side, _ = half_of(groups)
    start = pl.multiple_of(((lax.axis_index("tp") % 2) ^ 1) * cols, 128)
    wd = wd_ref[:, pl.ds(start, cols)]
    sum_ref[side] = back_ref[side] + dot(near_ref[...], wd, 1, 1)
    sum_ref[1 - side] = back_ref[1 - side] + dot(far_ref[...], wd, 1, 1)
    back = sum_ref[...].reshape(hid_ref.shape)
    hidden = hid_ref.shape[1]
    term = jnp.sum(hid_ref[...].astype(F32) * back, axis=1, keepdims=True)
    gu = back * up_ref[...]
    gg = back * gate_ref[...]
    pad = jnp.zeros((8, gu.shape[1]), F32)
    for e in range(groups):
        at = slice(e * slots, (e + 1) * slots)
        g_ref[e, :, :hidden] = jnp.concatenate([gg[at], pad], axis=0).astype(BF16)
        g_ref[e, :, hidden:] = jnp.concatenate([gu[at], pad], axis=0).astype(BF16)
    lane = lax.broadcasted_iota(jnp.int32, term_ref.shape, 1)
    tile = jnp.zeros(term_ref.shape, F32)
    for c in range(term.shape[0] // 8):
        tile = jnp.where(lane == c, term[8 * c : 8 * c + 8, :], tile)
    term_ref[...] = tile
    gg = gg.astype(BF16)
    gu = gu.astype(BF16)
    for j in range(shares // 2):
        part = slot_parts(2 * j + 1, gg, gu, wg_ref, wu_ref, shares)
        if j == 0:
            home_ref[...] = part.astype(BF16)
        else:
            chip_ref[j - 1] = part.astype(BF16)


def even_kernel(slots, shares, g_ref, wg_ref, wu_ref, home_ref, chip_ref):
    groups, span, double = g_ref.shape
    both = g_ref[...].reshape(groups * span, double)
    gg, gu = both[:, : double // 2], both[:, double // 2 :]
    for j in range(shares // 2):
        part = slot_parts(2 * j, gg, gu, wg_ref, wu_ref, shares)
        for e in range(groups):
            block = part[e * span : e * span + slots, :]
            if j == 0:
                home_ref[e * slots : (e + 1) * slots, :] = block
            else:
                chip_ref[j - 1, e * slots : (e + 1) * slots, :] = block


def add_core_kernel(own_ref, got_ref, out_ref):
    out_ref[...] = (own_ref[...] + got_ref[...].astype(F32)).astype(BF16)


def add_chip_kernel(own_ref, core_ref, tile_ref, *refs):
    total = own_ref[...] + core_ref[...].astype(F32)
    for chip_ref in refs[:-1]:
        total = total + chip_ref[...].astype(F32)
    out_ref = refs[-1]
    slots = out_ref.shape[1] - 8
    for e in range(out_ref.shape[0]):
        block = jnp.concatenate([total[e * slots : (e + 1) * slots], tile_ref[e]], axis=0)
        out_ref[e] = block.astype(BF16)


def grads_kernel(shares, q_ref, *refs):
    x_refs = refs[:shares]
    g_ref, gate_out, up_out, rows_out = refs[shares:]
    groups, span, cols = x_refs[0].shape
    double = g_ref.shape[2]
    for r in range(shares):

        @pl.when(pl.program_id(0) == r)
        def _(x_ref=x_refs[r]):
            x = x_ref[...].reshape(groups * span, cols)
            both = dot(x, g_ref[...].reshape(groups * span, double), 0, 0)
            gate, up = both[:, : double // 2], both[:, double // 2 :]
            gate_out[...] = gate.astype(BF16)
            up_out[...] = up.astype(BF16)
            rows_out[0, 0:1, :] = square_rows(gate)
            rows_out[0, 1:2, :] = square_rows(up)


def square_rows(value):
    square = value * value
    folded = square[:, :128]
    for at in range(128, value.shape[1], 128):
        folded = folded + square[:, at : at + 128]
    return jnp.sum(folded.T, axis=0, keepdims=True)


def down_kernel(slots, q_ref, *refs):
    x_ref, hid_ref, down_out, rows_out = refs[4:]
    groups = x_ref.shape[0]
    side, _ = half_of(groups)
    for h in range(2):

        @pl.when(pl.program_id(0) == h)
        def _(pair=refs[2 * h : 2 * h + 2]):
            down = 0.0
            for z_ref, at in zip(pair, (side, 1 - side)):
                scale = [scale_column(x_ref, at * (groups // 2) + e, slots) for e in range(groups // 2)]
                scale = jnp.concatenate(scale, axis=0)
                weighted = (scale * z_ref[...].astype(F32)).astype(BF16)
                down = down + dot(hid_ref[at], weighted, 0, 0)
            down_out[...] = down.astype(BF16)
            rows_out[0] = square_rows(down)


def add_kernel(a_ref, b_ref, out_ref):
    out_ref[...] = a_ref[...] + b_ref[...]


def terms_kernel(slots, a_ref, b_ref, x_ref, tile_ref, part_ref):
    term = (a_ref[...] + b_ref[...]).astype(BF16).astype(F32)
    groups, span, cols = x_ref.shape
    experts = part_ref.shape[0]
    count = slots // 8
    lanes = term.shape[1]
    lane = lax.broadcasted_iota(jnp.int32, (8, lanes), 1)
    blocks = []
    for b in range(groups):
        moved = pltpu.roll(term, (lanes - b * count) % lanes, 1)
        moved = jnp.where(lane < count, moved, 0.0)[:, :128]
        if cols > 128:
            moved = jnp.concatenate([moved, jnp.zeros((8, cols - 128), F32)], axis=1)
        tile_ref[b] = moved
        spare = x_ref[b, slots:, :128].astype(F32)
        for g in range(count):
            factors = pltpu.roll(spare, 128 - COEF_LANE - g * experts, 1)
            c = b * count + g
            blocks.append(term[:, c : c + 1] * factors)
        blocks.append(jnp.zeros((8, 128), F32))
    table = jnp.concatenate(blocks, axis=0)
    table = jnp.where(lax.broadcasted_iota(jnp.int32, table.shape, 1) < experts, table, 0.0)
    high = table.astype(BF16)
    low = (table - high.astype(F32)).astype(BF16)
    x = x_ref[...].reshape(groups * span, cols)
    part_ref[...] = (dot(high, x, 0, 0) + dot(low, x, 0, 0))[:experts]


def last_sum_kernel(a_ref, b_ref, sum_ref, rows_ref):
    total = a_ref[...] + b_ref[...]
    sum_ref[...] = total
    rows_ref[...] = jnp.sum(total * total, axis=0, keepdims=True)


def slot_map_kernel(slots, place_ref, hot_ref):
    hot_ref[...] = jnp.concatenate(one_hot(place_ref[...], slots), axis=0).astype(BF16)


def home_kernel(
    slots, got_hbm, hot_hbm, place_hbm, aff_hbm, router_hbm, token_out,
    got_ref, hot_ref, place_ref, aff_ref, router_ref, sems,
):
    experts, span, cols = got_ref.shape
    toks = place_ref.shape[1]
    start = pl.multiple_of(lax.axis_index("tp") * cols, 128)
    copies = fetch(
        sems, (place_hbm, place_ref), (aff_hbm, aff_ref), (got_hbm, got_ref),
        (router_hbm.at[:, pl.ds(start, cols)], router_ref), (hot_hbm, hot_ref),
    )
    for copy in copies:
        copy.wait()
    place = place_ref[...]
    aff = aff_ref[...]
    back = dot(hot_ref[...], got_ref[...].reshape(experts * span, cols), 0, 0)
    hot = one_hot(place, slots)
    rows = []
    for e in range(experts):
        tile = got_ref[e, slots:, :128].astype(F32)
        total = jnp.zeros((8, toks), F32)
        for g in range(slots // 8):
            total = total + hot[e][8 * g : 8 * g + 8, :] * tile[:, g : g + 1]
        rows.append(jnp.sum(total, axis=0, keepdims=True))
    term = jnp.concatenate(rows, axis=0)
    named = (place >= 0).astype(F32)
    chosen = named * aff
    total_aff = jnp.sum(chosen, axis=0, keepdims=True)
    weights = chosen / total_aff
    d_chosen = (term - jnp.sum(term * weights, axis=0, keepdims=True)) / total_aff
    d_logit = named * d_chosen * aff * (1.0 - aff)
    token_out[...] = (back + dot(d_logit.T.astype(BF16), router_ref[...])).astype(BF16)


def assemble_kernel(*refs):
    out_hbm, sems = refs[-2:]
    pairs = []
    for r, ref in enumerate(refs[:-2]):
        cols = ref.shape[1]
        start = pl.multiple_of((lax.axis_index("tp") ^ r) * cols, 128)
        pairs.append((ref, out_hbm.at[:, pl.ds(start, cols)]))
    for copy in fetch(sems, *pairs):
        copy.wait()


def call(kernel, outs, scalar, *args, flops=0, nbytes=0, scratch=(), hbm=(), out_hbm=False, limit=SHARED):
    single = not isinstance(outs, tuple)
    ins = [HBM if i in hbm else VMEM for i in range(int(scalar), len(args))]
    out = HBM if out_hbm else VMEM
    return pl.pallas_call(
        kernel,
        out_shape=outs,
        in_specs=([SMEM] if scalar else []) + ins,
        out_specs=out if single else tuple(out for _ in outs),
        scratch_shapes=list(scratch),
        compiler_params=params(limit),
        cost_estimate=cost(flops, nbytes),
    )(*args)


DMAS = pltpu.SemaphoreType.DMA


def buffer(*dims, dtype=BF16):
    return pltpu.VMEM(dims, dtype)


def shape(*dims, dtype=BF16):
    return jax.ShapeDtypeStruct(dims, dtype)


def per_device(tokens, routing, router_weight, gate_weight, up_weight, down_weight, cotangent):
    return layer(tokens, routing.T, router_weight.T, gate_weight[0], up_weight[0], down_weight[0], cotangent)


def layer(tokens, routing, router, wg, wu, wd, cotangent):
    groups = lax.axis_size("ep")
    shares = lax.axis_size("tp")
    chips = shares // 2
    toks, width = tokens.shape
    top = routing.shape[0]
    experts = router.shape[0]
    hidden = wg.shape[1]
    capacity = 7 * toks * top // (4 * experts)
    slots = -(-capacity // 8) * 8
    span = slots + 8
    count = groups * slots
    cols = width // shares
    half = width // 2
    unit = 2 * count * half * hidden
    q = lax.axis_index("tp").astype(jnp.int32).reshape(1)

    def swap(value, bit, axis="tp"):
        size = lax.axis_size(axis)
        return lax.ppermute(value, axis, [(i, i ^ bit) for i in range(size)])

    def exchange(value):
        return lax.all_to_all(value, "ep", split_axis=0, concat_axis=0, tiled=True)

    def spread(value):
        far = [value] + [swap(value, 2 * j) for j in range(1, chips)]
        return [part for piece in far for part in (piece, swap(piece, 1))]

    rows_send, aff, place = call(
        functools.partial(route_kernel, slots),
        (shape(experts, span, cols), shape(experts, toks, dtype=F32), shape(experts, toks, dtype=F32)),
        False, tokens, routing, router, hbm=(0, 1, 2), limit=ALONE,
        scratch=[buffer(toks, width), buffer(top, toks, dtype=jnp.int32), buffer(experts, width), DMAS((3,))],
    )
    rows_got = exchange(rows_send)
    pieces = call(
        functools.partial(cots_kernel, slots), tuple(shape(slots, half) for _ in range(experts)),
        False, cotangent, place, flops=2 * count * toks * half, hbm=(0,), limit=ALONE,
        scratch=[buffer(toks, half), DMAS((1,))],
    )
    pieces = list(pieces)
    for k in range(experts - 1, 0, -1):
        pieces[k] = swap(pieces[k], k, "ep")

    hot = call(functools.partial(slot_map_kernel, span), shape(groups * span, toks), False, place)

    x_parts = spread(rows_got)
    hid, up_factor, gate_factor = call(
        functools.partial(gate_up_kernel, slots, shares),
        (shape(groups, slots, hidden), shape(groups, slots, hidden, dtype=F32), shape(groups, slots, hidden, dtype=F32)),
        False, *x_parts, wg, wu, flops=4 * unit,
        scratch=[pltpu.VMEM((groups * span, hidden), F32)] * 2,
    )
    hid = hid.reshape(count, hidden)
    up_factor = up_factor.reshape(count, hidden)
    gate_factor = gate_factor.reshape(count, hidden)

    side = groups // 2
    near = call(join_kernel, shape(side, slots, half), False, *pieces[:side], wg, wu).reshape(count // 2, half)
    near_got = swap(near, 1)
    far = call(join_kernel, shape(side, slots, half), False, *pieces[side:]).reshape(count // 2, half)
    far_got = swap(far, 1)
    back = call(
        functools.partial(back_kernel, groups), shape(2, count // 2, hidden, dtype=F32),
        False, near, far, wd, flops=unit,
    )
    g, odd_home, odd_chip, term = call(
        functools.partial(middle_kernel, slots, shares),
        (
            shape(groups, span, 2 * hidden),
            shape(count, cols),
            shape(chips - 1, count, cols),
            shape(8, -(-count // 1024) * 128, dtype=F32),
        ),
        False, back, near_got, far_got, wd, hid, up_factor, gate_factor, wg, wu, flops=3 * unit,
        scratch=[buffer(2, count // 2, hidden, dtype=F32)],
    )
    term_got = swap(term, 1)
    core_chip = swap(odd_chip, 1)
    core_home = swap(odd_home, 1)
    even_home, even_chip = call(
        functools.partial(even_kernel, slots, shares),
        (shape(count, cols, dtype=F32), shape(chips - 1, count, cols, dtype=F32)),
        False, g, wg, wu, flops=2 * unit,
    )

    def add(a, b, kernel=add_kernel, lead=()):
        return call(kernel, shape(*lead, *a.shape, dtype=F32), False, a, b)

    term = add(term, term_got)
    bit = 2
    while 2 * bit < shares:
        term = add(term, swap(term, bit))
        bit *= 2
    term_got = swap(term, bit)
    chip_send = call(add_core_kernel, shape(chips - 1, count, cols), False, even_chip, core_chip)
    chip_got = [swap(chip_send[j], 2 * (j + 1)) for j in range(chips - 1)]
    tiles, router_sum = call(
        functools.partial(terms_kernel, slots),
        (shape(groups, 8, cols, dtype=F32), shape(experts, cols, dtype=F32)),
        False, term, term_got, rows_got,
    )
    bit = 1
    while 2 * bit < groups:
        router_got = swap(router_sum, bit, "ep")
        router_sum = add(router_sum, router_got)
        bit *= 2
    router_got = swap(router_sum, bit, "ep")
    router_sum, router_rows = call(
        last_sum_kernel, (shape(experts, cols, dtype=F32), shape(1, cols, dtype=F32)),
        False, router_sum, router_got,
    )
    router_rows = router_rows.reshape(cols)
    home_send = call(add_chip_kernel, shape(groups, span, cols), False, even_home, core_home, tiles, *chip_got)
    home_got = exchange(home_send)

    grad_spec = pl.BlockSpec((cols, hidden), lambda r, q: (q[0] ^ r, 0))
    gate_grad, up_grad, norms = pl.pallas_call(
        functools.partial(grads_kernel, shares),
        out_shape=(shape(width, hidden), shape(width, hidden), shape(shares, 2, cols, dtype=F32)),
        grid_spec=pltpu.PrefetchScalarGridSpec(
            num_scalar_prefetch=1,
            grid=(shares,),
            in_specs=[VMEM] * (shares + 1),
            out_specs=(grad_spec, grad_spec, pl.BlockSpec((1, 2, cols), lambda r, q: (q[0] ^ r, 0, 0))),
        ),
        compiler_params=params(),
        cost_estimate=cost(4 * unit, 0),
        name="grads",
    )(q, *x_parts, g)
    down_grad, down_norms = pl.pallas_call(
        functools.partial(down_kernel, slots),
        out_shape=(shape(hidden, width), shape(2, 1, hidden, dtype=F32)),
        grid_spec=pltpu.PrefetchScalarGridSpec(
            num_scalar_prefetch=1,
            grid=(2,),
            in_specs=[VMEM] * 6,
            out_specs=(
                pl.BlockSpec((hidden, half), lambda h, q: (0, (q[0] % 2) ^ h)),
                pl.BlockSpec((1, 1, hidden), lambda h, q: (h, 0, 0)),
            ),
        ),
        compiler_params=params(ALONE),
        cost_estimate=cost(2 * unit, 0),
        name="down",
    )(q, near, far, near_got, far_got, rows_got, hid.reshape(2, count // 2, hidden))
    norms = norms.transpose(1, 0, 2).reshape(2, width)
    norms = spread(norms)
    while len(norms) > 1:
        norms = [a + b for a, b in zip(norms[::2], norms[1::2])]
    norms = norms[0]
    down_rows = (down_norms[0] + down_norms[1]).reshape(1, hidden)

    token_part = call(
        functools.partial(home_kernel, slots), shape(toks, cols),
        False, home_got, hot, place, aff, router, hbm=range(5), limit=ALONE,
        scratch=[
            buffer(groups, span, cols),
            buffer(groups * span, toks),
            buffer(experts, toks, dtype=F32),
            buffer(experts, toks, dtype=F32),
            buffer(experts, cols),
            DMAS((5,)),
        ],
    )
    token_grad = call(
        assemble_kernel, shape(toks, width), False, *spread(token_part), out_hbm=True, scratch=[DMAS((shares,))],
    )
    return (
        token_grad,
        router_sum.T,
        router_rows,
        gate_grad[None],
        up_grad[None],
        down_grad[None],
        norms[0:1],
        norms[1:2],
        down_rows,
    )


def solution(mesh):
    return jax.shard_map(
        per_device,
        mesh=mesh,
        in_specs=(
            P("ep", None),
            P("ep", None),
            P(),
            P("ep", None, "tp"),
            P("ep", None, "tp"),
            P("ep", "tp", None),
            P("ep", None),
        ),
        out_specs=(
            P("ep", None),
            P("tp", None),
            P("tp"),
            P("ep", None, "tp"),
            P("ep", None, "tp"),
            P("ep", "tp", None),
            P("ep", None),
            P("ep", None),
            P("ep", "tp"),
        ),
        check_vma=False,
    )
```

```python
import functools

import jax
import jax.numpy as jnp
from jax import lax
from jax.experimental import pallas as pl
from jax.experimental.pallas import tpu as pltpu
from jax.sharding import PartitionSpec as P


BF16 = jnp.bfloat16
F32 = jnp.float32
VMEM = pl.BlockSpec(memory_space=pltpu.VMEM)
SMEM = pl.BlockSpec(memory_space=pltpu.SMEM)
HBM = pl.BlockSpec(memory_space=pltpu.HBM)


def dot(a, b, ca=1, cb=0):
    return lax.dot_general(a, b, (((ca,), (cb,)), ((), ())), preferred_element_type=F32)


ALONE = 67043328
SHARED = 16 * 1024 * 1024
GRADS_ROOM = 4500000
COEF_LANE = 64


def params(limit=SHARED):
    return pltpu.CompilerParams(vmem_limit_bytes=limit)


def cost(flops, bytes_accessed):
    return pl.CostEstimate(flops=flops, bytes_accessed=bytes_accessed, transcendentals=0)


def fetch(sems, *pairs):
    copies = [pltpu.make_async_copy(src, dst, sems.at[i]) for i, (src, dst) in enumerate(pairs)]
    for copy in copies:
        copy.start()
    return copies


def one_hot(place, slots):
    experts, toks = place.shape
    rows = lax.broadcasted_iota(jnp.int32, (slots, toks), 0).astype(F32)
    return [(rows == place[e : e + 1, :]).astype(F32) for e in range(experts)]


def route_kernel(
    slots, tok_hbm, routing_hbm, router_hbm, rows_ref, aff_ref, place_ref,
    tok_ref, routing_ref, router_ref, sems,
):
    copies = fetch(sems, (tok_hbm, tok_ref), (routing_hbm, routing_ref), (router_hbm, router_ref))
    toks = tok_ref.shape[0]
    experts = router_ref.shape[0]
    cols = rows_ref.shape[2]
    start = pl.multiple_of(lax.axis_index("tp") * cols, 128)
    for copy in copies:
        copy.wait()
    aff = jax.nn.sigmoid(dot(router_ref[...], tok_ref[...], 1, 1))
    ids = lax.broadcasted_iota(jnp.int32, (experts, toks), 0)
    routed = routing_ref[...]
    named = jnp.zeros((experts, toks), F32)
    for k in range(routed.shape[0]):
        named = named + (ids == routed[k : k + 1, :]).astype(F32)
    before = lax.broadcasted_iota(jnp.int32, (toks, toks), 0)
    after = lax.broadcasted_iota(jnp.int32, (toks, toks), 1)
    earlier = (before < after).astype(F32).astype(BF16)
    position = dot(named.astype(BF16), earlier)
    place = jnp.where(named > 0, position, -1.0)
    chosen = named * aff
    weights = chosen / jnp.sum(chosen, axis=0, keepdims=True)
    aff_ref[...] = aff
    place_ref[...] = place
    hot = one_hot(place, slots)
    full = jnp.concatenate(hot, axis=0).astype(BF16)
    sent = dot(full, tok_ref[:, pl.ds(start, cols)])
    slope = named * aff * (1.0 - aff) / jnp.sum(chosen, axis=0, keepdims=True)
    row = lax.broadcasted_iota(jnp.int32, (experts, toks), 0)
    lane = lax.broadcasted_iota(jnp.int32, (8, 128), 1)
    for e in range(experts):
        own = weights[e : e + 1, :]
        others = jnp.sum(jnp.where(row == e, 0.0, weights), axis=0, keepdims=True)
        factors = jnp.where(row == e, others, -own) * slope
        table = jnp.concatenate([factors, own, jnp.zeros((127 - experts, toks), F32)], axis=0)
        values = dot(hot[e].astype(BF16), table.astype(BF16), 1, 1)
        tile = jnp.zeros((8, 128), F32)
        for g in range(slots // 8):
            part = values[8 * g : 8 * g + 8, :]
            tile = jnp.where(lane == g, part[:, experts : experts + 1], tile)
            shift = COEF_LANE + g * experts
            moved = pltpu.roll(part, shift, 1)
            tile = jnp.where((lane >= shift) & (lane < shift + experts), moved, tile)
        if cols > 128:
            tile = jnp.concatenate([tile, jnp.zeros((8, cols - 128), F32)], axis=1)
        block = jnp.concatenate([sent[e * slots : (e + 1) * slots, :], tile], axis=0)
        rows_ref[e] = block.astype(BF16)


def cots_kernel(slots, cot_hbm, place_ref, *refs):
    cot_ref, sems = refs[-2:]
    experts, toks = place_ref.shape
    cols = cot_ref.shape[1]
    start = pl.multiple_of((lax.axis_index("tp") % 2) * cols, 128)
    copies = fetch(sems, (cot_hbm.at[:, pl.ds(start, cols)], cot_ref))
    rows = lax.broadcasted_iota(jnp.int32, (slots, toks), 0).astype(F32)
    hot = [
        (rows == place_ref[pl.ds(lax.axis_index("ep") ^ k, 1), :]).astype(F32) for k in range(experts)
    ]
    full = jnp.concatenate(hot, axis=0).astype(BF16)
    copies[0].wait()
    sent = dot(full, cot_ref[...])
    for k in range(experts):
        refs[k][...] = sent[k * slots : (k + 1) * slots, :].astype(BF16)


def half_of(groups):
    me = lax.axis_index("ep")
    return me // (groups // 2), me % (groups // 2)


def join_kernel(*refs):
    out_ref = refs[-1]
    count = out_ref.shape[0]
    _, place = half_of(2 * count)
    for k in range(count):
        out_ref[place ^ k] = refs[k][...]


def add_parts(tokens_of, x_refs, wg_ref, wu_ref, acc_g, acc_u, fresh):
    groups, span, cols = x_refs[0].shape
    for r, x_ref in zip(tokens_of, x_refs):
        x = x_ref[...].reshape(groups * span, cols)
        rows = pl.ds(pl.multiple_of((lax.axis_index("tp") ^ r) * cols, 128), cols)
        part_g = dot(x, wg_ref[rows, :])
        part_u = dot(x, wu_ref[rows, :])
        acc_g[...] = part_g if fresh else acc_g[...] + part_g
        acc_u[...] = part_u if fresh else acc_u[...] + part_u
        fresh = False


def first_parts_kernel(which, *refs):
    count = len(which)
    add_parts(which, refs[:count], *refs[count:], True)


def more_parts_kernel(which, got_g, got_u, *refs):
    count = len(which)
    acc_g, acc_u = refs[-2:]
    acc_g[...] = got_g[...]
    acc_u[...] = got_u[...]
    add_parts(which, refs[:count], *refs[count:], False)


def gate_up_kernel(slots, which, got_g, got_u, own_ref, *refs):
    count = len(which)
    wg_ref, wu_ref, hid_ref, up_ref, gate_ref, acc_g, acc_u = refs[count:]
    groups, span, _ = own_ref.shape
    acc_g[...] = got_g[...]
    acc_u[...] = got_u[...]
    add_parts(which, refs[:count], wg_ref, wu_ref, acc_g, acc_u, False)
    for e in range(groups):
        scale = scale_column(own_ref, e, slots)
        at = slice(e * span, e * span + slots)
        pre_gate = acc_g[at, :]
        pre_up = acc_u[at, :]
        sig = jax.nn.sigmoid(pre_gate)
        act = pre_gate * sig
        hid_ref[e] = (act * pre_up).astype(BF16)
        up_ref[e] = scale * act
        gate_ref[e] = scale * (pre_up * sig * (1.0 + pre_gate * (1.0 - sig)))


def scale_column(x_ref, e, slots):
    tile = x_ref[e, slots:, :128].astype(F32)
    return jnp.concatenate([tile[:, g : g + 1] for g in range(slots // 8)], axis=0)


def back_kernel(groups, near_hbm, far_hbm, wd_hbm, back_ref):
    cols = near_hbm.shape[1]
    side, _ = half_of(groups)
    start = pl.multiple_of((lax.axis_index("tp") % 2) * cols, 128)
    wd = wd_hbm[:, pl.ds(start, cols)]
    back_ref[side] = dot(near_hbm[...], wd, 1, 1)
    back_ref[1 - side] = dot(far_hbm[...], wd, 1, 1)


def slot_parts(first, gg, gu, wg_ref, wu_ref, shares):
    cols = wg_ref.shape[0] // shares
    start = pl.multiple_of((lax.axis_index("tp") ^ first) * cols, 128)
    return dot(gg, wg_ref[pl.ds(start, cols), :], 1, 1) + dot(
        gu, wu_ref[pl.ds(start, cols), :], 1, 1
    )


def middle_kernel(
    slots, shares, back_ref, near_ref, far_ref, wd_ref, hid_ref, up_ref, gate_ref, wg_ref, wu_ref,
    g_ref, home_ref, chip_ref, term_ref, sum_ref,
):
    cols = near_ref.shape[1]
    groups = g_ref.shape[0]
    side, _ = half_of(groups)
    start = pl.multiple_of(((lax.axis_index("tp") % 2) ^ 1) * cols, 128)
    wd = wd_ref[:, pl.ds(start, cols)]
    sum_ref[side] = back_ref[side] + dot(near_ref[...], wd, 1, 1)
    sum_ref[1 - side] = back_ref[1 - side] + dot(far_ref[...], wd, 1, 1)
    back = sum_ref[...].reshape(hid_ref.shape)
    hidden = hid_ref.shape[1]
    term = jnp.sum(hid_ref[...].astype(F32) * back, axis=1, keepdims=True)
    gu = back * up_ref[...]
    gg = back * gate_ref[...]
    pad = jnp.zeros((8, gu.shape[1]), F32)
    for e in range(groups):
        at = slice(e * slots, (e + 1) * slots)
        g_ref[e, :, :hidden] = jnp.concatenate([gg[at], pad], axis=0).astype(BF16)
        g_ref[e, :, hidden:] = jnp.concatenate([gu[at], pad], axis=0).astype(BF16)
    lane = lax.broadcasted_iota(jnp.int32, term_ref.shape, 1)
    tile = jnp.zeros(term_ref.shape, F32)
    for c in range(term.shape[0] // 8):
        tile = jnp.where(lane == c, term[8 * c : 8 * c + 8, :], tile)
    term_ref[...] = tile
    gg = gg.astype(BF16)
    gu = gu.astype(BF16)
    for j in range(shares // 2):
        part = slot_parts(2 * j + 1, gg, gu, wg_ref, wu_ref, shares)
        if j == 0:
            home_ref[...] = part.astype(BF16)
        else:
            chip_ref[j - 1] = part.astype(BF16)


def even_kernel(slots, shares, g_ref, wg_ref, wu_ref, home_ref, chip_ref):
    groups, span, double = g_ref.shape
    both = g_ref[...].reshape(groups * span, double)
    gg, gu = both[:, : double // 2], both[:, double // 2 :]
    for j in range(shares // 2):
        part = slot_parts(2 * j, gg, gu, wg_ref, wu_ref, shares)
        for e in range(groups):
            block = part[e * span : e * span + slots, :]
            if j == 0:
                home_ref[e * slots : (e + 1) * slots, :] = block
            else:
                chip_ref[j - 1, e * slots : (e + 1) * slots, :] = block


def add_core_kernel(own_ref, got_ref, out_ref):
    out_ref[...] = (own_ref[...] + got_ref[...].astype(F32)).astype(BF16)


def add_chip_kernel(own_ref, core_ref, tile_ref, *refs):
    total = own_ref[...] + core_ref[...].astype(F32)
    for chip_ref in refs[:-1]:
        total = total + chip_ref[...].astype(F32)
    out_ref = refs[-1]
    slots = out_ref.shape[1] - 8
    for e in range(out_ref.shape[0]):
        block = jnp.concatenate([total[e * slots : (e + 1) * slots], tile_ref[e]], axis=0)
        out_ref[e] = block.astype(BF16)


def grads_kernel(shares, q_ref, *refs):
    x_refs = refs[:shares]
    g_ref, gate_out, up_out, rows_out = refs[shares:]
    groups, span, cols = x_refs[0].shape
    double = g_ref.shape[2]
    for r in range(shares):

        @pl.when(pl.program_id(0) == r)
        def _(x_ref=x_refs[r]):
            x = x_ref[...].reshape(groups * span, cols)
            both = dot(x, g_ref[...].reshape(groups * span, double), 0, 0)
            gate, up = both[:, : double // 2], both[:, double // 2 :]
            gate_out[...] = gate.astype(BF16)
            up_out[...] = up.astype(BF16)
            rows_out[0, 0:1, :] = square_rows(gate)
            rows_out[0, 1:2, :] = square_rows(up)


def square_rows(value):
    square = value * value
    folded = square[:, :128]
    for at in range(128, value.shape[1], 128):
        folded = folded + square[:, at : at + 128]
    return jnp.sum(folded.T, axis=0, keepdims=True)


def down_kernel(slots, q_ref, *refs):
    x_ref, hid_ref, down_out, rows_out = refs[4:]
    groups = x_ref.shape[0]
    side, _ = half_of(groups)
    for h in range(2):

        @pl.when(pl.program_id(0) == h)
        def _(pair=refs[2 * h : 2 * h + 2]):
            down = 0.0
            for z_ref, at in zip(pair, (side, 1 - side)):
                scale = [scale_column(x_ref, at * (groups // 2) + e, slots) for e in range(groups // 2)]
                scale = jnp.concatenate(scale, axis=0)
                weighted = (scale * z_ref[...].astype(F32)).astype(BF16)
                down = down + dot(hid_ref[at], weighted, 0, 0)
            down_out[...] = down.astype(BF16)
            if h == 0:
                rows_out[...] = square_rows(down)
            else:
                rows_out[...] += square_rows(down)


def add_kernel(a_ref, b_ref, out_ref):
    out_ref[...] = a_ref[...] + b_ref[...]


def terms_kernel(slots, a_ref, b_ref, x_ref, tile_ref, part_ref):
    term = (a_ref[...] + b_ref[...]).astype(BF16).astype(F32)
    groups, span, cols = x_ref.shape
    experts = part_ref.shape[0]
    count = slots // 8
    lanes = term.shape[1]
    lane = lax.broadcasted_iota(jnp.int32, (8, lanes), 1)
    blocks = []
    for b in range(groups):
        moved = pltpu.roll(term, (lanes - b * count) % lanes, 1)
        moved = jnp.where(lane < count, moved, 0.0)[:, :128]
        if cols > 128:
            moved = jnp.concatenate([moved, jnp.zeros((8, cols - 128), F32)], axis=1)
        tile_ref[b] = moved
        spare = x_ref[b, slots:, :128].astype(F32)
        for g in range(count):
            factors = pltpu.roll(spare, 128 - COEF_LANE - g * experts, 1)
            c = b * count + g
            blocks.append(term[:, c : c + 1] * factors)
        blocks.append(jnp.zeros((8, 128), F32))
    table = jnp.concatenate(blocks, axis=0)
    table = jnp.where(lax.broadcasted_iota(jnp.int32, table.shape, 1) < experts, table, 0.0)
    high = table.astype(BF16)
    low = (table - high.astype(F32)).astype(BF16)
    x = x_ref[...].reshape(groups * span, cols)
    part_ref[...] = (dot(high, x, 0, 0) + dot(low, x, 0, 0))[:experts]


def last_sum_kernel(a_ref, b_ref, sum_ref, rows_ref):
    total = a_ref[...] + b_ref[...]
    sum_ref[...] = total
    rows_ref[...] = jnp.sum(total * total, axis=0, keepdims=True)


def slot_map_kernel(slots, place_ref, hot_ref):
    hot_ref[...] = jnp.concatenate(one_hot(place_ref[...], slots), axis=0).astype(BF16)


def home_kernel(
    slots, got_hbm, hot_hbm, place_hbm, aff_hbm, router_hbm, token_out, whole_hbm,
    got_ref, hot_ref, place_ref, aff_ref, router_ref, own_ref, sems,
):
    experts, span, cols = got_ref.shape
    toks = place_ref.shape[1]
    start = pl.multiple_of(lax.axis_index("tp") * cols, 128)
    copies = fetch(
        sems, (place_hbm, place_ref), (aff_hbm, aff_ref), (got_hbm, got_ref),
        (router_hbm.at[:, pl.ds(start, cols)], router_ref), (hot_hbm, hot_ref),
    )
    for copy in copies:
        copy.wait()
    place = place_ref[...]
    aff = aff_ref[...]
    back = dot(hot_ref[...], got_ref[...].reshape(experts * span, cols), 0, 0)
    hot = one_hot(place, slots)
    rows = []
    for e in range(experts):
        tile = got_ref[e, slots:, :128].astype(F32)
        total = jnp.zeros((8, toks), F32)
        for g in range(slots // 8):
            total = total + hot[e][8 * g : 8 * g + 8, :] * tile[:, g : g + 1]
        rows.append(jnp.sum(total, axis=0, keepdims=True))
    term = jnp.concatenate(rows, axis=0)
    named = (place >= 0).astype(F32)
    chosen = named * aff
    total_aff = jnp.sum(chosen, axis=0, keepdims=True)
    weights = chosen / total_aff
    d_chosen = (term - jnp.sum(term * weights, axis=0, keepdims=True)) / total_aff
    d_logit = named * d_chosen * aff * (1.0 - aff)
    own_ref[...] = (back + dot(d_logit.T.astype(BF16), router_ref[...])).astype(BF16)
    copies = fetch(sems, (own_ref, token_out), (own_ref, whole_hbm.at[:, pl.ds(start, cols)]))
    for copy in copies:
        copy.wait()


def assemble_kernel(*refs):
    out_hbm, sems = refs[-2:]
    pairs = []
    for r, ref in enumerate(refs[1:-2]):
        cols = ref.shape[1]
        start = pl.multiple_of((lax.axis_index("tp") ^ (r + 1)) * cols, 128)
        pairs.append((ref, out_hbm.at[:, pl.ds(start, cols)]))
    for copy in fetch(sems, *pairs):
        copy.wait()


def call(kernel, outs, scalar, *args, flops=0, nbytes=0, scratch=(), hbm=(), out_hbm=False, limit=SHARED):
    single = not isinstance(outs, tuple)
    ins = [HBM if i in hbm else VMEM for i in range(int(scalar), len(args))]
    out = HBM if out_hbm else VMEM
    return pl.pallas_call(
        kernel,
        out_shape=outs,
        in_specs=([SMEM] if scalar else []) + ins,
        out_specs=out if single else tuple(out for _ in outs),
        scratch_shapes=list(scratch),
        compiler_params=params(limit),
        cost_estimate=cost(flops, nbytes),
    )(*args)


DMAS = pltpu.SemaphoreType.DMA


def buffer(*dims, dtype=BF16):
    return pltpu.VMEM(dims, dtype)


def shape(*dims, dtype=BF16):
    return jax.ShapeDtypeStruct(dims, dtype)


def per_device(tokens, routing, router_weight, gate_weight, up_weight, down_weight, cotangent):
    return layer(tokens, routing.T, router_weight.T, gate_weight[0], up_weight[0], down_weight[0], cotangent)


def layer(tokens, routing, router, wg, wu, wd, cotangent):
    groups = lax.axis_size("ep")
    shares = lax.axis_size("tp")
    chips = shares // 2
    toks, width = tokens.shape
    top = routing.shape[0]
    experts = router.shape[0]
    hidden = wg.shape[1]
    capacity = 7 * toks * top // (4 * experts)
    slots = -(-capacity // 8) * 8
    span = slots + 8
    count = groups * slots
    cols = width // shares
    half = width // 2
    unit = 2 * count * half * hidden
    q = lax.axis_index("tp").astype(jnp.int32).reshape(1)

    def swap(value, bit, axis="tp"):
        size = lax.axis_size(axis)
        return lax.ppermute(value, axis, [(i, i ^ bit) for i in range(size)])

    def exchange(value):
        return lax.all_to_all(value, "ep", split_axis=0, concat_axis=0, tiled=True)

    def spread(value):
        far = [value] + [swap(value, 2 * j) for j in range(1, chips)]
        return [part for piece in far for part in (piece, swap(piece, 1))]

    rows_send, aff, place = call(
        functools.partial(route_kernel, slots),
        (shape(experts, span, cols), shape(experts, toks, dtype=F32), shape(experts, toks, dtype=F32)),
        False, tokens, routing, router, hbm=(0, 1, 2), limit=ALONE,
        scratch=[buffer(toks, width), buffer(top, toks, dtype=jnp.int32), buffer(experts, width), DMAS((3,))],
    )
    rows_got = exchange(rows_send)
    pieces = call(
        functools.partial(cots_kernel, slots), tuple(shape(slots, half) for _ in range(experts)),
        False, cotangent, place, flops=2 * count * toks * half, hbm=(0,), limit=ALONE,
        scratch=[buffer(toks, half), DMAS((1,))],
    )
    pieces = list(pieces)
    for k in range(experts - 1, 0, -1):
        pieces[k] = swap(pieces[k], k, "ep")

    hot = call(functools.partial(slot_map_kernel, span), shape(groups * span, toks), False, place)

    x_parts = spread(rows_got)
    sums = tuple(shape(groups * span, hidden, dtype=F32) for _ in range(2))
    chip_parts, core_parts = list(range(2, shares, 2)), list(range(3, shares, 2))
    pre = call(
        functools.partial(first_parts_kernel, (0, 1)), sums,
        False, *x_parts[:2], wg, wu, flops=unit,
    )
    pre = call(
        functools.partial(more_parts_kernel, chip_parts), sums,
        False, *pre, *[x_parts[r] for r in chip_parts], wg, wu, flops=unit,
    )
    hid, up_factor, gate_factor = call(
        functools.partial(gate_up_kernel, slots, core_parts),
        (shape(groups, slots, hidden), shape(groups, slots, hidden, dtype=F32), shape(groups, slots, hidden, dtype=F32)),
        False, *pre, x_parts[0], *[x_parts[r] for r in core_parts], wg, wu, flops=2 * unit,
        scratch=[pltpu.VMEM((groups * span, hidden), F32)] * 2,
    )
    hid = hid.reshape(count, hidden)
    up_factor = up_factor.reshape(count, hidden)
    gate_factor = gate_factor.reshape(count, hidden)

    side = groups // 2
    near = call(
        join_kernel, shape(side, slots, half), False, *pieces[:side],
    ).reshape(count // 2, half)
    near_got = swap(near, 1)
    far = call(
        join_kernel, shape(side, slots, half), False, *pieces[side:],
    ).reshape(count // 2, half)
    far_got = swap(far, 1)
    back = call(
        functools.partial(back_kernel, groups), shape(2, count // 2, hidden, dtype=F32),
        False, near, far, wd, flops=unit,
    )
    g, odd_home, odd_chip, term = call(
        functools.partial(middle_kernel, slots, shares),
        (
            shape(groups, span, 2 * hidden),
            shape(count, cols),
            shape(chips - 1, count, cols),
            shape(8, -(-count // 1024) * 128, dtype=F32),
        ),
        False, back, near_got, far_got, wd, hid, up_factor, gate_factor, wg, wu, flops=3 * unit,
        scratch=[buffer(2, count // 2, hidden, dtype=F32)],
    )
    term_got = swap(term, 1)
    core_chip = swap(odd_chip, 1)
    core_home = swap(odd_home, 1)
    even_home, even_chip = call(
        functools.partial(even_kernel, slots, shares),
        (shape(count, cols, dtype=F32), shape(chips - 1, count, cols, dtype=F32)),
        False, g, wg, wu, flops=2 * unit,
    )

    def add(a, b, kernel=add_kernel, lead=()):
        return call(kernel, shape(*lead, *a.shape, dtype=F32), False, a, b)

    term = add(term, term_got)
    bit = 2
    while 2 * bit < shares:
        term = add(term, swap(term, bit))
        bit *= 2
    term_got = swap(term, bit)
    chip_send = call(add_core_kernel, shape(chips - 1, count, cols), False, even_chip, core_chip)
    chip_got = [swap(chip_send[j], 2 * (j + 1)) for j in range(chips - 1)]
    tiles, router_sum = call(
        functools.partial(terms_kernel, slots),
        (shape(groups, 8, cols, dtype=F32), shape(experts, cols, dtype=F32)),
        False, term, term_got, rows_got,
    )
    bit = 1
    while 2 * bit < groups:
        router_got = swap(router_sum, bit, "ep")
        router_sum = add(router_sum, router_got)
        bit *= 2
    router_got = swap(router_sum, bit, "ep")
    router_sum, router_rows = call(
        last_sum_kernel, (shape(experts, cols, dtype=F32), shape(1, cols, dtype=F32)),
        False, router_sum, router_got,
    )
    router_rows = router_rows.reshape(cols)
    home_send = call(
        add_chip_kernel, shape(groups, span, cols), False, even_home, core_home, tiles, *chip_got,
    )
    home_got = exchange(home_send)

    grad_spec = pl.BlockSpec((cols, hidden), lambda r, q: (q[0] ^ r, 0))
    gate_grad, up_grad, norms = pl.pallas_call(
        functools.partial(grads_kernel, shares),
        out_shape=(shape(width, hidden), shape(width, hidden), shape(shares, 2, cols, dtype=F32)),
        grid_spec=pltpu.PrefetchScalarGridSpec(
            num_scalar_prefetch=1,
            grid=(shares,),
            in_specs=[VMEM] * (shares + 1),
            out_specs=(grad_spec, grad_spec, pl.BlockSpec((1, 2, cols), lambda r, q: (q[0] ^ r, 0, 0))),
        ),
        compiler_params=params(ALONE - GRADS_ROOM),
        cost_estimate=cost(4 * unit, 0),
        name="grads",
    )(q, *x_parts, g)
    down_grad, down_rows = pl.pallas_call(
        functools.partial(down_kernel, slots),
        out_shape=(shape(hidden, width), shape(1, hidden, dtype=F32)),
        grid_spec=pltpu.PrefetchScalarGridSpec(
            num_scalar_prefetch=1,
            grid=(2,),
            in_specs=[VMEM] * 6,
            out_specs=(
                pl.BlockSpec((hidden, half), lambda h, q: (0, (q[0] % 2) ^ h)),
                pl.BlockSpec((1, hidden), lambda h, q: (0, 0)),
            ),
        ),
        compiler_params=params(ALONE),
        cost_estimate=cost(2 * unit, 0),
        name="down",
    )(q, near, far, near_got, far_got, rows_got, hid.reshape(2, count // 2, hidden))
    norms = norms.transpose(1, 0, 2).reshape(2, width)
    norms = spread(norms)
    while len(norms) > 1:
        norms = [a + b for a, b in zip(norms[::2], norms[1::2])]
    norms = norms[0]

    token_part, token_grad = call(
        functools.partial(home_kernel, slots), (shape(toks, cols), shape(toks, width)),
        False, home_got, hot, place, aff, router, hbm=range(5), limit=ALONE, out_hbm=True,
        scratch=[
            buffer(groups, span, cols),
            buffer(groups * span, toks),
            buffer(experts, toks, dtype=F32),
            buffer(experts, toks, dtype=F32),
            buffer(experts, cols),
            buffer(toks, cols),
            DMAS((5,)),
        ],
    )
    token_parts = spread(token_part)[1:]
    token_grad = pl.pallas_call(
        assemble_kernel,
        out_shape=shape(toks, width),
        in_specs=[HBM] + [VMEM] * (shares - 1),
        out_specs=HBM,
        scratch_shapes=[DMAS((shares - 1,))],
        input_output_aliases={0: 0},
        compiler_params=params(),
        name="assemble",
    )(token_grad, *token_parts)
    return (
        token_grad,
        router_sum.T,
        router_rows,
        gate_grad[None],
        up_grad[None],
        down_grad[None],
        norms[0:1],
        norms[1:2],
        down_rows,
    )


def solution(mesh):
    return jax.shard_map(
        per_device,
        mesh=mesh,
        in_specs=(
            P("ep", None),
            P("ep", None),
            P(),
            P("ep", None, "tp"),
            P("ep", None, "tp"),
            P("ep", "tp", None),
            P("ep", None),
        ),
        out_specs=(
            P("ep", None),
            P("tp", None),
            P("tp"),
            P("ep", None, "tp"),
            P("ep", None, "tp"),
            P("ep", "tp", None),
            P("ep", None),
            P("ep", None),
            P("ep", "tp"),
        ),
        check_vma=False,
    )
```

```python
import functools

import jax
import jax.numpy as jnp
from jax import lax
from jax.experimental import pallas as pl
from jax.experimental.pallas import tpu as pltpu
from jax.sharding import PartitionSpec as P


BF16 = jnp.bfloat16
F32 = jnp.float32
VMEM = pl.BlockSpec(memory_space=pltpu.VMEM)
SMEM = pl.BlockSpec(memory_space=pltpu.SMEM)
HBM = pl.BlockSpec(memory_space=pltpu.HBM)


def dot(a, b, ca=1, cb=0):
    return lax.dot_general(a, b, (((ca,), (cb,)), ((), ())), preferred_element_type=F32)


ALONE = 67043328
SHARED = 16 * 1024 * 1024
GRADS_ROOM = 4500000
COEF_LANE = 64


def params(limit=SHARED):
    return pltpu.CompilerParams(vmem_limit_bytes=limit)


def cost(flops, bytes_accessed):
    return pl.CostEstimate(flops=flops, bytes_accessed=bytes_accessed, transcendentals=0)


def fetch(sems, *pairs):
    copies = [pltpu.make_async_copy(src, dst, sems.at[i]) for i, (src, dst) in enumerate(pairs)]
    for copy in copies:
        copy.start()
    return copies


def one_hot(place, slots):
    experts, toks = place.shape
    rows = lax.broadcasted_iota(jnp.int32, (slots, toks), 0).astype(F32)
    return [(rows == place[e : e + 1, :]).astype(F32) for e in range(experts)]


def route_kernel(
    slots, tok_hbm, routing_hbm, router_hbm, rows_ref, place_ref,
    tok_ref, routing_ref, router_ref, sems,
):
    copies = fetch(sems, (tok_hbm, tok_ref), (routing_hbm, routing_ref), (router_hbm, router_ref))
    toks = tok_ref.shape[0]
    experts = router_ref.shape[0]
    cols = rows_ref.shape[2]
    start = pl.multiple_of(lax.axis_index("tp") * cols, 128)
    for copy in copies:
        copy.wait()
    aff = jax.nn.sigmoid(dot(router_ref[...], tok_ref[...], 1, 1))
    ids = lax.broadcasted_iota(jnp.int32, (experts, toks), 0)
    routed = routing_ref[...]
    named = jnp.zeros((experts, toks), F32)
    for k in range(routed.shape[0]):
        named = named + (ids == routed[k : k + 1, :]).astype(F32)
    before = lax.broadcasted_iota(jnp.int32, (toks, toks), 0)
    after = lax.broadcasted_iota(jnp.int32, (toks, toks), 1)
    earlier = (before < after).astype(F32).astype(BF16)
    position = dot(named.astype(BF16), earlier)
    place = jnp.where(named > 0, position, -1.0)
    chosen = named * aff
    weights = chosen / jnp.sum(chosen, axis=0, keepdims=True)
    place_ref[...] = place
    hot = one_hot(place, slots)
    full = jnp.concatenate(hot, axis=0).astype(BF16)
    sent = dot(full, tok_ref[:, pl.ds(start, cols)])
    slope = named * aff * (1.0 - aff) / jnp.sum(chosen, axis=0, keepdims=True)
    row = lax.broadcasted_iota(jnp.int32, (experts, toks), 0)
    lane = lax.broadcasted_iota(jnp.int32, (8, 128), 1)
    for e in range(experts):
        own = weights[e : e + 1, :]
        others = jnp.sum(jnp.where(row == e, 0.0, weights), axis=0, keepdims=True)
        factors = jnp.where(row == e, others, -own) * slope
        table = jnp.concatenate([factors, own, jnp.zeros((127 - experts, toks), F32)], axis=0)
        values = dot(hot[e].astype(BF16), table.astype(BF16), 1, 1)
        tile = jnp.zeros((8, 128), F32)
        for g in range(slots // 8):
            part = values[8 * g : 8 * g + 8, :]
            tile = jnp.where(lane == g, part[:, experts : experts + 1], tile)
            shift = COEF_LANE + g * experts
            moved = pltpu.roll(part, shift, 1)
            tile = jnp.where((lane >= shift) & (lane < shift + experts), moved, tile)
        if cols > 128:
            tile = jnp.concatenate([tile, jnp.zeros((8, cols - 128), F32)], axis=1)
        block = jnp.concatenate([sent[e * slots : (e + 1) * slots, :], tile], axis=0)
        rows_ref[e] = block.astype(BF16)


def cots_kernel(slots, cot_hbm, place_ref, *refs):
    cot_ref, sems = refs[-2:]
    experts, toks = place_ref.shape
    cols = cot_ref.shape[1]
    start = pl.multiple_of((lax.axis_index("tp") % 2) * cols, 128)
    copies = fetch(sems, (cot_hbm.at[:, pl.ds(start, cols)], cot_ref))
    rows = lax.broadcasted_iota(jnp.int32, (slots, toks), 0).astype(F32)
    hot = [
        (rows == place_ref[pl.ds(lax.axis_index("ep") ^ k, 1), :]).astype(F32) for k in range(experts)
    ]
    full = jnp.concatenate(hot, axis=0).astype(BF16)
    copies[0].wait()
    sent = dot(full, cot_ref[...])
    for k in range(experts):
        refs[k][...] = sent[k * slots : (k + 1) * slots, :].astype(BF16)


def half_of(groups):
    me = lax.axis_index("ep")
    return me // (groups // 2), me % (groups // 2)


def join_kernel(*refs):
    out_ref = refs[-1]
    count = out_ref.shape[0]
    _, place = half_of(2 * count)
    for k in range(count):
        out_ref[place ^ k] = refs[k][...]


def add_parts(tokens_of, x_refs, wg_ref, wu_ref, acc_g, acc_u, fresh):
    groups, span, cols = x_refs[0].shape
    for r, x_ref in zip(tokens_of, x_refs):
        x = x_ref[...].reshape(groups * span, cols)
        rows = pl.ds(pl.multiple_of((lax.axis_index("tp") ^ r) * cols, 128), cols)
        part_g = dot(x, wg_ref[rows, :])
        part_u = dot(x, wu_ref[rows, :])
        acc_g[...] = part_g if fresh else acc_g[...] + part_g
        acc_u[...] = part_u if fresh else acc_u[...] + part_u
        fresh = False


def first_parts_kernel(which, *refs):
    count = len(which)
    add_parts(which, refs[:count], *refs[count:], True)


def more_parts_kernel(which, got_g, got_u, *refs):
    count = len(which)
    acc_g, acc_u = refs[-2:]
    acc_g[...] = got_g[...]
    acc_u[...] = got_u[...]
    add_parts(which, refs[:count], *refs[count:], False)


def gate_up_kernel(slots, which, got_g, got_u, own_ref, *refs):
    count = len(which)
    wg_ref, wu_ref, hid_ref, up_ref, gate_ref, acc_g, acc_u = refs[count:]
    groups, span, _ = own_ref.shape
    acc_g[...] = got_g[...]
    acc_u[...] = got_u[...]
    add_parts(which, refs[:count], wg_ref, wu_ref, acc_g, acc_u, False)
    for e in range(groups):
        scale = scale_column(own_ref, e, slots)
        at = slice(e * span, e * span + slots)
        pre_gate = acc_g[at, :]
        pre_up = acc_u[at, :]
        sig = jax.nn.sigmoid(pre_gate)
        act = pre_gate * sig
        hid_ref[e] = (act * pre_up).astype(BF16)
        up_ref[e] = scale * act
        gate_ref[e] = scale * (pre_up * sig * (1.0 + pre_gate * (1.0 - sig)))


def scale_column(x_ref, e, slots):
    tile = x_ref[e, slots:, :128].astype(F32)
    return jnp.concatenate([tile[:, g : g + 1] for g in range(slots // 8)], axis=0)


def back_kernel(groups, near_hbm, far_hbm, wd_hbm, back_ref):
    cols = near_hbm.shape[1]
    side, _ = half_of(groups)
    start = pl.multiple_of((lax.axis_index("tp") % 2) * cols, 128)
    wd = wd_hbm[:, pl.ds(start, cols)]
    back_ref[side] = dot(near_hbm[...], wd, 1, 1)
    back_ref[1 - side] = dot(far_hbm[...], wd, 1, 1)


def slot_parts(first, gg, gu, wg_ref, wu_ref, shares):
    cols = wg_ref.shape[0] // shares
    start = pl.multiple_of((lax.axis_index("tp") ^ first) * cols, 128)
    return dot(gg, wg_ref[pl.ds(start, cols), :], 1, 1) + dot(
        gu, wu_ref[pl.ds(start, cols), :], 1, 1
    )


def middle_kernel(
    slots, shares, back_ref, near_ref, far_ref, wd_ref, hid_ref, up_ref, gate_ref, wg_ref, wu_ref,
    g_ref, home_ref, chip_ref, term_ref, sum_ref,
):
    cols = near_ref.shape[1]
    groups = g_ref.shape[0]
    side, _ = half_of(groups)
    start = pl.multiple_of(((lax.axis_index("tp") % 2) ^ 1) * cols, 128)
    wd = wd_ref[:, pl.ds(start, cols)]
    sum_ref[side] = back_ref[side] + dot(near_ref[...], wd, 1, 1)
    sum_ref[1 - side] = back_ref[1 - side] + dot(far_ref[...], wd, 1, 1)
    back = sum_ref[...].reshape(hid_ref.shape)
    hidden = hid_ref.shape[1]
    term = jnp.sum(hid_ref[...].astype(F32) * back, axis=1, keepdims=True)
    gu = back * up_ref[...]
    gg = back * gate_ref[...]
    pad = jnp.zeros((8, gu.shape[1]), F32)
    for e in range(groups):
        at = slice(e * slots, (e + 1) * slots)
        g_ref[e, :, :hidden] = jnp.concatenate([gg[at], pad], axis=0).astype(BF16)
        g_ref[e, :, hidden:] = jnp.concatenate([gu[at], pad], axis=0).astype(BF16)
    lane = lax.broadcasted_iota(jnp.int32, term_ref.shape, 1)
    tile = jnp.zeros(term_ref.shape, F32)
    for c in range(term.shape[0] // 8):
        tile = jnp.where(lane == c, term[8 * c : 8 * c + 8, :], tile)
    term_ref[...] = tile
    gg = gg.astype(BF16)
    gu = gu.astype(BF16)
    for j in range(shares // 2):
        part = slot_parts(2 * j + 1, gg, gu, wg_ref, wu_ref, shares)
        if j == 0:
            home_ref[...] = part.astype(BF16)
        else:
            chip_ref[j - 1] = part.astype(BF16)


def even_kernel(slots, shares, g_ref, wg_ref, wu_ref, home_ref, chip_ref):
    groups, span, double = g_ref.shape
    both = g_ref[...].reshape(groups * span, double)
    gg, gu = both[:, : double // 2], both[:, double // 2 :]
    for j in range(shares // 2):
        part = slot_parts(2 * j, gg, gu, wg_ref, wu_ref, shares)
        for e in range(groups):
            block = part[e * span : e * span + slots, :]
            if j == 0:
                home_ref[e * slots : (e + 1) * slots, :] = block
            else:
                chip_ref[j - 1, e * slots : (e + 1) * slots, :] = block


def add_core_kernel(own_ref, got_ref, out_ref):
    out_ref[...] = (own_ref[...] + got_ref[...].astype(F32)).astype(BF16)


def add_chip_kernel(own_ref, core_ref, table_ref, router_ref, *refs):
    out_ref = refs[-1]
    experts = router_ref.shape[0]
    cols = out_ref.shape[1]
    start = pl.multiple_of(lax.axis_index("tp") * cols, 128)
    total = own_ref[...] + core_ref[...].astype(F32)
    total = total + dot(table_ref[...][:, :experts].astype(BF16), router_ref[:, pl.ds(start, cols)])
    for chip_ref in refs[:-1]:
        total = total + chip_ref[...].astype(F32)
    out_ref[...] = total.astype(BF16)


def grads_kernel(shares, q_ref, *refs):
    x_refs = refs[:shares]
    g_ref, gate_out, up_out, rows_out = refs[shares:]
    groups, span, cols = x_refs[0].shape
    double = g_ref.shape[2]
    for r in range(shares):

        @pl.when(pl.program_id(0) == r)
        def _(x_ref=x_refs[r]):
            x = x_ref[...].reshape(groups * span, cols)
            both = dot(x, g_ref[...].reshape(groups * span, double), 0, 0)
            gate, up = both[:, : double // 2], both[:, double // 2 :]
            gate_out[...] = gate.astype(BF16)
            up_out[...] = up.astype(BF16)
            rows_out[0, 0:1, :] = square_rows(gate)
            rows_out[0, 1:2, :] = square_rows(up)


def square_rows(value):
    square = value * value
    folded = square[:, :128]
    for at in range(128, value.shape[1], 128):
        folded = folded + square[:, at : at + 128]
    return jnp.sum(folded.T, axis=0, keepdims=True)


def down_kernel(slots, q_ref, *refs):
    x_ref, hid_ref, down_out, rows_out = refs[4:]
    groups = x_ref.shape[0]
    side, _ = half_of(groups)
    for h in range(2):

        @pl.when(pl.program_id(0) == h)
        def _(pair=refs[2 * h : 2 * h + 2]):
            down = 0.0
            for z_ref, at in zip(pair, (side, 1 - side)):
                scale = [scale_column(x_ref, at * (groups // 2) + e, slots) for e in range(groups // 2)]
                scale = jnp.concatenate(scale, axis=0)
                weighted = (scale * z_ref[...].astype(F32)).astype(BF16)
                down = down + dot(hid_ref[at], weighted, 0, 0)
            down_out[...] = down.astype(BF16)
            if h == 0:
                rows_out[...] = square_rows(down)
            else:
                rows_out[...] += square_rows(down)


def add_kernel(a_ref, b_ref, out_ref):
    out_ref[...] = a_ref[...] + b_ref[...]


def terms_kernel(slots, a_ref, b_ref, x_ref, table_ref, part_ref):
    term = (a_ref[...] + b_ref[...]).astype(BF16).astype(F32)
    groups, span, cols = x_ref.shape
    experts = part_ref.shape[0]
    count = slots // 8
    blocks = []
    for b in range(groups):
        spare = x_ref[b, slots:, :128].astype(F32)
        for g in range(count):
            factors = pltpu.roll(spare, 128 - COEF_LANE - g * experts, 1)
            c = b * count + g
            blocks.append(term[:, c : c + 1] * factors)
        blocks.append(jnp.zeros((8, 128), F32))
    table = jnp.concatenate(blocks, axis=0)
    table = jnp.where(lax.broadcasted_iota(jnp.int32, table.shape, 1) < experts, table, 0.0)
    for b in range(groups):
        table_ref[b * slots : (b + 1) * slots, :] = table[b * span : b * span + slots, :]
    high = table.astype(BF16)
    low = (table - high.astype(F32)).astype(BF16)
    x = x_ref[...].reshape(groups * span, cols)
    part_ref[...] = (dot(high, x, 0, 0) + dot(low, x, 0, 0))[:experts]


def last_sum_kernel(a_ref, b_ref, sum_ref, rows_ref):
    total = a_ref[...] + b_ref[...]
    sum_ref[...] = total
    rows_ref[...] = jnp.sum(total * total, axis=0, keepdims=True)


def slot_map_kernel(slots, place_ref, hot_ref):
    hot_ref[...] = jnp.concatenate(one_hot(place_ref[...], slots), axis=0).astype(BF16)


def home_kernel(got_hbm, hot_hbm, token_out, whole_hbm, got_ref, hot_ref, own_ref, sems):
    cols = got_ref.shape[1]
    start = pl.multiple_of(lax.axis_index("tp") * cols, 128)
    for copy in fetch(sems, (got_hbm, got_ref), (hot_hbm, hot_ref)):
        copy.wait()
    own_ref[...] = dot(hot_ref[...], got_ref[...], 0, 0).astype(BF16)
    copies = fetch(sems, (own_ref, token_out), (own_ref, whole_hbm.at[:, pl.ds(start, cols)]))
    for copy in copies:
        copy.wait()


def assemble_kernel(*refs):
    out_hbm, sems = refs[-2:]
    pairs = []
    for r, ref in enumerate(refs[1:-2]):
        cols = ref.shape[1]
        start = pl.multiple_of((lax.axis_index("tp") ^ (r + 1)) * cols, 128)
        pairs.append((ref, out_hbm.at[:, pl.ds(start, cols)]))
    for copy in fetch(sems, *pairs):
        copy.wait()


def call(kernel, outs, scalar, *args, flops=0, nbytes=0, scratch=(), hbm=(), out_hbm=False, limit=SHARED):
    single = not isinstance(outs, tuple)
    ins = [HBM if i in hbm else VMEM for i in range(int(scalar), len(args))]
    out = HBM if out_hbm else VMEM
    return pl.pallas_call(
        kernel,
        out_shape=outs,
        in_specs=([SMEM] if scalar else []) + ins,
        out_specs=out if single else tuple(out for _ in outs),
        scratch_shapes=list(scratch),
        compiler_params=params(limit),
        cost_estimate=cost(flops, nbytes),
    )(*args)


DMAS = pltpu.SemaphoreType.DMA


def buffer(*dims, dtype=BF16):
    return pltpu.VMEM(dims, dtype)


def shape(*dims, dtype=BF16):
    return jax.ShapeDtypeStruct(dims, dtype)


def per_device(tokens, routing, router_weight, gate_weight, up_weight, down_weight, cotangent):
    return layer(tokens, routing.T, router_weight.T, gate_weight[0], up_weight[0], down_weight[0], cotangent)


def layer(tokens, routing, router, wg, wu, wd, cotangent):
    groups = lax.axis_size("ep")
    shares = lax.axis_size("tp")
    chips = shares // 2
    toks, width = tokens.shape
    top = routing.shape[0]
    experts = router.shape[0]
    hidden = wg.shape[1]
    capacity = 7 * toks * top // (4 * experts)
    slots = -(-capacity // 8) * 8
    span = slots + 8
    count = groups * slots
    cols = width // shares
    half = width // 2
    unit = 2 * count * half * hidden
    q = lax.axis_index("tp").astype(jnp.int32).reshape(1)

    def swap(value, bit, axis="tp"):
        size = lax.axis_size(axis)
        return lax.ppermute(value, axis, [(i, i ^ bit) for i in range(size)])

    def exchange(value):
        return lax.all_to_all(value, "ep", split_axis=0, concat_axis=0, tiled=True)

    def spread(value):
        far = [value] + [swap(value, 2 * j) for j in range(1, chips)]
        return [part for piece in far for part in (piece, swap(piece, 1))]

    rows_send, place = call(
        functools.partial(route_kernel, slots),
        (shape(experts, span, cols), shape(experts, toks, dtype=F32)),
        False, tokens, routing, router, hbm=(0, 1, 2), limit=ALONE,
        scratch=[buffer(toks, width), buffer(top, toks, dtype=jnp.int32), buffer(experts, width), DMAS((3,))],
    )
    rows_got = exchange(rows_send)
    pieces = call(
        functools.partial(cots_kernel, slots), tuple(shape(slots, half) for _ in range(experts)),
        False, cotangent, place, flops=2 * count * toks * half, hbm=(0,), limit=ALONE,
        scratch=[buffer(toks, half), DMAS((1,))],
    )
    pieces = list(pieces)
    for k in range(experts - 1, 0, -1):
        pieces[k] = swap(pieces[k], k, "ep")

    hot = call(functools.partial(slot_map_kernel, slots), shape(count, toks), False, place)

    x_parts = spread(rows_got)
    sums = tuple(shape(groups * span, hidden, dtype=F32) for _ in range(2))
    chip_parts, core_parts = list(range(2, shares, 2)), list(range(3, shares, 2))
    pre = call(
        functools.partial(first_parts_kernel, (0, 1)), sums,
        False, *x_parts[:2], wg, wu, flops=unit,
    )
    pre = call(
        functools.partial(more_parts_kernel, chip_parts), sums,
        False, *pre, *[x_parts[r] for r in chip_parts], wg, wu, flops=unit,
    )
    hid, up_factor, gate_factor = call(
        functools.partial(gate_up_kernel, slots, core_parts),
        (shape(groups, slots, hidden), shape(groups, slots, hidden, dtype=F32), shape(groups, slots, hidden, dtype=F32)),
        False, *pre, x_parts[0], *[x_parts[r] for r in core_parts], wg, wu, flops=2 * unit,
        scratch=[pltpu.VMEM((groups * span, hidden), F32)] * 2,
    )
    hid = hid.reshape(count, hidden)
    up_factor = up_factor.reshape(count, hidden)
    gate_factor = gate_factor.reshape(count, hidden)

    side = groups // 2
    near = call(
        join_kernel, shape(side, slots, half), False, *pieces[:side],
    ).reshape(count // 2, half)
    near_got = swap(near, 1)
    far = call(
        join_kernel, shape(side, slots, half), False, *pieces[side:],
    ).reshape(count // 2, half)
    far_got = swap(far, 1)
    back = call(
        functools.partial(back_kernel, groups), shape(2, count // 2, hidden, dtype=F32),
        False, near, far, wd, flops=unit,
    )
    g, odd_home, odd_chip, term = call(
        functools.partial(middle_kernel, slots, shares),
        (
            shape(groups, span, 2 * hidden),
            shape(count, cols),
            shape(chips - 1, count, cols),
            shape(8, -(-count // 1024) * 128, dtype=F32),
        ),
        False, back, near_got, far_got, wd, hid, up_factor, gate_factor, wg, wu, flops=3 * unit,
        scratch=[buffer(2, count // 2, hidden, dtype=F32)],
    )
    term_got = swap(term, 1)
    core_chip = swap(odd_chip, 1)
    core_home = swap(odd_home, 1)
    even_home, even_chip = call(
        functools.partial(even_kernel, slots, shares),
        (shape(count, cols, dtype=F32), shape(chips - 1, count, cols, dtype=F32)),
        False, g, wg, wu, flops=2 * unit,
    )

    def add(a, b, kernel=add_kernel, lead=()):
        return call(kernel, shape(*lead, *a.shape, dtype=F32), False, a, b)

    term = add(term, term_got)
    bit = 2
    while 2 * bit < shares:
        term = add(term, swap(term, bit))
        bit *= 2
    term_got = swap(term, bit)
    chip_send = call(add_core_kernel, shape(chips - 1, count, cols), False, even_chip, core_chip)
    chip_got = [swap(chip_send[j], 2 * (j + 1)) for j in range(chips - 1)]
    table, router_sum = call(
        functools.partial(terms_kernel, slots),
        (shape(count, 128, dtype=F32), shape(experts, cols, dtype=F32)),
        False, term, term_got, rows_got,
    )
    bit = 1
    while 2 * bit < groups:
        router_got = swap(router_sum, bit, "ep")
        router_sum = add(router_sum, router_got)
        bit *= 2
    router_got = swap(router_sum, bit, "ep")
    router_sum, router_rows = call(
        last_sum_kernel, (shape(experts, cols, dtype=F32), shape(1, cols, dtype=F32)),
        False, router_sum, router_got,
    )
    router_rows = router_rows.reshape(cols)
    home_send = call(
        add_chip_kernel, shape(count, cols), False, even_home, core_home, table, router, *chip_got,
    )
    home_got = exchange(home_send.reshape(groups, slots, cols)).reshape(count, cols)

    grad_spec = pl.BlockSpec((cols, hidden), lambda r, q: (q[0] ^ r, 0))
    gate_grad, up_grad, norms = pl.pallas_call(
        functools.partial(grads_kernel, shares),
        out_shape=(shape(width, hidden), shape(width, hidden), shape(shares, 2, cols, dtype=F32)),
        grid_spec=pltpu.PrefetchScalarGridSpec(
            num_scalar_prefetch=1,
            grid=(shares,),
            in_specs=[VMEM] * (shares + 1),
            out_specs=(grad_spec, grad_spec, pl.BlockSpec((1, 2, cols), lambda r, q: (q[0] ^ r, 0, 0))),
        ),
        compiler_params=params(ALONE - GRADS_ROOM),
        cost_estimate=cost(4 * unit, 0),
        name="grads",
    )(q, *x_parts, g)
    down_grad, down_rows = pl.pallas_call(
        functools.partial(down_kernel, slots),
        out_shape=(shape(hidden, width), shape(1, hidden, dtype=F32)),
        grid_spec=pltpu.PrefetchScalarGridSpec(
            num_scalar_prefetch=1,
            grid=(2,),
            in_specs=[VMEM] * 6,
            out_specs=(
                pl.BlockSpec((hidden, half), lambda h, q: (0, (q[0] % 2) ^ h)),
                pl.BlockSpec((1, hidden), lambda h, q: (0, 0)),
            ),
        ),
        compiler_params=params(ALONE),
        cost_estimate=cost(2 * unit, 0),
        name="down",
    )(q, near, far, near_got, far_got, rows_got, hid.reshape(2, count // 2, hidden))
    norms = norms.transpose(1, 0, 2).reshape(2, width)
    norms = spread(norms)
    while len(norms) > 1:
        norms = [a + b for a, b in zip(norms[::2], norms[1::2])]
    norms = norms[0]

    token_part, token_grad = call(
        home_kernel, (shape(toks, cols), shape(toks, width)),
        False, home_got, hot, hbm=(0, 1), limit=ALONE, out_hbm=True,
        scratch=[buffer(count, cols), buffer(count, toks), buffer(toks, cols), DMAS((2,))],
    )
    token_parts = spread(token_part)[1:]
    token_grad = pl.pallas_call(
        assemble_kernel,
        out_shape=shape(toks, width),
        in_specs=[HBM] + [VMEM] * (shares - 1),
        out_specs=HBM,
        scratch_shapes=[DMAS((shares - 1,))],
        input_output_aliases={0: 0},
        compiler_params=params(),
        name="assemble",
    )(token_grad, *token_parts)
    return (
        token_grad,
        router_sum.T,
        router_rows,
        gate_grad[None],
        up_grad[None],
        down_grad[None],
        norms[0:1],
        norms[1:2],
        down_rows,
    )


def solution(mesh):
    return jax.shard_map(
        per_device,
        mesh=mesh,
        in_specs=(
            P("ep", None),
            P("ep", None),
            P(),
            P("ep", None, "tp"),
            P("ep", None, "tp"),
            P("ep", "tp", None),
            P("ep", None),
        ),
        out_specs=(
            P("ep", None),
            P("tp", None),
            P("tp"),
            P("ep", None, "tp"),
            P("ep", None, "tp"),
            P("ep", "tp", None),
            P("ep", None),
            P("ep", None),
            P("ep", "tp"),
        ),
        check_vma=False,
    )
```

```python
import functools

import jax
import jax.numpy as jnp
from jax import lax
from jax.experimental import pallas as pl
from jax.experimental.pallas import tpu as pltpu
from jax.sharding import PartitionSpec as P


BF16 = jnp.bfloat16
F32 = jnp.float32
VMEM = pl.BlockSpec(memory_space=pltpu.VMEM)
SMEM = pl.BlockSpec(memory_space=pltpu.SMEM)
HBM = pl.BlockSpec(memory_space=pltpu.HBM)


def dot(a, b, ca=1, cb=0):
    return lax.dot_general(a, b, (((ca,), (cb,)), ((), ())), preferred_element_type=F32)


ALONE = 67043328
SHARED = 16 * 1024 * 1024
GRADS_ROOM = 4500000
COEF_LANE = 64


def params(limit=SHARED):
    return pltpu.CompilerParams(vmem_limit_bytes=limit)


def cost(flops, bytes_accessed):
    return pl.CostEstimate(flops=flops, bytes_accessed=bytes_accessed, transcendentals=0)


def fetch(sems, *pairs):
    copies = [pltpu.make_async_copy(src, dst, sems.at[i]) for i, (src, dst) in enumerate(pairs)]
    for copy in copies:
        copy.start()
    return copies


def one_hot(place, slots):
    experts, toks = place.shape
    rows = lax.broadcasted_iota(jnp.int32, (slots, toks), 0).astype(F32)
    return [(rows == place[e : e + 1, :]).astype(F32) for e in range(experts)]


def route_kernel(
    slots, tok_hbm, routing_hbm, router_hbm, rows_ref, place_ref,
    tok_ref, routing_ref, router_ref, sems,
):
    copies = fetch(sems, (tok_hbm, tok_ref), (routing_hbm, routing_ref), (router_hbm, router_ref))
    toks = tok_ref.shape[0]
    experts = router_ref.shape[0]
    cols = rows_ref.shape[2]
    start = pl.multiple_of(lax.axis_index("tp") * cols, 128)
    for copy in copies:
        copy.wait()
    aff = jax.nn.sigmoid(dot(router_ref[...], tok_ref[...], 1, 1))
    ids = lax.broadcasted_iota(jnp.int32, (experts, toks), 0)
    routed = routing_ref[...]
    named = jnp.zeros((experts, toks), F32)
    for k in range(routed.shape[0]):
        named = named + (ids == routed[k : k + 1, :]).astype(F32)
    before = lax.broadcasted_iota(jnp.int32, (toks, toks), 0)
    after = lax.broadcasted_iota(jnp.int32, (toks, toks), 1)
    earlier = (before < after).astype(F32).astype(BF16)
    position = dot(named.astype(BF16), earlier)
    place = jnp.where(named > 0, position, -1.0)
    chosen = named * aff
    weights = chosen / jnp.sum(chosen, axis=0, keepdims=True)
    place_ref[...] = place
    hot = one_hot(place, slots)
    full = jnp.concatenate(hot, axis=0).astype(BF16)
    sent = dot(full, tok_ref[:, pl.ds(start, cols)])
    slope = named * aff * (1.0 - aff) / jnp.sum(chosen, axis=0, keepdims=True)
    row = lax.broadcasted_iota(jnp.int32, (experts, toks), 0)
    lane = lax.broadcasted_iota(jnp.int32, (8, 128), 1)
    for e in range(experts):
        own = weights[e : e + 1, :]
        others = jnp.sum(jnp.where(row == e, 0.0, weights), axis=0, keepdims=True)
        factors = jnp.where(row == e, others, -own) * slope
        table = jnp.concatenate([factors, own, jnp.zeros((127 - experts, toks), F32)], axis=0)
        values = dot(hot[e].astype(BF16), table.astype(BF16), 1, 1)
        tile = jnp.zeros((8, 128), F32)
        for g in range(slots // 8):
            part = values[8 * g : 8 * g + 8, :]
            tile = jnp.where(lane == g, part[:, experts : experts + 1], tile)
            shift = COEF_LANE + g * experts
            moved = pltpu.roll(part, shift, 1)
            tile = jnp.where((lane >= shift) & (lane < shift + experts), moved, tile)
        if cols > 128:
            tile = jnp.concatenate([tile, jnp.zeros((8, cols - 128), F32)], axis=1)
        block = jnp.concatenate([sent[e * slots : (e + 1) * slots, :], tile], axis=0)
        rows_ref[e] = block.astype(BF16)


def cots_kernel(slots, cot_hbm, place_ref, *refs):
    cot_ref, sems = refs[-2:]
    experts, toks = place_ref.shape
    cols = cot_ref.shape[1]
    start = pl.multiple_of((lax.axis_index("tp") % 2) * cols, 128)
    copies = fetch(sems, (cot_hbm.at[:, pl.ds(start, cols)], cot_ref))
    rows = lax.broadcasted_iota(jnp.int32, (slots, toks), 0).astype(F32)
    hot = [
        (rows == place_ref[pl.ds(lax.axis_index("ep") ^ k, 1), :]).astype(F32) for k in range(experts)
    ]
    full = jnp.concatenate(hot, axis=0).astype(BF16)
    copies[0].wait()
    sent = dot(full, cot_ref[...])
    for k in range(experts):
        refs[k][...] = sent[k * slots : (k + 1) * slots, :].astype(BF16)


def half_of(groups):
    me = lax.axis_index("ep")
    return me // (groups // 2), me % (groups // 2)


def join_kernel(*refs):
    out_ref = refs[-1]
    count = out_ref.shape[0]
    _, place = half_of(2 * count)
    for k in range(count):
        out_ref[place ^ k] = refs[k][...]


def add_parts(tokens_of, x_refs, wg_ref, wu_ref, acc_g, acc_u, fresh):
    groups, span, cols = x_refs[0].shape
    for r, x_ref in zip(tokens_of, x_refs):
        x = x_ref[...].reshape(groups * span, cols)
        rows = pl.ds(pl.multiple_of((lax.axis_index("tp") ^ r) * cols, 128), cols)
        part_g = dot(x, wg_ref[rows, :])
        part_u = dot(x, wu_ref[rows, :])
        acc_g[...] = part_g if fresh else acc_g[...] + part_g
        acc_u[...] = part_u if fresh else acc_u[...] + part_u
        fresh = False


def first_parts_kernel(which, *refs):
    count = len(which)
    add_parts(which, refs[:count], *refs[count:], True)


def more_parts_kernel(which, got_g, got_u, *refs):
    count = len(which)
    acc_g, acc_u = refs[-2:]
    acc_g[...] = got_g[...]
    acc_u[...] = got_u[...]
    add_parts(which, refs[:count], *refs[count:], False)


def gate_up_kernel(slots, which, got_g, got_u, own_ref, *refs):
    count = len(which)
    wg_ref, wu_ref, hid_ref, up_ref, gate_ref, acc_g, acc_u = refs[count:]
    groups, span, _ = own_ref.shape
    acc_g[...] = got_g[...]
    acc_u[...] = got_u[...]
    add_parts(which, refs[:count], wg_ref, wu_ref, acc_g, acc_u, False)
    for e in range(groups):
        scale = scale_column(own_ref, e, slots)
        at = slice(e * span, e * span + slots)
        pre_gate = acc_g[at, :]
        pre_up = acc_u[at, :]
        sig = jax.nn.sigmoid(pre_gate)
        act = pre_gate * sig
        hid_ref[e] = (act * pre_up).astype(BF16)
        up_ref[e] = scale * act
        gate_ref[e] = scale * (pre_up * sig * (1.0 + pre_gate * (1.0 - sig)))


def scale_column(x_ref, e, slots):
    tile = x_ref[e, slots:, :128].astype(F32)
    return jnp.concatenate([tile[:, g : g + 1] for g in range(slots // 8)], axis=0)


def back_kernel(groups, near_ref, far_ref, near_got, wd_ref, back_ref):
    cols = near_ref.shape[1]
    side, _ = half_of(groups)
    core = lax.axis_index("tp") % 2
    own = wd_ref[:, pl.ds(pl.multiple_of(core * cols, 128), cols)]
    other = wd_ref[:, pl.ds(pl.multiple_of((core ^ 1) * cols, 128), cols)]
    back_ref[1 - side] = dot(far_ref[...], own, 1, 1)
    back_ref[side] = dot(near_ref[...], own, 1, 1) + dot(near_got[...], other, 1, 1)


def slot_parts(first, gg, gu, wg_ref, wu_ref, shares):
    cols = wg_ref.shape[0] // shares
    start = pl.multiple_of((lax.axis_index("tp") ^ first) * cols, 128)
    return dot(gg, wg_ref[pl.ds(start, cols), :], 1, 1) + dot(
        gu, wu_ref[pl.ds(start, cols), :], 1, 1
    )


def middle_kernel(
    slots, shares, back_ref, far_ref, wd_ref, hid_ref, up_ref, gate_ref, wg_ref, wu_ref,
    g_ref, chip_ref, term_ref, sum_ref,
):
    cols = far_ref.shape[1]
    groups = g_ref.shape[0]
    side, _ = half_of(groups)
    start = pl.multiple_of(((lax.axis_index("tp") % 2) ^ 1) * cols, 128)
    wd = wd_ref[:, pl.ds(start, cols)]
    sum_ref[side] = back_ref[side]
    sum_ref[1 - side] = back_ref[1 - side] + dot(far_ref[...], wd, 1, 1)
    back = sum_ref[...].reshape(hid_ref.shape)
    hidden = hid_ref.shape[1]
    term = jnp.sum(hid_ref[...].astype(F32) * back, axis=1, keepdims=True)
    gu = back * up_ref[...]
    gg = back * gate_ref[...]
    pad = jnp.zeros((8, gu.shape[1]), F32)
    for e in range(groups):
        at = slice(e * slots, (e + 1) * slots)
        g_ref[e, :, :hidden] = jnp.concatenate([gg[at], pad], axis=0).astype(BF16)
        g_ref[e, :, hidden:] = jnp.concatenate([gu[at], pad], axis=0).astype(BF16)
    lane = lax.broadcasted_iota(jnp.int32, term_ref.shape, 1)
    tile = jnp.zeros(term_ref.shape, F32)
    for c in range(term.shape[0] // 8):
        tile = jnp.where(lane == c, term[8 * c : 8 * c + 8, :], tile)
    term_ref[...] = tile
    gg = gg.astype(BF16)
    gu = gu.astype(BF16)
    for j in range(1, shares // 2):
        chip_ref[j - 1] = slot_parts(2 * j + 1, gg, gu, wg_ref, wu_ref, shares).astype(BF16)


def even_kernel(slots, shares, g_ref, wg_ref, wu_ref, chip_ref):
    groups, span, double = g_ref.shape
    both = g_ref[...].reshape(groups * span, double)
    gg, gu = both[:, : double // 2], both[:, double // 2 :]
    for j in range(1, shares // 2):
        part = slot_parts(2 * j, gg, gu, wg_ref, wu_ref, shares)
        for e in range(groups):
            chip_ref[j - 1, e * slots : (e + 1) * slots, :] = part[e * span : e * span + slots, :]


def rest_kernel(slots, shares, g_ref, wg_ref, wu_ref, odd_ref, even_ref):
    groups, span, double = g_ref.shape
    both = g_ref[...].reshape(groups * span, double)
    gg, gu = both[:, : double // 2], both[:, double // 2 :]
    for r, out_ref in enumerate((even_ref, odd_ref)):
        part = slot_parts(r, gg, gu, wg_ref, wu_ref, shares)
        for e in range(groups):
            block = part[e * span : e * span + slots, :]
            out_ref[e] = block.astype(out_ref.dtype)


def add_core_kernel(own_ref, got_ref, out_ref):
    out_ref[...] = (own_ref[...] + got_ref[...].astype(F32)).astype(BF16)


def base_kernel(own_ref, core_ref, table_ref, router_ref, out_ref):
    experts = router_ref.shape[0]
    cols = out_ref.shape[1]
    start = pl.multiple_of(lax.axis_index("tp") * cols, 128)
    total = own_ref[...] + core_ref[...].astype(F32)
    out_ref[...] = total + dot(table_ref[...][:, :experts].astype(BF16), router_ref[:, pl.ds(start, cols)])


def add_chip_kernel(base_ref, *refs):
    total = base_ref[...]
    for chip_ref in refs[:-1]:
        total = total + chip_ref[...].astype(F32)
    refs[-1][...] = total.astype(BF16)


def grads_kernel(shares, q_ref, *refs):
    x_refs = refs[:shares]
    g_ref, gate_out, up_out, rows_out = refs[shares:]
    groups, span, cols = x_refs[0].shape
    double = g_ref.shape[2]
    for r in range(shares):

        @pl.when(pl.program_id(0) == r)
        def _(x_ref=x_refs[r]):
            x = x_ref[...].reshape(groups * span, cols)
            both = dot(x, g_ref[...].reshape(groups * span, double), 0, 0)
            gate, up = both[:, : double // 2], both[:, double // 2 :]
            gate_out[...] = gate.astype(BF16)
            up_out[...] = up.astype(BF16)
            rows_out[0, 0:1, :] = square_rows(gate)
            rows_out[0, 1:2, :] = square_rows(up)


def square_rows(value):
    square = value * value
    folded = square[:, :128]
    for at in range(128, value.shape[1], 128):
        folded = folded + square[:, at : at + 128]
    return jnp.sum(folded.T, axis=0, keepdims=True)


def down_kernel(slots, q_ref, *refs):
    x_ref, hid_ref, down_out, rows_out = refs[4:]
    groups = x_ref.shape[0]
    side, _ = half_of(groups)
    for h in range(2):

        @pl.when(pl.program_id(0) == h)
        def _(pair=refs[2 * h : 2 * h + 2]):
            down = 0.0
            for z_ref, at in zip(pair, (side, 1 - side)):
                scale = [scale_column(x_ref, at * (groups // 2) + e, slots) for e in range(groups // 2)]
                scale = jnp.concatenate(scale, axis=0)
                weighted = (scale * z_ref[...].astype(F32)).astype(BF16)
                down = down + dot(hid_ref[at], weighted, 0, 0)
            down_out[...] = down.astype(BF16)
            if h == 0:
                rows_out[...] = square_rows(down)
            else:
                rows_out[...] += square_rows(down)


def add_kernel(a_ref, b_ref, out_ref):
    out_ref[...] = a_ref[...] + b_ref[...]


def terms_kernel(slots, a_ref, b_ref, x_ref, table_ref, part_ref):
    term = (a_ref[...] + b_ref[...]).astype(BF16).astype(F32)
    groups, span, cols = x_ref.shape
    experts = part_ref.shape[0]
    count = slots // 8
    blocks = []
    for b in range(groups):
        spare = x_ref[b, slots:, :128].astype(F32)
        for g in range(count):
            factors = pltpu.roll(spare, 128 - COEF_LANE - g * experts, 1)
            c = b * count + g
            blocks.append(term[:, c : c + 1] * factors)
        blocks.append(jnp.zeros((8, 128), F32))
    table = jnp.concatenate(blocks, axis=0)
    table = jnp.where(lax.broadcasted_iota(jnp.int32, table.shape, 1) < experts, table, 0.0)
    for b in range(groups):
        table_ref[b * slots : (b + 1) * slots, :] = table[b * span : b * span + slots, :]
    high = table.astype(BF16)
    low = (table - high.astype(F32)).astype(BF16)
    x = x_ref[...].reshape(groups * span, cols)
    part_ref[...] = (dot(high, x, 0, 0) + dot(low, x, 0, 0))[:experts]


def last_sum_kernel(a_ref, b_ref, sum_ref, rows_ref):
    total = a_ref[...] + b_ref[...]
    sum_ref[...] = total
    rows_ref[...] = jnp.sum(total * total, axis=0, keepdims=True)


def slot_map_kernel(slots, place_ref, hot_ref):
    hot_ref[...] = jnp.concatenate(one_hot(place_ref[...], slots), axis=0).astype(BF16)


def home_kernel(got_hbm, hot_hbm, token_out, whole_hbm, got_ref, hot_ref, own_ref, sems):
    cols = got_ref.shape[1]
    start = pl.multiple_of(lax.axis_index("tp") * cols, 128)
    for copy in fetch(sems, (got_hbm, got_ref), (hot_hbm, hot_ref)):
        copy.wait()
    own_ref[...] = dot(hot_ref[...], got_ref[...], 0, 0).astype(BF16)
    copies = fetch(sems, (own_ref, token_out), (own_ref, whole_hbm.at[:, pl.ds(start, cols)]))
    for copy in copies:
        copy.wait()


def assemble_kernel(*refs):
    out_hbm, sems = refs[-2:]
    pairs = []
    for r, ref in enumerate(refs[1:-2]):
        cols = ref.shape[1]
        start = pl.multiple_of((lax.axis_index("tp") ^ (r + 1)) * cols, 128)
        pairs.append((ref, out_hbm.at[:, pl.ds(start, cols)]))
    for copy in fetch(sems, *pairs):
        copy.wait()


def call(kernel, outs, scalar, *args, flops=0, nbytes=0, scratch=(), hbm=(), out_hbm=False, limit=SHARED):
    single = not isinstance(outs, tuple)
    ins = [HBM if i in hbm else VMEM for i in range(int(scalar), len(args))]
    out = HBM if out_hbm else VMEM
    return pl.pallas_call(
        kernel,
        out_shape=outs,
        in_specs=([SMEM] if scalar else []) + ins,
        out_specs=out if single else tuple(out for _ in outs),
        scratch_shapes=list(scratch),
        compiler_params=params(limit),
        cost_estimate=cost(flops, nbytes),
    )(*args)


DMAS = pltpu.SemaphoreType.DMA


def buffer(*dims, dtype=BF16):
    return pltpu.VMEM(dims, dtype)


def shape(*dims, dtype=BF16):
    return jax.ShapeDtypeStruct(dims, dtype)


def per_device(tokens, routing, router_weight, gate_weight, up_weight, down_weight, cotangent):
    return layer(tokens, routing.T, router_weight.T, gate_weight[0], up_weight[0], down_weight[0], cotangent)


def layer(tokens, routing, router, wg, wu, wd, cotangent):
    groups = lax.axis_size("ep")
    shares = lax.axis_size("tp")
    chips = shares // 2
    toks, width = tokens.shape
    top = routing.shape[0]
    experts = router.shape[0]
    hidden = wg.shape[1]
    capacity = 7 * toks * top // (4 * experts)
    slots = -(-capacity // 8) * 8
    span = slots + 8
    count = groups * slots
    cols = width // shares
    half = width // 2
    unit = 2 * count * half * hidden
    q = lax.axis_index("tp").astype(jnp.int32).reshape(1)

    def swap(value, bit, axis="tp"):
        size = lax.axis_size(axis)
        return lax.ppermute(value, axis, [(i, i ^ bit) for i in range(size)])

    def exchange(value):
        return lax.all_to_all(value, "ep", split_axis=0, concat_axis=0, tiled=True)

    def spread(value):
        far = [value] + [swap(value, 2 * j) for j in range(1, chips)]
        return [part for piece in far for part in (piece, swap(piece, 1))]

    rows_send, place = call(
        functools.partial(route_kernel, slots),
        (shape(experts, span, cols), shape(experts, toks, dtype=F32)),
        False, tokens, routing, router, hbm=(0, 1, 2), limit=ALONE,
        scratch=[buffer(toks, width), buffer(top, toks, dtype=jnp.int32), buffer(experts, width), DMAS((3,))],
    )
    rows_got = exchange(rows_send)
    pieces = call(
        functools.partial(cots_kernel, slots), tuple(shape(slots, half) for _ in range(experts)),
        False, cotangent, place, flops=2 * count * toks * half, hbm=(0,), limit=ALONE,
        scratch=[buffer(toks, half), DMAS((1,))],
    )
    pieces = list(pieces)
    for k in range(experts - 1, 0, -1):
        pieces[k] = swap(pieces[k], k, "ep")

    hot = call(functools.partial(slot_map_kernel, slots), shape(count, toks), False, place)

    x_parts = spread(rows_got)
    sums = tuple(shape(groups * span, hidden, dtype=F32) for _ in range(2))
    chip_parts, core_parts = list(range(2, shares, 2)), list(range(3, shares, 2))
    pre = call(
        functools.partial(first_parts_kernel, (0, 1)), sums,
        False, *x_parts[:2], wg, wu, flops=unit,
    )
    pre = call(
        functools.partial(more_parts_kernel, chip_parts), sums,
        False, *pre, *[x_parts[r] for r in chip_parts], wg, wu, flops=unit,
    )
    hid, up_factor, gate_factor = call(
        functools.partial(gate_up_kernel, slots, core_parts),
        (shape(groups, slots, hidden), shape(groups, slots, hidden, dtype=F32), shape(groups, slots, hidden, dtype=F32)),
        False, *pre, x_parts[0], *[x_parts[r] for r in core_parts], wg, wu, flops=2 * unit,
        scratch=[pltpu.VMEM((groups * span, hidden), F32)] * 2,
    )
    hid = hid.reshape(count, hidden)
    up_factor = up_factor.reshape(count, hidden)
    gate_factor = gate_factor.reshape(count, hidden)

    side = groups // 2
    near = call(join_kernel, shape(side, slots, half), False, *pieces[:side]).reshape(count // 2, half)
    near_got = swap(near, 1)
    far = call(join_kernel, shape(side, slots, half), False, *pieces[side:]).reshape(count // 2, half)
    far_got = swap(far, 1)
    back = call(
        functools.partial(back_kernel, groups), shape(2, count // 2, hidden, dtype=F32),
        False, near, far, near_got, wd, flops=unit,
    )
    g, odd_chip, term = call(
        functools.partial(middle_kernel, slots, shares),
        (
            shape(groups, span, 2 * hidden),
            shape(chips - 1, count, cols),
            shape(8, -(-count // 1024) * 128, dtype=F32),
        ),
        False, back, far_got, wd, hid, up_factor, gate_factor, wg, wu, flops=3 * unit,
        scratch=[buffer(2, count // 2, hidden, dtype=F32)],
    )
    term_got = swap(term, 1)
    core_chip = swap(odd_chip, 1)
    even_chip = call(
        functools.partial(even_kernel, slots, shares), shape(chips - 1, count, cols, dtype=F32),
        False, g, wg, wu, flops=unit,
    )
    odd_home, even_home = call(
        functools.partial(rest_kernel, slots, shares),
        (shape(groups, slots, cols), shape(groups, slots, cols, dtype=F32)),
        False, g, wg, wu, flops=2 * unit,
    )
    even_home = even_home.reshape(count, cols)
    core_home = swap(odd_home.reshape(count, cols), 1)

    def add(a, b, kernel=add_kernel, lead=()):
        return call(kernel, shape(*lead, *a.shape, dtype=F32), False, a, b)

    term = add(term, term_got)
    bit = 2
    while 2 * bit < shares:
        term = add(term, swap(term, bit))
        bit *= 2
    term_got = swap(term, bit)
    chip_send = call(add_core_kernel, shape(chips - 1, count, cols), False, even_chip, core_chip)
    chip_got = [swap(chip_send[j], 2 * (j + 1)) for j in range(chips - 1)]
    table, router_sum = call(
        functools.partial(terms_kernel, slots),
        (shape(count, 128, dtype=F32), shape(experts, cols, dtype=F32)),
        False, term, term_got, rows_got,
    )
    bit = 1
    while 2 * bit < groups:
        router_got = swap(router_sum, bit, "ep")
        router_sum = add(router_sum, router_got)
        bit *= 2
    router_got = swap(router_sum, bit, "ep")
    router_sum, router_rows = call(
        last_sum_kernel, (shape(experts, cols, dtype=F32), shape(1, cols, dtype=F32)),
        False, router_sum, router_got,
    )
    router_rows = router_rows.reshape(cols)
    base = call(base_kernel, shape(count, cols, dtype=F32), False, even_home, core_home, table, router)
    home_send = call(add_chip_kernel, shape(count, cols), False, base, *chip_got)
    home_got = exchange(home_send.reshape(groups, slots, cols)).reshape(count, cols)

    grad_spec = pl.BlockSpec((cols, hidden), lambda r, q: (q[0] ^ r, 0))
    gate_grad, up_grad, norms = pl.pallas_call(
        functools.partial(grads_kernel, shares),
        out_shape=(shape(width, hidden), shape(width, hidden), shape(shares, 2, cols, dtype=F32)),
        grid_spec=pltpu.PrefetchScalarGridSpec(
            num_scalar_prefetch=1,
            grid=(shares,),
            in_specs=[VMEM] * (shares + 1),
            out_specs=(grad_spec, grad_spec, pl.BlockSpec((1, 2, cols), lambda r, q: (q[0] ^ r, 0, 0))),
        ),
        compiler_params=params(ALONE - GRADS_ROOM),
        cost_estimate=cost(4 * unit, 0),
        name="grads",
    )(q, *x_parts, g)
    down_grad, down_rows = pl.pallas_call(
        functools.partial(down_kernel, slots),
        out_shape=(shape(hidden, width), shape(1, hidden, dtype=F32)),
        grid_spec=pltpu.PrefetchScalarGridSpec(
            num_scalar_prefetch=1,
            grid=(2,),
            in_specs=[VMEM] * 6,
            out_specs=(
                pl.BlockSpec((hidden, half), lambda h, q: (0, (q[0] % 2) ^ h)),
                pl.BlockSpec((1, hidden), lambda h, q: (0, 0)),
            ),
        ),
        compiler_params=params(ALONE),
        cost_estimate=cost(2 * unit, 0),
        name="down",
    )(q, near, far, near_got, far_got, rows_got, hid.reshape(2, count // 2, hidden))
    norms = norms.transpose(1, 0, 2).reshape(2, width)
    norms = spread(norms)
    while len(norms) > 1:
        norms = [a + b for a, b in zip(norms[::2], norms[1::2])]
    norms = norms[0]

    token_part, token_grad = call(
        home_kernel, (shape(toks, cols), shape(toks, width)),
        False, home_got, hot, hbm=(0, 1), limit=ALONE, out_hbm=True,
        scratch=[buffer(count, cols), buffer(count, toks), buffer(toks, cols), DMAS((2,))],
    )
    token_parts = spread(token_part)[1:]
    token_grad = pl.pallas_call(
        assemble_kernel,
        out_shape=shape(toks, width),
        in_specs=[HBM] + [VMEM] * (shares - 1),
        out_specs=HBM,
        scratch_shapes=[DMAS((shares - 1,))],
        input_output_aliases={0: 0},
        compiler_params=params(),
        name="assemble",
    )(token_grad, *token_parts)
    return (
        token_grad,
        router_sum.T,
        router_rows,
        gate_grad[None],
        up_grad[None],
        down_grad[None],
        norms[0:1],
        norms[1:2],
        down_rows,
    )


def solution(mesh):
    return jax.shard_map(
        per_device,
        mesh=mesh,
        in_specs=(
            P("ep", None),
            P("ep", None),
            P(),
            P("ep", None, "tp"),
            P("ep", None, "tp"),
            P("ep", "tp", None),
            P("ep", None),
        ),
        out_specs=(
            P("ep", None),
            P("tp", None),
            P("tp"),
            P("ep", None, "tp"),
            P("ep", None, "tp"),
            P("ep", "tp", None),
            P("ep", None),
            P("ep", None),
            P("ep", "tp"),
        ),
        check_vma=False,
    )
```

```python
import functools

import jax
import jax.numpy as jnp
from jax import lax
from jax.experimental import pallas as pl
from jax.experimental.pallas import tpu as pltpu
from jax.sharding import PartitionSpec as P


BF16 = jnp.bfloat16
F32 = jnp.float32
VMEM = pl.BlockSpec(memory_space=pltpu.VMEM)
SMEM = pl.BlockSpec(memory_space=pltpu.SMEM)
HBM = pl.BlockSpec(memory_space=pltpu.HBM)


def dot(a, b, ca=1, cb=0):
    return lax.dot_general(a, b, (((ca,), (cb,)), ((), ())), preferred_element_type=F32)


ALONE = 67043328
SHARED = 16 * 1024 * 1024
GRADS_ROOM = 4500000
COEF_LANE = 64


def params(limit=SHARED):
    return pltpu.CompilerParams(vmem_limit_bytes=limit)


def cost(flops, bytes_accessed):
    return pl.CostEstimate(flops=flops, bytes_accessed=bytes_accessed, transcendentals=0)


def fetch(sems, *pairs):
    copies = [pltpu.make_async_copy(src, dst, sems.at[i]) for i, (src, dst) in enumerate(pairs)]
    for copy in copies:
        copy.start()
    return copies


def one_hot(place, slots):
    experts, toks = place.shape
    rows = lax.broadcasted_iota(jnp.int32, (slots, toks), 0).astype(F32)
    return [(rows == place[e : e + 1, :]).astype(F32) for e in range(experts)]


def route_kernel(
    slots, tok_hbm, routing_hbm, router_hbm, rows_ref, place_ref,
    tok_ref, routing_ref, router_ref, sems,
):
    copies = fetch(sems, (tok_hbm, tok_ref), (routing_hbm, routing_ref), (router_hbm, router_ref))
    toks = tok_ref.shape[0]
    experts = router_ref.shape[0]
    cols = rows_ref.shape[2]
    start = pl.multiple_of(lax.axis_index("tp") * cols, 128)
    copies[1].wait()
    ids = lax.broadcasted_iota(jnp.int32, (experts, toks), 0)
    routed = routing_ref[...]
    named = jnp.zeros((experts, toks), F32)
    for k in range(routed.shape[0]):
        named = named + (ids == routed[k : k + 1, :]).astype(F32)
    before = lax.broadcasted_iota(jnp.int32, (toks, toks), 0)
    after = lax.broadcasted_iota(jnp.int32, (toks, toks), 1)
    earlier = (before < after).astype(F32).astype(BF16)
    position = dot(named.astype(BF16), earlier)
    place = jnp.where(named > 0, position, -1.0)
    copies[0].wait()
    copies[2].wait()
    aff = jax.nn.sigmoid(dot(router_ref[...], tok_ref[...], 1, 1))
    chosen = named * aff
    weights = chosen / jnp.sum(chosen, axis=0, keepdims=True)
    place_ref[...] = place
    hot = one_hot(place, slots)
    full = jnp.concatenate(hot, axis=0).astype(BF16)
    sent = dot(full, tok_ref[:, pl.ds(start, cols)])
    slope = named * aff * (1.0 - aff) / jnp.sum(chosen, axis=0, keepdims=True)
    row = lax.broadcasted_iota(jnp.int32, (experts, toks), 0)
    lane = lax.broadcasted_iota(jnp.int32, (8, 128), 1)
    for e in range(experts):
        own = weights[e : e + 1, :]
        others = jnp.sum(jnp.where(row == e, 0.0, weights), axis=0, keepdims=True)
        factors = jnp.where(row == e, others, -own) * slope
        table = jnp.concatenate([factors, own, jnp.zeros((127 - experts, toks), F32)], axis=0)
        values = dot(hot[e].astype(BF16), table.astype(BF16), 1, 1)
        tile = jnp.zeros((8, 128), F32)
        for g in range(slots // 8):
            part = values[8 * g : 8 * g + 8, :]
            tile = jnp.where(lane == g, part[:, experts : experts + 1], tile)
            shift = COEF_LANE + g * experts
            moved = pltpu.roll(part, shift, 1)
            tile = jnp.where((lane >= shift) & (lane < shift + experts), moved, tile)
        if cols > 128:
            tile = jnp.concatenate([tile, jnp.zeros((8, cols - 128), F32)], axis=1)
        block = jnp.concatenate([sent[e * slots : (e + 1) * slots, :], tile], axis=0)
        rows_ref[e] = block.astype(BF16)


def cots_kernel(slots, cot_hbm, place_ref, *refs):
    cot_ref, sems = refs[-2:]
    experts, toks = place_ref.shape
    cols = cot_ref.shape[1]
    start = pl.multiple_of((lax.axis_index("tp") % 2) * cols, 128)
    copies = fetch(sems, (cot_hbm.at[:, pl.ds(start, cols)], cot_ref))
    rows = lax.broadcasted_iota(jnp.int32, (slots, toks), 0).astype(F32)
    hot = [
        (rows == place_ref[pl.ds(lax.axis_index("ep") ^ k, 1), :]).astype(F32) for k in range(experts)
    ]
    full = jnp.concatenate(hot, axis=0).astype(BF16)
    copies[0].wait()
    sent = dot(full, cot_ref[...])
    for k in range(experts):
        refs[k][...] = sent[k * slots : (k + 1) * slots, :].astype(BF16)


def half_of(groups):
    me = lax.axis_index("ep")
    return me // (groups // 2), me % (groups // 2)


def join_kernel(*refs):
    out_ref = refs[-1]
    count = out_ref.shape[0]
    _, place = half_of(2 * count)
    for k in range(count):
        out_ref[place ^ k] = refs[k][...]


def add_parts(tokens_of, x_refs, wg_ref, wu_ref, acc_g, acc_u, fresh):
    groups, span, cols = x_refs[0].shape
    for r, x_ref in zip(tokens_of, x_refs):
        x = x_ref[...].reshape(groups * span, cols)
        rows = pl.ds(pl.multiple_of((lax.axis_index("tp") ^ r) * cols, 128), cols)
        part_g = dot(x, wg_ref[rows, :])
        part_u = dot(x, wu_ref[rows, :])
        acc_g[...] = part_g if fresh else acc_g[...] + part_g
        acc_u[...] = part_u if fresh else acc_u[...] + part_u
        fresh = False


def first_parts_kernel(which, *refs):
    count = len(which)
    add_parts(which, refs[:count], *refs[count:], True)


def more_parts_kernel(which, got_g, got_u, *refs):
    count = len(which)
    acc_g, acc_u = refs[-2:]
    acc_g[...] = got_g[...]
    acc_u[...] = got_u[...]
    add_parts(which, refs[:count], *refs[count:], False)


def gate_up_kernel(slots, which, got_g, got_u, own_ref, *refs):
    count = len(which)
    wg_ref, wu_ref, hid_ref, up_ref, gate_ref, acc_g, acc_u = refs[count:]
    groups, span, _ = own_ref.shape
    acc_g[...] = got_g[...]
    acc_u[...] = got_u[...]
    add_parts(which, refs[:count], wg_ref, wu_ref, acc_g, acc_u, False)
    for e in range(groups):
        scale = scale_column(own_ref, e, slots)
        at = slice(e * span, e * span + slots)
        pre_gate = acc_g[at, :]
        pre_up = acc_u[at, :]
        sig = jax.nn.sigmoid(pre_gate)
        act = pre_gate * sig
        hid_ref[e] = (act * pre_up).astype(BF16)
        up_ref[e] = scale * act
        gate_ref[e] = scale * (pre_up * sig * (1.0 + pre_gate * (1.0 - sig)))


def scale_column(x_ref, e, slots):
    tile = x_ref[e, slots:, :128].astype(F32)
    return jnp.concatenate([tile[:, g : g + 1] for g in range(slots // 8)], axis=0)


def back_kernel(groups, near_ref, far_ref, near_got, wd_ref, back_ref):
    cols = near_ref.shape[1]
    side, _ = half_of(groups)
    core = lax.axis_index("tp") % 2
    own = wd_ref[:, pl.ds(pl.multiple_of(core * cols, 128), cols)]
    other = wd_ref[:, pl.ds(pl.multiple_of((core ^ 1) * cols, 128), cols)]
    back_ref[1 - side] = dot(far_ref[...], own, 1, 1)
    back_ref[side] = dot(near_ref[...], own, 1, 1) + dot(near_got[...], other, 1, 1)


def slot_parts(first, gg, gu, wg_ref, wu_ref, shares):
    cols = wg_ref.shape[0] // shares
    start = pl.multiple_of((lax.axis_index("tp") ^ first) * cols, 128)
    return dot(gg, wg_ref[pl.ds(start, cols), :], 1, 1) + dot(
        gu, wu_ref[pl.ds(start, cols), :], 1, 1
    )


def middle_kernel(
    slots, shares, back_ref, far_ref, wd_ref, hid_ref, up_ref, gate_ref, wg_ref, wu_ref,
    g_ref, chip_ref, term_ref, sum_ref,
):
    cols = far_ref.shape[1]
    groups = g_ref.shape[0]
    side, _ = half_of(groups)
    start = pl.multiple_of(((lax.axis_index("tp") % 2) ^ 1) * cols, 128)
    wd = wd_ref[:, pl.ds(start, cols)]
    sum_ref[side] = back_ref[side]
    sum_ref[1 - side] = back_ref[1 - side] + dot(far_ref[...], wd, 1, 1)
    back = sum_ref[...].reshape(hid_ref.shape)
    hidden = hid_ref.shape[1]
    term = jnp.sum(hid_ref[...].astype(F32) * back, axis=1, keepdims=True)
    gu = back * up_ref[...]
    gg = back * gate_ref[...]
    pad = jnp.zeros((8, gu.shape[1]), F32)
    for e in range(groups):
        at = slice(e * slots, (e + 1) * slots)
        g_ref[e, :, :hidden] = jnp.concatenate([gg[at], pad], axis=0).astype(BF16)
        g_ref[e, :, hidden:] = jnp.concatenate([gu[at], pad], axis=0).astype(BF16)
    lane = lax.broadcasted_iota(jnp.int32, term_ref.shape, 1)
    tile = jnp.zeros(term_ref.shape, F32)
    for c in range(term.shape[0] // 8):
        tile = jnp.where(lane == c, term[8 * c : 8 * c + 8, :], tile)
    term_ref[...] = tile
    gg = gg.astype(BF16)
    gu = gu.astype(BF16)
    for j in range(1, shares // 2):
        chip_ref[j - 1] = slot_parts(2 * j + 1, gg, gu, wg_ref, wu_ref, shares).astype(BF16)


def even_kernel(slots, shares, g_ref, wg_ref, wu_ref, chip_ref):
    groups, span, double = g_ref.shape
    both = g_ref[...].reshape(groups * span, double)
    gg, gu = both[:, : double // 2], both[:, double // 2 :]
    for j in range(1, shares // 2):
        part = slot_parts(2 * j, gg, gu, wg_ref, wu_ref, shares)
        for e in range(groups):
            chip_ref[j - 1, e * slots : (e + 1) * slots, :] = part[e * span : e * span + slots, :]


def rest_kernel(slots, shares, g_ref, wg_ref, wu_ref, odd_ref, even_ref):
    groups, span, double = g_ref.shape
    both = g_ref[...].reshape(groups * span, double)
    gg, gu = both[:, : double // 2], both[:, double // 2 :]
    for r, out_ref in enumerate((even_ref, odd_ref)):
        part = slot_parts(r, gg, gu, wg_ref, wu_ref, shares)
        for e in range(groups):
            block = part[e * span : e * span + slots, :]
            out_ref[e] = block.astype(out_ref.dtype)


def add_core_kernel(own_ref, got_ref, out_ref):
    out_ref[...] = (own_ref[...] + got_ref[...].astype(F32)).astype(BF16)


def base_kernel(own_ref, core_ref, table_ref, router_ref, out_ref):
    experts = router_ref.shape[0]
    cols = out_ref.shape[1]
    start = pl.multiple_of(lax.axis_index("tp") * cols, 128)
    total = own_ref[...] + core_ref[...].astype(F32)
    out_ref[...] = total + dot(table_ref[...][:, :experts].astype(BF16), router_ref[:, pl.ds(start, cols)])


def add_chip_kernel(base_ref, *refs):
    total = base_ref[...]
    for chip_ref in refs[:-1]:
        total = total + chip_ref[...].astype(F32)
    refs[-1][...] = total.astype(BF16)


def grads_kernel(shares, q_ref, *refs):
    x_refs = refs[:shares]
    g_ref, gate_out, up_out, rows_out = refs[shares:]
    groups, span, cols = x_refs[0].shape
    double = g_ref.shape[2]
    for r in range(shares):

        @pl.when(pl.program_id(0) == r)
        def _(x_ref=x_refs[r]):
            x = x_ref[...].reshape(groups * span, cols)
            both = dot(x, g_ref[...].reshape(groups * span, double), 0, 0)
            gate, up = both[:, : double // 2], both[:, double // 2 :]
            gate_out[...] = gate.astype(BF16)
            up_out[...] = up.astype(BF16)
            rows_out[0, 0:1, :] = square_rows(gate)
            rows_out[0, 1:2, :] = square_rows(up)


def square_rows(value):
    square = value * value
    folded = square[:, :128]
    for at in range(128, value.shape[1], 128):
        folded = folded + square[:, at : at + 128]
    return jnp.sum(folded.T, axis=0, keepdims=True)


def down_kernel(slots, q_ref, *refs):
    x_ref, hid_ref, down_out, rows_out = refs[4:]
    groups = x_ref.shape[0]
    side, _ = half_of(groups)
    for h in range(2):

        @pl.when(pl.program_id(0) == h)
        def _(pair=refs[2 * h : 2 * h + 2]):
            down = 0.0
            for z_ref, at in zip(pair, (side, 1 - side)):
                scale = [scale_column(x_ref, at * (groups // 2) + e, slots) for e in range(groups // 2)]
                scale = jnp.concatenate(scale, axis=0)
                weighted = (scale * z_ref[...].astype(F32)).astype(BF16)
                down = down + dot(hid_ref[at], weighted, 0, 0)
            down_out[...] = down.astype(BF16)
            if h == 0:
                rows_out[...] = square_rows(down)
            else:
                rows_out[...] += square_rows(down)


def add_kernel(a_ref, b_ref, out_ref):
    out_ref[...] = a_ref[...] + b_ref[...]


def terms_kernel(slots, a_ref, b_ref, x_ref, table_ref, part_ref):
    term = (a_ref[...] + b_ref[...]).astype(BF16).astype(F32)
    groups, span, cols = x_ref.shape
    experts = part_ref.shape[0]
    count = slots // 8
    blocks = []
    for b in range(groups):
        spare = x_ref[b, slots:, :128].astype(F32)
        for g in range(count):
            factors = pltpu.roll(spare, 128 - COEF_LANE - g * experts, 1)
            c = b * count + g
            blocks.append(term[:, c : c + 1] * factors)
        blocks.append(jnp.zeros((8, 128), F32))
    table = jnp.concatenate(blocks, axis=0)
    table = jnp.where(lax.broadcasted_iota(jnp.int32, table.shape, 1) < experts, table, 0.0)
    for b in range(groups):
        table_ref[b * slots : (b + 1) * slots, :] = table[b * span : b * span + slots, :]
    high = table.astype(BF16)
    low = (table - high.astype(F32)).astype(BF16)
    x = x_ref[...].reshape(groups * span, cols)
    part_ref[...] = (dot(high, x, 0, 0) + dot(low, x, 0, 0))[:experts]


def last_sum_kernel(a_ref, b_ref, sum_ref, rows_ref):
    total = a_ref[...] + b_ref[...]
    sum_ref[...] = total
    rows_ref[...] = jnp.sum(total * total, axis=0, keepdims=True)


def slot_map_kernel(slots, place_ref, hot_ref):
    hot_ref[...] = jnp.concatenate(one_hot(place_ref[...], slots), axis=0).astype(BF16)


def home_kernel(got_hbm, hot_hbm, token_out, whole_hbm, got_ref, hot_ref, own_ref, sems):
    cols = got_ref.shape[1]
    start = pl.multiple_of(lax.axis_index("tp") * cols, 128)
    middle = got_ref.shape[0] // 2
    first, second = slice(0, middle), slice(middle, 2 * middle)
    copies = fetch(
        sems, (hot_hbm, hot_ref), (got_hbm.at[first], got_ref.at[first]), (got_hbm.at[second], got_ref.at[second])
    )
    copies[0].wait()
    copies[1].wait()
    total = dot(hot_ref[first], got_ref[first], 0, 0)
    copies[2].wait()
    own_ref[...] = (total + dot(hot_ref[second], got_ref[second], 0, 0)).astype(BF16)
    copies = fetch(sems, (own_ref, token_out), (own_ref, whole_hbm.at[:, pl.ds(start, cols)]))
    for copy in copies:
        copy.wait()


def assemble_kernel(*refs):
    out_hbm, sems = refs[-2:]
    pairs = []
    for r, ref in enumerate(refs[1:-2]):
        cols = ref.shape[1]
        start = pl.multiple_of((lax.axis_index("tp") ^ (r + 1)) * cols, 128)
        pairs.append((ref, out_hbm.at[:, pl.ds(start, cols)]))
    for copy in fetch(sems, *pairs):
        copy.wait()


def call(kernel, outs, scalar, *args, flops=0, nbytes=0, scratch=(), hbm=(), out_hbm=False, limit=SHARED):
    single = not isinstance(outs, tuple)
    ins = [HBM if i in hbm else VMEM for i in range(int(scalar), len(args))]
    out = HBM if out_hbm else VMEM
    return pl.pallas_call(
        kernel,
        out_shape=outs,
        in_specs=([SMEM] if scalar else []) + ins,
        out_specs=out if single else tuple(out for _ in outs),
        scratch_shapes=list(scratch),
        compiler_params=params(limit),
        cost_estimate=cost(flops, nbytes),
    )(*args)


DMAS = pltpu.SemaphoreType.DMA


def buffer(*dims, dtype=BF16):
    return pltpu.VMEM(dims, dtype)


def shape(*dims, dtype=BF16):
    return jax.ShapeDtypeStruct(dims, dtype)


def per_device(tokens, routing, router_weight, gate_weight, up_weight, down_weight, cotangent):
    return layer(tokens, routing.T, router_weight.T, gate_weight[0], up_weight[0], down_weight[0], cotangent)


def layer(tokens, routing, router, wg, wu, wd, cotangent):
    groups = lax.axis_size("ep")
    shares = lax.axis_size("tp")
    chips = shares // 2
    toks, width = tokens.shape
    top = routing.shape[0]
    experts = router.shape[0]
    hidden = wg.shape[1]
    capacity = 7 * toks * top // (4 * experts)
    slots = -(-capacity // 8) * 8
    span = slots + 8
    count = groups * slots
    cols = width // shares
    half = width // 2
    unit = 2 * count * half * hidden
    q = lax.axis_index("tp").astype(jnp.int32).reshape(1)

    def swap(value, bit, axis="tp"):
        size = lax.axis_size(axis)
        return lax.ppermute(value, axis, [(i, i ^ bit) for i in range(size)])

    def exchange(value):
        return lax.all_to_all(value, "ep", split_axis=0, concat_axis=0, tiled=True)

    def spread(value):
        far = [value] + [swap(value, 2 * j) for j in range(1, chips)]
        return [part for piece in far for part in (piece, swap(piece, 1))]

    rows_send, place = call(
        functools.partial(route_kernel, slots),
        (shape(experts, span, cols), shape(experts, toks, dtype=F32)),
        False, tokens, routing, router, hbm=(0, 1, 2), limit=ALONE,
        scratch=[buffer(toks, width), buffer(top, toks, dtype=jnp.int32), buffer(experts, width), DMAS((3,))],
    )
    rows_got = exchange(rows_send)
    pieces = call(
        functools.partial(cots_kernel, slots), tuple(shape(slots, half) for _ in range(experts)),
        False, cotangent, place, flops=2 * count * toks * half, hbm=(0,), limit=ALONE,
        scratch=[buffer(toks, half), DMAS((1,))],
    )
    pieces = list(pieces)
    for k in range(experts - 1, 0, -1):
        pieces[k] = swap(pieces[k], k, "ep")

    hot = call(functools.partial(slot_map_kernel, slots), shape(count, toks), False, place)

    x_parts = spread(rows_got)
    sums = tuple(shape(groups * span, hidden, dtype=F32) for _ in range(2))
    chip_parts, core_parts = list(range(2, shares, 2)), list(range(3, shares, 2))
    pre = call(
        functools.partial(first_parts_kernel, (0, 1)), sums,
        False, *x_parts[:2], wg, wu, flops=unit,
    )
    pre = call(
        functools.partial(more_parts_kernel, chip_parts), sums,
        False, *pre, *[x_parts[r] for r in chip_parts], wg, wu, flops=unit,
    )
    hid, up_factor, gate_factor = call(
        functools.partial(gate_up_kernel, slots, core_parts),
        (shape(groups, slots, hidden), shape(groups, slots, hidden, dtype=F32), shape(groups, slots, hidden, dtype=F32)),
        False, *pre, x_parts[0], *[x_parts[r] for r in core_parts], wg, wu, flops=2 * unit,
        scratch=[pltpu.VMEM((groups * span, hidden), F32)] * 2,
    )
    hid = hid.reshape(count, hidden)
    up_factor = up_factor.reshape(count, hidden)
    gate_factor = gate_factor.reshape(count, hidden)

    side = groups // 2
    near = call(join_kernel, shape(side, slots, half), False, *pieces[:side]).reshape(count // 2, half)
    near_got = swap(near, 1)
    far = call(join_kernel, shape(side, slots, half), False, *pieces[side:]).reshape(count // 2, half)
    far_got = swap(far, 1)
    back = call(
        functools.partial(back_kernel, groups), shape(2, count // 2, hidden, dtype=F32),
        False, near, far, near_got, wd, flops=unit,
    )
    g, odd_chip, term = call(
        functools.partial(middle_kernel, slots, shares),
        (
            shape(groups, span, 2 * hidden),
            shape(chips - 1, count, cols),
            shape(8, -(-count // 1024) * 128, dtype=F32),
        ),
        False, back, far_got, wd, hid, up_factor, gate_factor, wg, wu, flops=3 * unit,
        scratch=[buffer(2, count // 2, hidden, dtype=F32)],
    )
    term_got = swap(term, 1)
    core_chip = swap(odd_chip, 1)
    even_chip = call(
        functools.partial(even_kernel, slots, shares), shape(chips - 1, count, cols, dtype=F32),
        False, g, wg, wu, flops=unit,
    )
    odd_home, even_home = call(
        functools.partial(rest_kernel, slots, shares),
        (shape(groups, slots, cols), shape(groups, slots, cols, dtype=F32)),
        False, g, wg, wu, flops=2 * unit,
    )
    even_home = even_home.reshape(count, cols)
    core_home = swap(odd_home.reshape(count, cols), 1)

    def add(a, b, kernel=add_kernel, lead=()):
        return call(kernel, shape(*lead, *a.shape, dtype=F32), False, a, b)

    term = add(term, term_got)
    bit = 2
    while 2 * bit < shares:
        term = add(term, swap(term, bit))
        bit *= 2
    term_got = swap(term, bit)
    chip_send = call(add_core_kernel, shape(chips - 1, count, cols), False, even_chip, core_chip)
    chip_got = [swap(chip_send[j], 2 * (j + 1)) for j in range(chips - 1)]
    table, router_sum = call(
        functools.partial(terms_kernel, slots),
        (shape(count, 128, dtype=F32), shape(experts, cols, dtype=F32)),
        False, term, term_got, rows_got,
    )
    bit = 1
    while 2 * bit < groups:
        router_got = swap(router_sum, bit, "ep")
        router_sum = add(router_sum, router_got)
        bit *= 2
    router_got = swap(router_sum, bit, "ep")
    router_sum, router_rows = call(
        last_sum_kernel, (shape(experts, cols, dtype=F32), shape(1, cols, dtype=F32)),
        False, router_sum, router_got,
    )
    router_rows = router_rows.reshape(cols)
    base = call(base_kernel, shape(count, cols, dtype=F32), False, even_home, core_home, table, router)
    home_send = call(add_chip_kernel, shape(count, cols), False, base, *chip_got)
    home_got = exchange(home_send.reshape(groups, slots, cols)).reshape(count, cols)

    grad_spec = pl.BlockSpec((cols, hidden), lambda r, q: (q[0] ^ r, 0))
    gate_grad, up_grad, norms = pl.pallas_call(
        functools.partial(grads_kernel, shares),
        out_shape=(shape(width, hidden), shape(width, hidden), shape(shares, 2, cols, dtype=F32)),
        grid_spec=pltpu.PrefetchScalarGridSpec(
            num_scalar_prefetch=1,
            grid=(shares,),
            in_specs=[VMEM] * (shares + 1),
            out_specs=(grad_spec, grad_spec, pl.BlockSpec((1, 2, cols), lambda r, q: (q[0] ^ r, 0, 0))),
        ),
        compiler_params=params(ALONE - GRADS_ROOM),
        cost_estimate=cost(4 * unit, 0),
        name="grads",
    )(q, *x_parts, g)
    down_grad, down_rows = pl.pallas_call(
        functools.partial(down_kernel, slots),
        out_shape=(shape(hidden, width), shape(1, hidden, dtype=F32)),
        grid_spec=pltpu.PrefetchScalarGridSpec(
            num_scalar_prefetch=1,
            grid=(2,),
            in_specs=[VMEM] * 6,
            out_specs=(
                pl.BlockSpec((hidden, half), lambda h, q: (0, (q[0] % 2) ^ h)),
                pl.BlockSpec((1, hidden), lambda h, q: (0, 0)),
            ),
        ),
        compiler_params=params(ALONE),
        cost_estimate=cost(2 * unit, 0),
        name="down",
    )(q, near, far, near_got, far_got, rows_got, hid.reshape(2, count // 2, hidden))
    norms = norms.transpose(1, 0, 2).reshape(2, width)
    norms = spread(norms)
    while len(norms) > 1:
        norms = [a + b for a, b in zip(norms[::2], norms[1::2])]
    norms = norms[0]

    token_part, token_grad = call(
        home_kernel, (shape(toks, cols), shape(toks, width)),
        False, home_got, hot, hbm=(0, 1), limit=ALONE, out_hbm=True,
        scratch=[buffer(count, cols), buffer(count, toks), buffer(toks, cols), DMAS((3,))],
    )
    token_parts = spread(token_part)[1:]
    token_grad = pl.pallas_call(
        assemble_kernel,
        out_shape=shape(toks, width),
        in_specs=[HBM] + [VMEM] * (shares - 1),
        out_specs=HBM,
        scratch_shapes=[DMAS((shares - 1,))],
        input_output_aliases={0: 0},
        compiler_params=params(),
        name="assemble",
    )(token_grad, *token_parts)
    return (
        token_grad,
        router_sum.T,
        router_rows,
        gate_grad[None],
        up_grad[None],
        down_grad[None],
        norms[0:1],
        norms[1:2],
        down_rows,
    )


def solution(mesh):
    return jax.shard_map(
        per_device,
        mesh=mesh,
        in_specs=(
            P("ep", None),
            P("ep", None),
            P(),
            P("ep", None, "tp"),
            P("ep", None, "tp"),
            P("ep", "tp", None),
            P("ep", None),
        ),
        out_specs=(
            P("ep", None),
            P("tp", None),
            P("tp"),
            P("ep", None, "tp"),
            P("ep", None, "tp"),
            P("ep", "tp", None),
            P("ep", None),
            P("ep", None),
            P("ep", "tp"),
        ),
        check_vma=False,
    )
```
